128 devices in a mesh: sp: 16 (over z, y), fs: 4 (over x), tp: 2 (over core).
Axes of the slice: x: 4, y: 4, z: 4, core: 2. Of those that a mesh axis runs over, the one named last changes fastest.
Arguments:
- tokens: bfloat16 [8, 2048, 2048], P('fs', 'sp', 'tp'), may hold values from -8 to 8
- norm_gain: float32 [2048], replicated, may hold values from 0.1 to 1.9
- w_recept: bfloat16 [2048, 768], P(None, 'tp'), may hold values from -0.125 to 0.125
- w_key: bfloat16 [2048, 768], P(None, 'tp'), may hold values from -0.125 to 0.125
- w_value: bfloat16 [2048, 768], P(None, 'tp'), may hold values from -0.125 to 0.125
- w_decay: bfloat16 [2048, 768], P(None, 'tp'), may hold values from -0.125 to 0.125
- w_rate: bfloat16 [2048, 768], P(None, 'tp'), may hold values from -0.125 to 0.125
- w_gate_rec: bfloat16 [2048, 768], P(None, 'tp'), may hold values from -0.125 to 0.125
- w_pool: bfloat16 [2048, 512], P(None, 'tp'), may hold values from -0.125 to 0.125
- w_gate_pool: bfloat16 [2048, 512], P(None, 'tp'), may hold values from -0.125 to 0.125
- decay_base: float32 [768], replicated, may hold values from -12 to -2.5
- rate_base: float32 [768], replicated, may hold values from -7 to 1
- head_gain: float32 [768], replicated, may hold values from 0.1 to 1.9
- pool_mix: bfloat16 [4, 128, 128], replicated, may hold values from -0.5 to 0.5
- pool_scale: float32 [512], replicated, may hold values from 0.3 to 3
- w_out_rec: bfloat16 [768, 2048], P('tp'), may hold values from -0.15625 to 0.15625
- w_out_pool: bfloat16 [512, 2048], P('tp'), may hold values from -0.15625 to 0.15625
- init_state: float32 [8, 12, 64, 64], P('fs', 'tp'), may hold values from -240 to 240
Outputs:
- mixed: bfloat16 [8, 2048, 2048], P('fs', 'sp', 'tp')
The draws below stay inside these ranges and needn't reach their ends.
All inputs are finite; a program needn't handle non-finite values.
Results may differ from the reference program's by a relative error of at most 0.015.
Values may be sent and summed in bfloat16 or wider, within the bound.
A program may use at most 128 MiB of HBM per device.

```python
import math
import jax
import jax.numpy as jnp
from jax import lax

D = 2048
HEADS = 12
HEAD_DIM = 64
GROUPS = 4
GROUP_W = 128
RW = 768
PW = 512
LENGTH = 2048
SEQS = 8
N_TP = 2


def head_kinds(key):
    base = jax.random.fold_in(key, 7)
    first, second, third = jax.random.split(base, 3)
    head_ids = jnp.arange(HEADS)
    coins = jax.random.randint(first, (HEADS,), 0, 2)
    slow_pick = jax.random.randint(second, (), 0, HEADS)
    fast_pick = (slow_pick + 1 + jax.random.randint(third, (), 0, HEADS - 1)) % HEADS
    slow = jnp.where(head_ids == slow_pick, 1, jnp.where(head_ids == fast_pick, 0, coins))
    return jnp.repeat(slow, HEAD_DIM)


def draw_decay_base(key, part):
    slow = head_kinds(key)
    slow_value = jax.random.uniform(jax.random.fold_in(key, 21), (RW,), jnp.float32, -12.0, -10.0)
    fast_value = jax.random.uniform(jax.random.fold_in(key, 22), (RW,), jnp.float32, -3.5, -2.5)
    return jnp.where(slow == 1, slow_value, fast_value).astype(jnp.float32)


def draw_rate_base(key, part):
    slow = head_kinds(key)
    slow_value = jax.random.uniform(jax.random.fold_in(key, 31), (RW,), jnp.float32, -7.0, -5.5)
    fast_value = jax.random.uniform(jax.random.fold_in(key, 32), (RW,), jnp.float32, -1.0, 1.0)
    return jnp.where(slow == 1, slow_value, fast_value).astype(jnp.float32)


def draw_tokens(key, part):
    first, second = jax.random.split(jax.random.fold_in(key, 3))
    means = jax.random.truncated_normal(second, -4.0, 4.0, (SEQS, LENGTH // 64, D), jnp.float32)
    means = jnp.repeat(means, 64, axis=1)
    noise = jax.random.truncated_normal(first, -4.0, 4.0, (SEQS, LENGTH, D), jnp.float32)
    values = noise + 0.8 * means
    return values.astype(jnp.bfloat16)


def steps_of(key, shape, shards, low, top_value):
    def one(position, parts):
        draws = jax.random.uniform(jax.random.fold_in(jax.random.fold_in(key, 6), position), (parts,), jnp.float32, low / len(shards), top_value / len(shards))
        return jnp.repeat(jnp.exp(draws), shape[position] // parts).reshape((-1,) + (1,) * (len(shape) - position - 1))

    factor_of = one(*shards[0])
    for cut in shards[1:]:
        factor_of = factor_of * one(*cut)
    return factor_of


def bell_draw(own_key, extent, scale, most, shards=(), held_as=jnp.bfloat16):
    gain = steps_of(own_key, extent, shards, -0.22, 0.18) if shards else 1.0
    values = jax.random.normal(own_key, extent, jnp.float32) * scale * gain
    return jnp.minimum(jnp.maximum(values, -most), most).astype(held_as)


def setup_inputs(seed: int = 0) -> dict:
    splits = jax.random.split(jax.random.key(seed), 19)
    return {
        "tokens": draw_tokens(jax.random.fold_in(splits[18], 71), 0),
        "norm_gain": jnp.clip(1.0 + 0.18 * jax.random.normal(splits[1], (D,), jnp.float32), 0.1, 1.9),
        "w_recept": bell_draw(splits[2], (D, RW), D ** -0.5, 0.125, ((1, 2),)),
        "w_key": bell_draw(splits[3], (D, RW), D ** -0.5, 0.125, ((1, 2),)),
        "w_value": bell_draw(splits[4], (D, RW), D ** -0.5, 0.125, ((1, 2),)),
        "w_decay": bell_draw(splits[5], (D, RW), D ** -0.5, 0.125, ((1, 2),)),
        "w_rate": bell_draw(splits[6], (D, RW), D ** -0.5, 0.125, ((1, 2),)),
        "w_gate_rec": bell_draw(splits[7], (D, RW), D ** -0.5, 0.125, ((1, 2),)),
        "w_pool": bell_draw(splits[8], (D, PW), D ** -0.5, 0.125, ((1, 2),)),
        "w_gate_pool": bell_draw(splits[9], (D, PW), D ** -0.5, 0.125, ((1, 2),)),
        "decay_base": draw_decay_base(jax.random.fold_in(splits[18], 71), 0),
        "rate_base": draw_rate_base(jax.random.fold_in(splits[18], 71), 0),
        "head_gain": jnp.clip(1.0 + 0.18 * jax.random.normal(splits[12], (RW,), jnp.float32), 0.1, 1.9),
        "pool_mix": bell_draw(splits[13], (GROUPS, GROUP_W, GROUP_W), GROUP_W ** -0.5, 0.5),
        "pool_scale": jnp.clip(jnp.exp(jax.random.uniform(splits[14], (PW,), jnp.float32, math.log(0.3), math.log(3.0))), 0.3, 3.0),
        "w_out_rec": bell_draw(splits[15], (RW, D), (RW + PW) ** -0.5, 0.15625, ((0, 2),)),
        "w_out_pool": bell_draw(splits[16], (PW, D), (RW + PW) ** -0.5, 0.15625, ((0, 2),)),
        "init_state": bell_draw(splits[17], (SEQS, HEADS, HEAD_DIM, HEAD_DIM), 40.0, 240.0, ((0, 4), (1, 2)), jnp.float32),
    }


HIGHEST = lax.Precision.HIGHEST

def reference(tokens, norm_gain, w_recept, w_key, w_value, w_decay, w_rate, w_gate_rec, w_pool, w_gate_pool, decay_base, rate_base, head_gain, pool_mix, pool_scale, w_out_rec, w_out_pool, init_state):
    wide = tokens.astype(jnp.float32)
    scale = lax.rsqrt(lax.optimization_barrier(jnp.mean(wide * wide, axis=-1, keepdims=True)) + 0.25)
    normed = (wide * norm_gain).astype(jnp.bfloat16)
    flat = normed.reshape(-1, D)

    def project(weight):
        product = jnp.dot(flat, weight, preferred_element_type=jnp.float32).reshape(SEQS, LENGTH, -1)
        return (product * scale).astype(jnp.bfloat16)
    receptance, key_proj, value, decay_in, rate_in, gate_rec, pool_in, gate_pool = [project(weight) for weight in (w_recept, w_key, w_value, w_decay, w_rate, w_gate_rec, w_pool, w_gate_pool)]

    def split_heads(array):
        return array.astype(jnp.float32).reshape(SEQS, LENGTH, HEADS, HEAD_DIM)
    log_decay = -jnp.exp(-jax.nn.softplus(-(decay_base + decay_in.astype(jnp.float32))) - 0.5)
    rate = jax.nn.sigmoid(rate_base + rate_in.astype(jnp.float32))
    keys = split_heads(key_proj)
    unit_key = keys * lax.rsqrt(lax.optimization_barrier(jnp.sum(keys * keys, axis=-1, keepdims=True)) + 1.0)
    removal = unit_key * split_heads(rate)
    inputs = tuple((jnp.moveaxis(array, 1, 0) for array in (split_heads(receptance), keys, split_heads(value), jnp.exp(split_heads(log_decay)), unit_key, removal)))

    def advance(state, item):
        read, write_key, write_value, decay, unit, remove = item
        removed = jnp.einsum('bhvk,bhk->bhv', state, unit, precision=HIGHEST)
        state = state * decay[:, :, None, :] - removed[..., None] * remove[:, :, None, :] + write_value[..., None] * write_key[:, :, None, :]
        return (state, jnp.einsum('bhvk,bhk->bhv', state, read, precision=HIGHEST))
    _, outputs = lax.scan(advance, init_state, inputs)
    recurrent = jnp.moveaxis(outputs, 0, 1)
    center = lax.optimization_barrier(jnp.mean(recurrent, axis=-1, keepdims=True))
    spread = lax.optimization_barrier(jnp.mean(jnp.square(recurrent - center), axis=-1, keepdims=True))
    normal_out = ((recurrent - center) * lax.rsqrt(spread + 1.0)).reshape(SEQS, LENGTH, RW) * head_gain
    rec_out = (normal_out * jax.nn.silu(gate_rec.astype(jnp.float32))).astype(jnp.bfloat16)
    pool_wide = pool_in.astype(jnp.float32)
    padded = jnp.pad(pool_wide, ((0, 0), (15, 0), (0, 0)))
    places = jnp.arange(1, LENGTH + 1, dtype=jnp.float32)[None, :, None]
    pieces = []
    for group in range(GROUPS):
        window = 2 ** (group + 1)
        low = group * GROUP_W
        trailing = padded[:, 15:15 + LENGTH, low:low + GROUP_W]
        for offset in range(1, window):
            trailing = trailing + padded[:, 15 - offset:15 - offset + LENGTH, low:low + GROUP_W]
        pieces.append(trailing / jnp.minimum(places, float(window)) - pool_wide[:, :, low:low + GROUP_W])
    diffs = jnp.stack(pieces, axis=2).astype(jnp.bfloat16)
    pool_mixed = jnp.einsum('bsgc,gcd->bsgd', diffs.astype(jnp.float32), pool_mix.astype(jnp.float32)).reshape(SEQS, LENGTH, PW)
    pool_out = (pool_mixed * pool_scale * jax.nn.silu(gate_pool.astype(jnp.float32))).astype(jnp.bfloat16)
    rec_block = RW // N_TP
    pool_block = PW // N_TP
    rec_flat = rec_out.reshape(-1, RW)
    pool_flat = pool_out.reshape(-1, PW)
    total = jnp.zeros((SEQS * LENGTH, D), jnp.float32)
    for index in range(N_TP):
        first = jnp.dot(rec_flat[:, index * rec_block:(index + 1) * rec_block], w_out_rec[index * rec_block:(index + 1) * rec_block], preferred_element_type=jnp.float32)
        second = jnp.dot(pool_flat[:, index * pool_block:(index + 1) * pool_block], w_out_pool[index * pool_block:(index + 1) * pool_block], preferred_element_type=jnp.float32)
        partial_sum = lax.optimization_barrier((first + second).astype(jnp.bfloat16))
        total = total + partial_sum.astype(jnp.float32)
    return total.reshape(SEQS, LENGTH, D).astype(jnp.bfloat16)
```

```python
import math

import jax
import jax.numpy as jnp
from jax import lax
from jax.experimental import pallas as pl
from jax.experimental.pallas import tpu as pltpu
from jax.sharding import PartitionSpec as P

D = 2048
HALF = 1024
SEQ = 2
ROWS = 128
TOK = SEQ * ROWS
RCOLS = 384
PCOLS = 256
PAIRS = 3
GROUPS = SEQ * PAIRS
HD = 64
N_SP = 16
COLS = 6 * RCOLS + 2 * PCOLS
OFFS = (0, 384, 768, 1152, 1536, 1920, 2304, 2560)
WIDTHS = (384, 384, 384, 384, 384, 384, 256, 256)
MESH = pl.DeviceIdType.MESH
f32 = jnp.float32
bf16 = jnp.bfloat16


def dot(a, b):
    return lax.dot_general(a, b, (((1,), (0,)), ((), ())), preferred_element_type=f32)


def dot_nt(a, b):
    return lax.dot_general(a, b, (((1,), (1,)), ((), ())), preferred_element_type=f32)


def dot_tn(a, b):
    return lax.dot_general(a, b, (((0,), (0,)), ((), ())), preferred_element_type=f32)


def split2(x):
    hi = x.astype(bf16)
    return hi, (x - hi.astype(f32)).astype(bf16)


def cat(parts, axis):
    return jnp.concatenate(parts, axis=axis)


def sig(x):
    e = jnp.exp(-jnp.abs(x))
    return jnp.where(x >= 0, 1.0, e) / (1.0 + e)


def lane_first(shape):
    return lax.broadcasted_iota(jnp.int32, shape, len(shape) - 1) < HD


def keep(x, head):
    first = lane_first(x.shape)
    zero = jnp.zeros_like(x)
    return jnp.where(first, x, zero) if head == 0 else jnp.where(first, zero, x)


def two_heads(x):
    return cat([keep(x, 0), keep(x, 1)], 0)


def block_ones():
    i = lax.broadcasted_iota(jnp.int32, (128, 128), 0) < HD
    j = lax.broadcasted_iota(jnp.int32, (128, 128), 1) < HD
    return jnp.where(i == j, 1.0, 0.0).astype(bf16)


def head_sums(x, ones2):
    hi, lo = split2(x)
    return dot(cat([hi, lo], 1), ones2)


def prepare(r, k, v, d_in, a_in, d_base, a_base):
    ones = block_ones()
    ones2 = cat([ones, ones], 0)
    x = d_base + d_in
    log_decay = -math.exp(-0.5) * sig(x)
    rate = sig(a_base + a_in)
    unit = k * lax.rsqrt(head_sums(k * k, ones2) + 1.0)
    removal = unit * rate
    i = lax.broadcasted_iota(jnp.int32, (128, 128), 0)
    j = lax.broadcasted_iota(jnp.int32, (128, 128), 1)
    tri = jnp.where(i >= j, 1.0, 0.0).astype(bf16)
    hi, lo = split2(log_decay)
    rest = (log_decay - hi.astype(f32) - lo.astype(f32)).astype(bf16)
    cum = dot(cat([tri, tri], 1), cat([hi, lo], 0)) + dot(tri, rest)
    mid = cum[63:64, :]
    last = cum[127:128, :]
    shrink = jnp.exp(cum - mid)
    grow = jnp.exp(mid - cum)
    alpha = jnp.exp(cum - log_decay - mid) * unit
    rho = r * shrink
    beta = removal * grow
    kappa = k * grow
    return alpha, rho, beta, kappa, jnp.exp(mid), jnp.exp(last - mid), jnp.exp(last)


def pair_products(alpha, rho, beta, kappa):
    x_hi, x_lo = split2(cat([alpha, rho], 0))
    b_hi, b_lo = split2(beta)
    k_hi, k_lo = split2(kappa)
    y_hi = cat([two_heads(b_hi), two_heads(k_hi)], 0)
    y_lo = cat([two_heads(b_lo), two_heads(k_lo)], 0)
    return dot_nt(cat([x_hi, x_lo], 1), cat([y_hi, y_hi], 1)) + dot_nt(x_hi, y_lo)


def block_diag(a, b):
    zero = jnp.zeros_like(a)
    return cat([cat([a, zero], 1), cat([zero, b], 1)], 0)


def masks():
    i = lax.broadcasted_iota(jnp.int32, (128, 256), 0)
    j = lax.broadcasted_iota(jnp.int32, (128, 256), 1) & 127
    return i, j


def inverses(lowers):
    i, j = masks()
    apart = i ^ j
    eye = jnp.where(i == j, 1.0, 0.0)
    inv = [eye - jnp.where(apart == 1, low, 0.0) for low in lowers]
    for level in range(1, 7):
        size = 1 << level
        inside = (apart >= size) & (apart < 2 * size)
        inv_b = [x.astype(bf16) for x in inv]
        steps = [jnp.where(inside, low, 0.0).astype(bf16) for low in lowers]
        half = [
            dot(x, block_diag(c[:, :128], c[:, 128:])).astype(bf16)
            for x, c in zip(inv_b, steps)
        ]
        full = [dot(h, block_diag(x[:, :128], x[:, 128:])) for h, x in zip(half, inv_b)]
        inv = [x - y for x, y in zip(inv, full)]
    return [x.astype(bf16) for x in inv]


def stacked(left, right):
    return cat([cat([keep(left, h), keep(right, h)], 1) for h in (0, 1)], 0)


def solve(inv, low, carried, alpha_full):
    first = dot(inv, stacked(alpha_full.astype(bf16), carried.astype(bf16)))
    first_b = first.astype(bf16)
    l_hi, l_lo = split2(low)
    weights = stacked(first_b[:, :128], first_b[:, 128:])
    back = dot(l_hi, weights) + dot(l_lo, weights)
    kept = first_b.astype(f32)
    miss = (cat([alpha_full, carried], 1) - kept - back).astype(bf16)
    return kept + dot(inv, stacked(miss[:, :128], miss[:, 128:]))


def maps_of(z, value, beta_end, kappa_end, gain_end):
    z_hi, z_lo = split2(z)
    zero = jnp.zeros((128, 128), bf16)
    v_side = cat([zero, -value], 1)
    e_hi, e_lo = split2(cat([beta_end, kappa_end], 0))
    lhs = cat([z_hi, v_side], 0)
    both = dot_tn(lhs, e_hi) + dot_tn(lhs, e_lo) + dot_tn(z_lo, e_hi[:128])
    first = lane_first((64, 128))
    packed = [
        jnp.where(first, both[o : o + 64], both[o + 64 : o + 128]) for o in (0, 128)
    ]
    i = lax.broadcasted_iota(jnp.int32, (64, 128), 0)
    j = lax.broadcasted_iota(jnp.int32, (64, 128), 1) & 63
    transit = jnp.where(i == j, gain_end, 0.0) - packed[0]
    return transit.astype(bf16), (-packed[1]).astype(bf16)


def reads_of(within_beta, z, rho_full, within_value):
    w_hi, w_lo = split2(within_beta)
    z_hi, z_lo = split2(z)
    weights = stacked(z_hi[:, :128], z_hi[:, 128:])
    drop = dot(w_hi, weights) + dot(w_lo, weights)
    drop = drop + dot(w_hi, stacked(z_lo[:, :128], z_lo[:, 128:]))
    return rho_full - drop[:, :128], within_value - drop[:, 128:]


def advance(state, transit, written):
    hi, lo = split2(state)
    moved = dot(cat([hi, lo], 0), two_heads(transit))
    return moved[:64] + moved[64:] + written.astype(f32)


def recurrent_of(reads, state, local):
    hi, lo = split2(reads)
    weights = two_heads(state)
    return dot_nt(cat([hi, lo], 1), cat([weights, weights], 1)) + local


def head_norm(rec, gain, gate):
    ones = block_ones()
    ones2 = cat([ones, ones], 0)
    centred = rec - head_sums(rec, ones2) * (1.0 / HD)
    spread = head_sums(centred * centred, ones2) * (1.0 / HD)
    return (centred * lax.rsqrt(spread + 1.0) * gain * gate * sig(gate)).astype(bf16)


def kernel(
    tok, gain, wr, wk, wv, wd, wa, wg, wp, wgp, dbase, rbase, hgain, mix, pscale, wor, wop, init,
    out,
    tok_v, gain_v, weight_v, acc_v, proj_v, norm_v, base_v, mix_v, pscale_v, wout_v, init_v,
    pool_v, alpha_v, low_v, within_v, rho_v, wval_v, z_v, reads_v, local_v, map_v, maps_in,
    state_v, states_in, merged_v, recout_v, part_v, part_in, out_v,
    w_sem, small_sem, tok_send, tok_recv, halo_send, halo_recv, map_send, map_recv,
    st_send, st_recv, part_send, part_recv, out_sem,
):
    sp = lax.axis_index("sp")
    tp = lax.axis_index("tp")
    other = 1 - tp
    weights = (wr, wk, wv, wd, wa, wg, wp, wgp)
    group_of = lax.div(sp, 2)
    is_owner = (lax.rem(sp, 2) == tp) & (sp < 2 * GROUPS)

    barrier = pltpu.get_barrier_semaphore()
    pl.semaphore_signal(barrier, inc=1, device_id={"tp": other}, device_id_type=MESH)

    @pl.loop(1, N_SP)
    def _(step):
        pl.semaphore_signal(
            barrier, inc=1, device_id={"sp": lax.rem(sp + step, N_SP)}, device_id_type=MESH
        )

    mine = pl.multiple_of(tp * HALF, HALF)
    theirs = pl.multiple_of(other * HALF, HALF)
    rec_at = pl.multiple_of(tp * RCOLS, 128)
    pool_at = pl.multiple_of(tp * PCOLS, 128)
    small = [
        pltpu.make_async_copy(tok, tok_v.at[0], small_sem.at[0]),
        pltpu.make_async_copy(gain.at[:, pl.ds(mine, HALF)], gain_v.at[0], small_sem.at[1]),
        pltpu.make_async_copy(gain.at[:, pl.ds(theirs, HALF)], gain_v.at[1], small_sem.at[2]),
        pltpu.make_async_copy(dbase.at[:, pl.ds(rec_at, RCOLS)], base_v.at[0], small_sem.at[3]),
        pltpu.make_async_copy(rbase.at[:, pl.ds(rec_at, RCOLS)], base_v.at[1], small_sem.at[4]),
        pltpu.make_async_copy(hgain.at[:, pl.ds(rec_at, RCOLS)], base_v.at[2], small_sem.at[5]),
        pltpu.make_async_copy(mix.at[pl.ds(tp * 2, 2)], mix_v, small_sem.at[6]),
        pltpu.make_async_copy(pscale.at[:, pl.ds(pool_at, PCOLS)], pscale_v, small_sem.at[7]),
        pltpu.make_async_copy(init, init_v, small_sem.at[8]),
        pltpu.make_async_copy(wor, wout_v.at[pl.ds(0, RCOLS)], small_sem.at[9]),
        pltpu.make_async_copy(wop, wout_v.at[pl.ds(RCOLS, PCOLS)], small_sem.at[10]),
    ]
    loads = [
        [
            pltpu.make_async_copy(
                w.at[pl.ds(at, HALF)],
                weight_v.at[half, :, pl.ds(OFFS[i], WIDTHS[i])],
                w_sem.at[half, i],
            )
            for i, w in enumerate(weights)
        ]
        for half, at in ((0, mine), (1, theirs))
    ]
    for copy in small[:3]:
        copy.start()
    for half in loads:
        for copy in half:
            copy.start()
    for copy in small[3:]:
        copy.start()

    def take(half):
        wide = tok_v[half].reshape(TOK, HALF).astype(f32)
        norm_v[half] = (wide * gain_v[half]).astype(bf16)
        return jnp.sum(wide * wide, axis=1, keepdims=True)

    for copy in small[:2]:
        copy.wait()
    squares = take(0)

    def tiles_of(step):
        return (3 * step, 3 if step < 3 else 2)

    for step in range(4):
        for copy in loads[0][2 * step : 2 * step + 2]:
            copy.wait()
        start, count = tiles_of(step)

        @pl.loop(start, start + count)
        def _(tile):
            at = pl.ds(pl.multiple_of(tile * 256, 256), 256)
            acc_v[:, at] = dot(norm_v[0], weight_v[0, :, at])

        if step == 1:
            pl.semaphore_wait(barrier, N_SP)
            send_tok = pltpu.make_async_remote_copy(
                src_ref=tok_v.at[0],
                dst_ref=tok_v.at[1],
                send_sem=tok_send,
                recv_sem=tok_recv,
                device_id={"tp": other},
                device_id_type=MESH,
            )
            send_tok.start()

    send_tok.wait_recv()
    small[2].wait()
    squares = squares + take(1)
    scale = lax.rsqrt(squares * (1.0 / D) + 0.25)
    for step in range(4):
        for copy in loads[1][2 * step : 2 * step + 2]:
            copy.wait()
        start, count = tiles_of(step)

        @pl.loop(start, start + count)
        def _(tile):
            at = pl.ds(pl.multiple_of(tile * 256, 256), 256)
            total = acc_v[:, at] + dot(norm_v[1], weight_v[1, :, at])
            proj_v[:, at] = (total * scale).astype(bf16)

    for b in range(SEQ):
        pool_v[b, 16:, :] = proj_v[b * ROWS : (b + 1) * ROWS, OFFS[6] : OFFS[7]]
    halo = pltpu.make_async_remote_copy(
        src_ref=pool_v.at[:, pl.ds(ROWS, 16), :],
        dst_ref=pool_v.at[:, pl.ds(0, 16), :],
        send_sem=halo_send,
        recv_sem=halo_recv,
        device_id={"sp": lax.rem(sp + 1, N_SP)},
        device_id_type=MESH,
    )

    @pl.when(sp < N_SP - 1)
    def _():
        halo.start()

    @pl.when(sp == 0)
    def _():
        pool_v[:, 0:16, :] = jnp.zeros((SEQ, 16, PCOLS), bf16)

    for copy in small[3:6]:
        copy.wait()
    groups = [(b, p) for b in range(SEQ) for p in range(PAIRS)]

    def part(index, b, p):
        at = OFFS[index] + 128 * p
        return proj_v[b * ROWS : (b + 1) * ROWS, at : at + 128]

    i2, j2 = masks()
    strict = i2 > j2
    inclusive = i2 >= j2
    lowers, ends = [], []
    for g, (b, p) in enumerate(groups):
        lanes = pl.ds(128 * p, 128)
        alpha, rho, beta, kappa, e_mid, e_tail, e_last = prepare(
            part(0, b, p).astype(f32),
            part(1, b, p).astype(f32),
            None,
            part(3, b, p).astype(f32),
            part(4, b, p).astype(f32),
            base_v[0, :, lanes],
            base_v[1, :, lanes],
        )
        pairs = pair_products(alpha, rho, beta, kappa)
        low = jnp.where(strict, pairs[:128, :256], 0.0)
        cross = cat(
            [
                jnp.where(strict, pairs[:128, 256:], 0.0),
                jnp.where(inclusive, pairs[128:, 256:], 0.0),
            ],
            0,
        )
        value = part(2, b, p)
        c_hi, c_lo = split2(cross)
        v2 = two_heads(value)
        mixed = dot(c_hi, v2) + dot(c_lo, v2)
        low_v[g] = low
        within_v[g] = jnp.where(inclusive, pairs[128:, :256], 0.0)
        alpha_v[g, 0] = alpha * e_mid
        alpha_v[g, 1] = mixed[:128]
        rho_v[g] = rho * e_mid
        wval_v[g] = mixed[128:]
        ends.append((beta * e_tail, kappa * e_tail, e_last))
    invs = inverses([low_v[g] for g in range(GROUPS)])
    for g, (b, p) in enumerate(groups):
        z = solve(invs[g], low_v[g], alpha_v[g, 1], alpha_v[g, 0])
        z_v[g] = z
        transit, written = maps_of(z, part(2, b, p), *ends[g])
        map_v[g, 0] = transit
        map_v[g, 1] = written

    map_copies = []
    for g in range(GROUPS):
        owner = 2 * g + tp
        copy = pltpu.make_async_remote_copy(
            src_ref=map_v.at[g],
            dst_ref=maps_in.at[sp],
            send_sem=map_send.at[g],
            recv_sem=map_recv.at[sp],
            device_id={"sp": owner},
            device_id_type=MESH,
        )
        map_copies.append(copy)

        @pl.when((sp != owner) & (sp < N_SP - 1))
        def _():
            copy.start()

        @pl.when(sp == owner)
        def _():
            maps_in[sp] = map_v[g]

    for copy in small[6:]:
        copy.wait()

    @pl.when(sp > 0)
    def _():
        halo.wait_recv()

    places = (sp * ROWS + 1 + lax.broadcasted_iota(jnp.int32, (ROWS, 128), 0)).astype(f32)
    for b in range(SEQ):
        outs = []
        for s in range(2):
            at = slice(128 * s, 128 * s + 128)
            own = pool_v[b, :, at].astype(f32)
            total = own + pltpu.roll(own, 1, 0)
            if s == 1:
                total = total + pltpu.roll(total, 2, 0)
            wide = total + pltpu.roll(total, 2 if s == 0 else 4, 0)
            wide = wide + pltpu.roll(wide, 4 if s == 0 else 8, 0)
            trail = jnp.where(tp == 0, total, wide)[16:]
            window = jnp.where(tp == 0, float(2 << s), float(8 << s))
            diff = (trail / jnp.minimum(places, window) - own[16:]).astype(bf16)
            pooled = dot(diff, mix_v[s])
            gate = proj_v[b * ROWS : (b + 1) * ROWS, OFFS[7] + 128 * s : OFFS[7] + 128 * s + 128]
            gate = gate.astype(f32)
            outs.append((pooled * pscale_v[:, at] * (gate * sig(gate))).astype(bf16))
        recout_v[b * ROWS : (b + 1) * ROWS, RCOLS:] = cat(outs, 1)

    @pl.loop(0, 8)
    def _(tile):
        at = pl.ds(pl.multiple_of(tile * 256, 256), 256)
        merged_v[:, at] = dot(recout_v[:, RCOLS:], wout_v[RCOLS:, at])

    def send_state(j):
        return pltpu.make_async_remote_copy(
            src_ref=state_v.at[j],
            dst_ref=states_in.at[group_of],
            send_sem=st_send.at[j],
            recv_sem=st_recv.at[group_of],
            device_id={"sp": j},
            device_id_type=MESH,
        )

    def wait_map(j):
        pltpu.make_async_remote_copy(
            src_ref=map_v.at[0],
            dst_ref=maps_in.at[j],
            send_sem=map_send.at[0],
            recv_sem=map_recv.at[j],
            device_id={"sp": j},
            device_id_type=MESH,
        ).wait_recv()

    @pl.when(is_owner)
    def _():
        seq = lax.div(group_of, PAIRS)
        pair = lax.rem(group_of, PAIRS)
        state0 = cat([init_v[seq, 2 * pair], init_v[seq, 2 * pair + 1]], 1)

        def emit(j, state):
            state_v[j] = state.astype(bf16)

            @pl.when(j != sp)
            def _():
                send_state(j).start()

            @pl.when(j == sp)
            def _():
                states_in[group_of] = state.astype(bf16)

        def body(j, state):
            emit(j, state)

            @pl.when(j != sp)
            def _():
                wait_map(j)

            return advance(state, maps_in[j, 0], maps_in[j, 1])

        emit(N_SP - 1, lax.fori_loop(0, N_SP - 1, body, state0))

    for g in range(GROUPS):
        reads, local = reads_of(
            within_v[g], z_v[g], rho_v[g], wval_v[g]
        )
        reads_v[g] = reads
        local_v[g] = local

    for g, (b, p) in enumerate(groups):
        owner = 2 * g + tp

        @pl.when(sp != owner)
        def _():
            pltpu.make_async_remote_copy(
                src_ref=state_v.at[0],
                dst_ref=states_in.at[g],
                send_sem=st_send.at[0],
                recv_sem=st_recv.at[g],
                device_id={"sp": owner},
                device_id_type=MESH,
            ).wait_recv()

        rec = recurrent_of(reads_v[g], states_in[g], local_v[g])
        lanes = pl.ds(128 * p, 128)
        recout_v[b * ROWS : (b + 1) * ROWS, 128 * p : 128 * p + 128] = head_norm(
            rec, base_v[2, :, lanes], part(5, b, p).astype(f32)
        )

    def product(at):
        return (merged_v[:, at] + dot(recout_v[:, :RCOLS], wout_v[:RCOLS, at])).astype(bf16)

    def send_part(tile):
        return pltpu.make_async_remote_copy(
            src_ref=part_v.at[tile],
            dst_ref=part_in.at[tile],
            send_sem=part_send.at[tile],
            recv_sem=part_recv.at[tile],
            device_id={"tp": other},
            device_id_type=MESH,
        )

    def store_out(tile):
        at = pl.ds(pl.multiple_of(tile * 256, 256), 256)
        return pltpu.make_async_copy(out_v.at[:, :, at], out.at[:, :, at], out_sem.at[tile])

    @pl.loop(0, 4)
    def _(tile):
        at = pl.ds(pl.multiple_of(theirs + tile * 256, 256), 256)
        part_v[tile] = product(at)
        send_part(tile).start()

    @pl.loop(0, 4)
    def _(tile):
        at = pl.ds(pl.multiple_of(mine + tile * 256, 256), 256)
        own = product(at).astype(f32)
        send_part(tile).wait_recv()
        total = (own + part_in[tile].astype(f32)).astype(bf16)
        out_v[:, :, pl.ds(pl.multiple_of(tile * 256, 256), 256)] = total.reshape(SEQ, ROWS, 256)
        store_out(tile).start()

    send_tok.wait_send()

    @pl.when(sp < N_SP - 1)
    def _():
        halo.wait_send()

    for g, copy in enumerate(map_copies):
        @pl.when((sp != 2 * g + tp) & (sp < N_SP - 1))
        def _():
            copy.wait_send()

    @pl.when(is_owner)
    def _():
        @pl.loop(0, N_SP)
        def _(j):
            @pl.when(j != sp)
            def _():
                send_state(j).wait_send()

    @pl.loop(0, 4)
    def _(tile):
        send_part(tile).wait_send()
        store_out(tile).wait()


def shards(
    tokens, norm_gain, w_recept, w_key, w_value, w_decay, w_rate, w_gate_rec, w_pool, w_gate_pool,
    decay_base, rate_base, head_gain, pool_mix, pool_scale, w_out_rec, w_out_pool, init_state,
):
    vmem, sem = pltpu.VMEM, pltpu.SemaphoreType.DMA
    row = lambda x: x.reshape(1, -1)
    scratch = [
        vmem((2, SEQ, ROWS, HALF), bf16),
        vmem((2, 1, HALF), f32),
        vmem((2, HALF, COLS), bf16),
        vmem((TOK, COLS), f32),
        vmem((TOK, COLS), bf16),
        vmem((2, TOK, HALF), bf16),
        vmem((3, 1, RCOLS), f32),
        vmem((2, 128, 128), bf16),
        vmem((1, PCOLS), f32),
        vmem((RCOLS + PCOLS, D), bf16),
        vmem((SEQ, 2 * PAIRS, HD, HD), f32),
        vmem((SEQ, 16 + ROWS, PCOLS), bf16),
        vmem((GROUPS, 2, 128, 128), f32),
        vmem((GROUPS, 128, 256), f32),
        vmem((GROUPS, 128, 256), f32),
        vmem((GROUPS, 128, 128), f32),
        vmem((GROUPS, 128, 128), f32),
        vmem((GROUPS, 128, 256), f32),
        vmem((GROUPS, 128, 128), f32),
        vmem((GROUPS, 128, 128), f32),
        vmem((GROUPS, 2, HD, 128), bf16),
        vmem((N_SP, 2, HD, 128), bf16),
        vmem((N_SP, HD, 128), bf16),
        vmem((GROUPS, HD, 128), bf16),
        vmem((TOK, D), f32),
        vmem((TOK, RCOLS + PCOLS), bf16),
        vmem((4, TOK, 256), bf16),
        vmem((4, TOK, 256), bf16),
        vmem((SEQ, ROWS, HALF), bf16),
        sem((2, 8)),
        sem((11,)),
        sem,
        sem,
        sem,
        sem,
        sem((GROUPS,)),
        sem((N_SP,)),
        sem((N_SP,)),
        sem((GROUPS,)),
        sem((4,)),
        sem((4,)),
        sem((4,)),
    ]
    return pl.pallas_call(
        kernel,
        out_shape=jax.ShapeDtypeStruct((SEQ, ROWS, HALF), bf16),
        in_specs=[pl.BlockSpec(memory_space=pl.ANY)] * 18,
        out_specs=pl.BlockSpec(memory_space=pl.ANY),
        scratch_shapes=scratch,
        compiler_params=pltpu.CompilerParams(
            collective_id=0, has_side_effects=True, vmem_limit_bytes=56 << 20
        ),
        name="layer",
    )(
        tokens, row(norm_gain), w_recept, w_key, w_value, w_decay, w_rate, w_gate_rec, w_pool,
        w_gate_pool, row(decay_base), row(rate_base), row(head_gain), pool_mix, row(pool_scale),
        w_out_rec, w_out_pool, init_state,
    )


def solution(mesh):
    split = P(None, "tp")
    placed = (
        P("fs", "sp", "tp"), P(),
        split, split, split, split, split, split, split, split,
        P(), P(), P(), P(), P(),
        P("tp", None), P("tp", None), P("fs", "tp", None, None),
    )
    return jax.shard_map(
        shards, mesh=mesh, in_specs=placed, out_specs=P("fs", "sp", "tp"), check_vma=False
    )
```

```python
import math

import jax
import jax.numpy as jnp
from jax import lax
from jax.experimental import pallas as pl
from jax.experimental.pallas import tpu as pltpu
from jax.sharding import PartitionSpec as P

D = 2048
HALF = 1024
SEQ = 2
ROWS = 128
TOK = SEQ * ROWS
RCOLS = 384
PCOLS = 256
PAIRS = 3
GROUPS = SEQ * PAIRS
HD = 64
N_SP = 16
COLS = 6 * RCOLS + 2 * PCOLS
OFFS = (0, 384, 768, 1152, 1536, 1920, 2304, 2560)
WIDTHS = (384, 384, 384, 384, 384, 384, 256, 256)
MESH = pl.DeviceIdType.MESH
f32 = jnp.float32
bf16 = jnp.bfloat16


def dot(a, b):
    return lax.dot_general(a, b, (((1,), (0,)), ((), ())), preferred_element_type=f32)


def dot_nt(a, b):
    return lax.dot_general(a, b, (((1,), (1,)), ((), ())), preferred_element_type=f32)


def dot_tn(a, b):
    return lax.dot_general(a, b, (((0,), (0,)), ((), ())), preferred_element_type=f32)


def split2(x):
    hi = x.astype(bf16)
    return hi, (x - hi.astype(f32)).astype(bf16)


def cat(parts, axis):
    return jnp.concatenate(parts, axis=axis)


def sig(x):
    e = jnp.exp(-jnp.abs(x))
    return jnp.where(x >= 0, 1.0, e) / (1.0 + e)


def lane_first(shape):
    return lax.broadcasted_iota(jnp.int32, shape, len(shape) - 1) < HD


def keep(x, head):
    first = lane_first(x.shape)
    zero = jnp.zeros_like(x)
    return jnp.where(first, x, zero) if head == 0 else jnp.where(first, zero, x)


def two_heads(x):
    return cat([keep(x, 0), keep(x, 1)], 0)


def block_ones():
    i = lax.broadcasted_iota(jnp.int32, (128, 128), 0) < HD
    j = lax.broadcasted_iota(jnp.int32, (128, 128), 1) < HD
    return jnp.where(i == j, 1.0, 0.0).astype(bf16)


def head_sums(x, ones2):
    hi, lo = split2(x)
    return dot(cat([hi, lo], 1), ones2)


def prepare(r, k, d_in, a_in, d_base, a_base):
    ones = block_ones()
    ones2 = cat([ones, ones], 0)
    x = d_base + d_in
    log_decay = -math.exp(-0.5) * sig(x)
    rate = sig(a_base + a_in)
    squares = k * k
    sums = cat([head_sums(squares[:, o : o + 128], ones2) for o in range(0, RCOLS, 128)], 1)
    unit = k * lax.rsqrt(sums + 1.0)
    removal = unit * rate
    i = lax.broadcasted_iota(jnp.int32, (128, 128), 0)
    j = lax.broadcasted_iota(jnp.int32, (128, 128), 1)
    tri = jnp.where(i >= j, 1.0, 0.0).astype(bf16)
    hi, lo = split2(log_decay)
    rest = (log_decay - hi.astype(f32) - lo.astype(f32)).astype(bf16)
    cum = dot(cat([tri, tri, tri], 1), cat([hi, lo, rest], 0))
    mid = cum[63:64, :]
    last = cum[127:128, :]
    shrink = jnp.exp(cum - mid)
    grow = jnp.exp(mid - cum)
    alpha = jnp.exp(cum - log_decay - mid) * unit
    rho = r * shrink
    beta = removal * grow
    kappa = k * grow
    return alpha, rho, beta, kappa, jnp.exp(mid), jnp.exp(last - mid), jnp.exp(last)


def pair_products(x, beta, kappa):
    x_hi, x_lo = split2(x)
    b_hi, b_lo = split2(beta)
    k_hi, k_lo = split2(kappa)
    y_hi = cat([two_heads(b_hi), two_heads(k_hi)], 0)
    y_lo = cat([two_heads(b_lo), two_heads(k_lo)], 0)
    return dot_nt(cat([x_hi, x_lo], 1), cat([y_hi, y_hi], 1)) + dot_nt(x_hi, y_lo)


def block_diag(x):
    a, b = x[:, :128], x[:, 128:]
    zero = jnp.zeros_like(a)
    return cat([cat([a, zero], 1), cat([zero, b], 1)], 0)


def masks():
    i = lax.broadcasted_iota(jnp.int32, (128, 256), 0)
    j = lax.broadcasted_iota(jnp.int32, (128, 256), 1) & 127
    return i, j


def inverses(lowers):
    i, j = masks()
    apart = i ^ j
    eye = jnp.where(i == j, 1.0, 0.0)
    zero = jnp.zeros((128, 256), bf16)
    inv = [eye - jnp.where(apart == 1, low, zero).astype(f32) for low in lowers]
    for size in (2, 8, 32):
        inside = (apart >= size) & (apart < 4 * size)
        inv_b = [block_diag(x.astype(bf16)) for x in inv]
        steps = [block_diag(jnp.where(inside, low, zero)) for low in lowers]
        hop = [dot(x.astype(bf16), c).astype(bf16) for x, c in zip(inv, steps)]
        twice = [dot(h, block_diag(h)).astype(bf16) for h in hop]
        once = [x - dot(h, b) for x, h, b in zip(inv, hop, inv_b)]
        inv = [x + dot(t, block_diag(x.astype(bf16))) for x, t in zip(once, twice)]
    return [x.astype(bf16) for x in inv]


def stacked(x):
    left, right = x[:, :128], x[:, 128:]
    return cat([cat([keep(left, h), keep(right, h)], 1) for h in (0, 1)], 0)


def solve_all(invs, lows, sides):
    first = [dot(inv, stacked(side.astype(bf16))).astype(bf16) for inv, side in zip(invs, sides)]
    back = [dot(low, stacked(x)) for low, x in zip(lows, first)]
    miss = [
        (side - x.astype(f32) - y).astype(bf16) for side, x, y in zip(sides, first, back)
    ]
    return [x.astype(f32) + dot(inv, stacked(m)) for x, inv, m in zip(first, invs, miss)]


def maps_of(z, value, beta_end, kappa_end, gain_end):
    zero = jnp.zeros((128, 128), bf16)
    lhs = cat([z.astype(bf16), cat([zero, -value], 1)], 0)
    both = dot_tn(lhs, cat([beta_end, kappa_end], 0).astype(bf16))
    first = lane_first((64, 128))
    packed = [
        jnp.where(first, both[o : o + 64], both[o + 64 : o + 128]) for o in (0, 128)
    ]
    i = lax.broadcasted_iota(jnp.int32, (64, 128), 0)
    j = lax.broadcasted_iota(jnp.int32, (64, 128), 1) & 63
    transit = jnp.where(i == j, gain_end, 0.0) - packed[0]
    return transit.astype(bf16), (-packed[1]).astype(bf16)


def after(left, transit, written):
    l_hi, l_lo = split2(left)
    t_hi, t_lo = split2(transit)
    weights = two_heads(t_hi)
    moved = dot(cat([l_hi, l_lo], 1), cat([weights, weights], 0)) + dot(l_hi, two_heads(t_lo))
    return moved + written


def after_given(left, transit):
    hi, lo = split2(left)
    weights = two_heads(transit)
    return dot(cat([hi, lo], 1), cat([weights, weights], 0))


def recurrent_of(reads, state, local):
    hi, lo = split2(reads)
    weights = two_heads(state)
    return dot_nt(cat([hi, lo], 1), cat([weights, weights], 1)) + local


def head_norm(rec, gain, gate):
    ones = block_ones()
    ones2 = cat([ones, ones], 0)
    offs = range(0, RCOLS, 128)
    total = cat([head_sums(rec[:, o : o + 128], ones2) for o in offs], 1)
    centred = rec - total * (1.0 / HD)
    squares = centred * centred
    spread = cat([head_sums(squares[:, o : o + 128], ones2) for o in offs], 1) * (1.0 / HD)
    return (centred * lax.rsqrt(spread + 1.0) * gain * gate * sig(gate)).astype(bf16)


def kernel(
    tok, gain, wr, wk, wv, wd, wa, wg, wp, wgp, dbase, rbase, hgain, mix, pscale, wor, wop, init,
    out,
    tok_v, gain_v, weight_v, acc_v, proj_v, norm_v, base_v, mix_v, pscale_v, wout_v, init_v,
    pool_v, keys_v, low_v, side_v, z_v, reads_v, local_v, map_v, maps_in,
    state_v, states_in, merged_v, recout_v, part_v, part_in, part_own, out_v,
    w_sem, small_sem, tok_send, tok_recv, halo_send, halo_recv, map_send, map_recv,
    st_send, st_recv, part_send, part_recv, out_sem,
):
    sp = lax.axis_index("sp")
    tp = lax.axis_index("tp")
    other = 1 - tp
    weights = (wr, wk, wv, wd, wa, wg, wp, wgp)
    group_of = lax.div(sp, 2)
    is_owner = (lax.rem(sp, 2) == tp) & (sp < 2 * GROUPS)

    barrier = pltpu.get_barrier_semaphore()
    pl.semaphore_signal(barrier, inc=1, device_id={"tp": other}, device_id_type=MESH)

    @pl.loop(1, N_SP)
    def _(step):
        pl.semaphore_signal(
            barrier, inc=1, device_id={"sp": lax.rem(sp + step, N_SP)}, device_id_type=MESH
        )

    mine = pl.multiple_of(tp * HALF, HALF)
    theirs = pl.multiple_of(other * HALF, HALF)
    pool_at = pl.multiple_of(tp * PCOLS, 128)
    small = [
        pltpu.make_async_copy(tok, tok_v.at[0], small_sem.at[0]),
        pltpu.make_async_copy(gain.at[:, pl.ds(mine, HALF)], gain_v.at[0], small_sem.at[1]),
        pltpu.make_async_copy(gain.at[:, pl.ds(theirs, HALF)], gain_v.at[1], small_sem.at[2]),
        pltpu.make_async_copy(dbase, base_v.at[0], small_sem.at[3]),
        pltpu.make_async_copy(rbase, base_v.at[1], small_sem.at[4]),
        pltpu.make_async_copy(hgain, base_v.at[2], small_sem.at[5]),
        pltpu.make_async_copy(mix.at[pl.ds(tp * 2, 2)], mix_v, small_sem.at[6]),
        pltpu.make_async_copy(pscale.at[:, pl.ds(pool_at, PCOLS)], pscale_v, small_sem.at[7]),
        pltpu.make_async_copy(init, init_v, small_sem.at[8]),
        pltpu.make_async_copy(wor, wout_v.at[pl.ds(0, RCOLS)], small_sem.at[9]),
        pltpu.make_async_copy(wop, wout_v.at[pl.ds(RCOLS, PCOLS)], small_sem.at[10]),
    ]
    loads = [
        [
            pltpu.make_async_copy(
                w.at[pl.ds(at, HALF)],
                weight_v.at[half, :, pl.ds(OFFS[i], WIDTHS[i])],
                w_sem.at[half, i],
            )
            for i, w in enumerate(weights)
        ]
        for half, at in ((0, mine), (1, theirs))
    ]
    def start(copies):
        for copy in copies:
            copy.start()

    start(small[:3])
    start(loads[0][:4])

    def take(half):
        wide = tok_v[half].reshape(TOK, HALF).astype(f32)
        norm_v[half] = (wide * gain_v[half]).astype(bf16)
        return jnp.sum(wide * wide, axis=1, keepdims=True)

    for copy in small[:2]:
        copy.wait()
    start(loads[0][4:] + loads[1][:2])
    squares = take(0)

    def columns(step):
        return slice(768 * step, min(768 * step + 768, COLS))

    for step in range(4):
        for copy in loads[0][2 * step : 2 * step + 2]:
            copy.wait()
        at = columns(step)
        acc_v[:, at] = dot(norm_v[0], weight_v[0, :, at])
        start((loads[1][2:4], loads[1][4:], small[3:], [])[step])
        if step == 0:
            pl.semaphore_wait(barrier, N_SP)
            send_tok = pltpu.make_async_remote_copy(
                src_ref=tok_v.at[0],
                dst_ref=tok_v.at[1],
                send_sem=tok_send,
                recv_sem=tok_recv,
                device_id={"tp": other},
                device_id_type=MESH,
            )
            send_tok.start()

    send_tok.wait_recv()
    small[2].wait()
    squares = squares + take(1)
    scale = lax.rsqrt(squares * (1.0 / D) + 0.25)
    for step in range(4):
        for copy in loads[1][2 * step : 2 * step + 2]:
            copy.wait()
        at = columns(step)
        total = acc_v[:, at] + dot(norm_v[1], weight_v[1, :, at])
        proj_v[:, at] = (total * scale).astype(bf16)

    for b in range(SEQ):
        pool_v[b, 16:, :] = proj_v[b * ROWS : (b + 1) * ROWS, OFFS[6] : OFFS[7]]
    halo = pltpu.make_async_remote_copy(
        src_ref=pool_v.at[:, pl.ds(ROWS, 16), :],
        dst_ref=pool_v.at[:, pl.ds(0, 16), :],
        send_sem=halo_send,
        recv_sem=halo_recv,
        device_id={"sp": lax.rem(sp + 1, N_SP)},
        device_id_type=MESH,
    )

    @pl.when(sp < N_SP - 1)
    def _():
        halo.start()

    @pl.when(sp == 0)
    def _():
        pool_v[:, 0:16, :] = jnp.zeros((SEQ, 16, PCOLS), bf16)

    for copy in small[3:6]:
        copy.wait()
    groups = [(b, p) for b in range(SEQ) for p in range(PAIRS)]

    def part(index, b, p):
        at = OFFS[index] + 128 * p
        return proj_v[b * ROWS : (b + 1) * ROWS, at : at + 128]

    i2, j2 = masks()
    strict = i2 > j2
    inclusive = i2 >= j2

    def rows_of(index, b):
        at = OFFS[index]
        return proj_v[b * ROWS : (b + 1) * ROWS, at : at + WIDTHS[index]].astype(f32)

    def local_row(index):
        return cat([base_v[index, pl.ds(3 * tp + p, 1), :] for p in range(PAIRS)], 1)

    ends = []
    for b in range(SEQ):
        alpha, rho, beta, kappa, e_mid, e_tail, e_last = prepare(
            rows_of(0, b), rows_of(1, b), rows_of(3, b), rows_of(4, b), local_row(0), local_row(1)
        )
        keys_v[b, 0] = alpha
        keys_v[b, 1] = rho
        keys_v[b, 2] = beta
        keys_v[b, 3] = kappa
        ends.append((e_mid, e_tail, e_last))

    def pair_of(index, g):
        b, p = groups[g]
        return keys_v[b, index, :, 128 * p : 128 * p + 128]

    def end_of(index, g):
        b, p = groups[g]
        return ends[b][index][:, 128 * p : 128 * p + 128]

    every = range(GROUPS)
    for g in every:
        pairs = pair_products(pair_of(0, g), pair_of(2, g), pair_of(3, g))
        low_v[g] = jnp.where(strict, pairs[:, :256], 0.0).astype(bf16)
        cross = jnp.where(strict, pairs[:, 256:], 0.0).astype(bf16)
        side_v[g, :, :128] = pair_of(0, g) * end_of(0, g)
        side_v[g, :, 128:] = dot(cross, two_heads(part(2, *groups[g])))
    invs = inverses([low_v[g] for g in every])
    map_copies = []
    for some in (range(0, 3), range(3, 6)):
        solved = solve_all(
            [invs[g] for g in some], [low_v[g] for g in some], [side_v[g] for g in some]
        )
        for g, z in zip(some, solved):
            z_v[g] = z.astype(bf16)
            tail = end_of(1, g)
            transit, written = maps_of(
                z, part(2, *groups[g]), pair_of(2, g) * tail, pair_of(3, g) * tail, end_of(2, g)
            )
            map_v[g, 0] = transit
            map_v[g, 1] = written
        for g in some:
            owner = 2 * g + tp
            copy = pltpu.make_async_remote_copy(
                src_ref=map_v.at[g],
                dst_ref=maps_in.at[sp],
                send_sem=map_send.at[g],
                recv_sem=map_recv.at[sp],
                device_id={"sp": owner},
                device_id_type=MESH,
            )
            map_copies.append(copy)

            @pl.when((sp != owner) & (sp < N_SP - 1))
            def _():
                copy.start()

            @pl.when(sp == owner)
            def _():
                pltpu.make_async_copy(map_v.at[g], maps_in.at[sp], map_recv.at[sp]).start()

    for copy in small[6:]:
        copy.wait()

    @pl.when(sp > 0)
    def _():
        halo.wait_recv()

    places = (sp * ROWS + 1 + lax.broadcasted_iota(jnp.int32, (ROWS, 128), 0)).astype(f32)
    for b in range(SEQ):
        outs = []
        for s in range(2):
            at = slice(128 * s, 128 * s + 128)
            own = pool_v[b, :, at].astype(f32)
            total = own + pltpu.roll(own, 1, 0)
            if s == 1:
                total = total + pltpu.roll(total, 2, 0)
            wide = total + pltpu.roll(total, 2 if s == 0 else 4, 0)
            wide = wide + pltpu.roll(wide, 4 if s == 0 else 8, 0)
            trail = jnp.where(tp == 0, total, wide)[16:]
            window = jnp.where(tp == 0, float(2 << s), float(8 << s))
            diff = (trail / jnp.minimum(places, window) - own[16:]).astype(bf16)
            pooled = dot(diff, mix_v[s])
            gate = proj_v[b * ROWS : (b + 1) * ROWS, OFFS[7] + 128 * s : OFFS[7] + 128 * s + 128]
            gate = gate.astype(f32)
            outs.append((pooled * pscale_v[:, at] * (gate * sig(gate))).astype(bf16))
        recout_v[b * ROWS : (b + 1) * ROWS, RCOLS:] = cat(outs, 1)

    for at in (slice(0, 1024), slice(1024, D)):
        merged_v[:, at] = dot(recout_v[:, RCOLS:], wout_v[RCOLS:, at])

    def send_state(j):
        return pltpu.make_async_remote_copy(
            src_ref=state_v.at[j],
            dst_ref=states_in.at[group_of],
            send_sem=st_send.at[j],
            recv_sem=st_recv.at[group_of],
            device_id={"sp": j},
            device_id_type=MESH,
        )

    def wait_map(j):
        pltpu.make_async_copy(map_v.at[0], maps_in.at[j], map_recv.at[j]).wait()

    @pl.when(is_owner)
    def _():
        seq = lax.div(group_of, PAIRS)
        pair = lax.rem(group_of, PAIRS)
        state = cat([init_v[seq, 2 * pair], init_v[seq, 2 * pair + 1]], 1)
        for j in range(N_SP - 1):
            wait_map(j)
        zero = jnp.zeros((HD, 128), f32)
        prefixes = []
        for block in range(4):
            held = [cat([maps_in[4 * block, 0], maps_in[4 * block, 1]], 0).astype(f32)]
            prefixes.append(held)
        for y in (1, 2, 3):
            for block in range(4):
                j = 4 * block + y
                if j < N_SP - 1:
                    held = prefixes[block]
                    moved = after_given(held[-1], maps_in[j, 0])
                    held.append(moved + cat([zero, maps_in[j, 1].astype(f32)], 0))
        for block in range(4):
            held = prefixes[block]
            state_v[4 * block] = state.astype(bf16)
            for y in (1, 2, 3):
                inside = held[y - 1]
                state_v[4 * block + y] = after(state, inside[:HD], inside[HD:]).astype(bf16)
            if block < 3:
                state = after(state, held[3][:HD], held[3][HD:])

        @pl.loop(0, N_SP)
        def _(j):
            @pl.when(j != sp)
            def _():
                send_state(j).start()

            @pl.when(j == sp)
            def _():
                pltpu.make_async_copy(
                    state_v.at[j], states_in.at[group_of], st_recv.at[group_of]
                ).start()

    for g in every:
        pairs = pair_products(pair_of(1, g), pair_of(2, g), pair_of(3, g))
        within_beta = jnp.where(inclusive, pairs[:, :256], 0.0).astype(bf16)
        within_kappa = jnp.where(inclusive, pairs[:, 256:], 0.0).astype(bf16)
        drop = dot(within_beta, stacked(z_v[g]))
        reads_v[g] = pair_of(1, g) * end_of(0, g) - drop[:, :128]
        local_v[g] = dot(within_kappa, two_heads(part(2, *groups[g]))) - drop[:, 128:]

    for b in range(SEQ):
        recs = []
        for g in range(PAIRS * b, PAIRS * b + PAIRS):
            pltpu.make_async_copy(state_v.at[0], states_in.at[g], st_recv.at[g]).wait()
            recs.append(recurrent_of(reads_v[g], states_in[g], local_v[g]))
        recout_v[b * ROWS : (b + 1) * ROWS, :RCOLS] = head_norm(
            cat(recs, 1), local_row(2), rows_of(5, b)
        )

    def product(at):
        return (merged_v[:, at] + dot(recout_v[:, :RCOLS], wout_v[:RCOLS, at])).astype(bf16)

    def send_part(tile):
        return pltpu.make_async_remote_copy(
            src_ref=part_v.at[tile],
            dst_ref=part_in.at[tile],
            send_sem=part_send.at[tile],
            recv_sem=part_recv.at[tile],
            device_id={"tp": other},
            device_id_type=MESH,
        )

    def store_out(tile):
        at = pl.ds(512 * tile, 512)
        return pltpu.make_async_copy(out_v.at[:, :, at], out.at[:, :, at], out_sem.at[tile])

    for tile in range(2):
        part_v[tile] = product(pl.ds(pl.multiple_of(theirs + tile * 512, 512), 512))
        send_part(tile).start()
    for tile in range(2):
        part_own[tile] = product(pl.ds(pl.multiple_of(mine + tile * 512, 512), 512))
    for tile in range(2):
        send_part(tile).wait_recv()
        total = part_own[tile].astype(f32) + part_in[tile].astype(f32)
        out_v[:, :, 512 * tile : 512 * tile + 512] = total.astype(bf16).reshape(SEQ, ROWS, 512)
        store_out(tile).start()

    send_tok.wait_send()

    @pl.when(sp < N_SP - 1)
    def _():
        halo.wait_send()

    for g, copy in enumerate(map_copies):
        @pl.when((sp != 2 * g + tp) & (sp < N_SP - 1))
        def _():
            copy.wait_send()

    @pl.when(is_owner)
    def _():
        @pl.loop(0, N_SP)
        def _(j):
            @pl.when(j != sp)
            def _():
                send_state(j).wait_send()

    for tile in range(2):
        send_part(tile).wait_send()
        store_out(tile).wait()


def shards(
    tokens, norm_gain, w_recept, w_key, w_value, w_decay, w_rate, w_gate_rec, w_pool, w_gate_pool,
    decay_base, rate_base, head_gain, pool_mix, pool_scale, w_out_rec, w_out_pool, init_state,
):
    vmem, sem = pltpu.VMEM, pltpu.SemaphoreType.DMA
    row = lambda x: x.reshape(1, -1)
    tile = lambda x: x.reshape(6, 128)
    scratch = [
        vmem((2, SEQ, ROWS, HALF), bf16),
        vmem((2, 1, HALF), f32),
        vmem((2, HALF, COLS), bf16),
        vmem((TOK, COLS), f32),
        vmem((TOK, COLS), bf16),
        vmem((2, TOK, HALF), bf16),
        vmem((3, 6, 128), f32),
        vmem((2, 128, 128), bf16),
        vmem((1, PCOLS), f32),
        vmem((RCOLS + PCOLS, D), bf16),
        vmem((SEQ, 2 * PAIRS, HD, HD), f32),
        vmem((SEQ, 16 + ROWS, PCOLS), bf16),
        vmem((SEQ, 4, ROWS, RCOLS), f32),
        vmem((GROUPS, 128, 256), bf16),
        vmem((GROUPS, 128, 256), f32),
        vmem((GROUPS, 128, 256), bf16),
        vmem((GROUPS, 128, 128), f32),
        vmem((GROUPS, 128, 128), f32),
        vmem((GROUPS, 2, HD, 128), bf16),
        vmem((N_SP, 2, HD, 128), bf16),
        vmem((N_SP, HD, 128), bf16),
        vmem((GROUPS, HD, 128), bf16),
        vmem((TOK, D), f32),
        vmem((TOK, RCOLS + PCOLS), bf16),
        vmem((2, TOK, 512), bf16),
        vmem((2, TOK, 512), bf16),
        vmem((2, TOK, 512), bf16),
        vmem((SEQ, ROWS, HALF), bf16),
        sem((2, 8)),
        sem((11,)),
        sem,
        sem,
        sem,
        sem,
        sem((GROUPS,)),
        sem((N_SP,)),
        sem((N_SP,)),
        sem((GROUPS,)),
        sem((2,)),
        sem((2,)),
        sem((2,)),
    ]
    return pl.pallas_call(
        kernel,
        out_shape=jax.ShapeDtypeStruct((SEQ, ROWS, HALF), bf16),
        in_specs=[pl.BlockSpec(memory_space=pl.ANY)] * 18,
        out_specs=pl.BlockSpec(memory_space=pl.ANY),
        scratch_shapes=scratch,
        compiler_params=pltpu.CompilerParams(
            collective_id=0, has_side_effects=True, vmem_limit_bytes=56 << 20
        ),
        name="layer",
    )(
        tokens, row(norm_gain), w_recept, w_key, w_value, w_decay, w_rate, w_gate_rec, w_pool,
        w_gate_pool, tile(decay_base), tile(rate_base), tile(head_gain), pool_mix, row(pool_scale),
        w_out_rec, w_out_pool, init_state,
    )


def solution(mesh):
    split = P(None, "tp")
    placed = (
        P("fs", "sp", "tp"), P(),
        split, split, split, split, split, split, split, split,
        P(), P(), P(), P(), P(),
        P("tp", None), P("tp", None), P("fs", "tp", None, None),
    )
    return jax.shard_map(
        shards, mesh=mesh, in_specs=placed, out_specs=P("fs", "sp", "tp"), check_vma=False
    )
```

```python
import math

import jax
import jax.numpy as jnp
from jax import lax
from jax.experimental import pallas as pl
from jax.experimental.pallas import tpu as pltpu
from jax.sharding import PartitionSpec as P

D = 2048
HALF = 1024
SEQ = 2
ROWS = 128
TOK = SEQ * ROWS
RCOLS = 384
PCOLS = 256
PAIRS = 3
GROUPS = SEQ * PAIRS
HD = 64
N_SP = 16
COLS = 6 * RCOLS + 2 * PCOLS
OFFS = (1536, 0, 1152, 384, 768, 1920, 2304, 2560)
NEED = (1, 3, 4, 2, 0, 5, 6, 7)
EARLY = 4 * RCOLS
WIDTHS = (384, 384, 384, 384, 384, 384, 256, 256)
MESH = pl.DeviceIdType.MESH
f32 = jnp.float32
bf16 = jnp.bfloat16


def dot(a, b):
    return lax.dot_general(a, b, (((1,), (0,)), ((), ())), preferred_element_type=f32)


def dot_nt(a, b):
    return lax.dot_general(a, b, (((1,), (1,)), ((), ())), preferred_element_type=f32)


def dot_tn(a, b):
    return lax.dot_general(a, b, (((0,), (0,)), ((), ())), preferred_element_type=f32)


def split2(x):
    hi = x.astype(bf16)
    return hi, (x - hi.astype(f32)).astype(bf16)


def cat(parts, axis):
    return jnp.concatenate(parts, axis=axis)


def sig(x):
    e = jnp.exp(-jnp.abs(x))
    return jnp.where(x >= 0, 1.0, e) / (1.0 + e)


def lane_first(shape):
    return lax.broadcasted_iota(jnp.int32, shape, len(shape) - 1) < HD


def keep(x, head):
    first = lane_first(x.shape)
    zero = jnp.zeros_like(x)
    return jnp.where(first, x, zero) if head == 0 else jnp.where(first, zero, x)


def two_heads(x):
    return cat([keep(x, 0), keep(x, 1)], 0)


def block_ones():
    i = lax.broadcasted_iota(jnp.int32, (128, 128), 0) < HD
    j = lax.broadcasted_iota(jnp.int32, (128, 128), 1) < HD
    return jnp.where(i == j, 1.0, 0.0).astype(bf16)


def head_sums(x, ones2):
    hi, lo = split2(x)
    return dot(cat([hi, lo], 1), ones2)


def prepare(k, d_in, a_in, d_base, a_base):
    ones = block_ones()
    ones2 = cat([ones, ones], 0)
    x = d_base + d_in
    log_decay = -math.exp(-0.5) * sig(x)
    rate = sig(a_base + a_in)
    squares = k * k
    sums = cat([head_sums(squares[:, o : o + 128], ones2) for o in range(0, RCOLS, 128)], 1)
    unit = k * lax.rsqrt(sums + 1.0)
    removal = unit * rate
    i = lax.broadcasted_iota(jnp.int32, (128, 128), 0)
    j = lax.broadcasted_iota(jnp.int32, (128, 128), 1)
    tri = jnp.where(i >= j, 1.0, 0.0).astype(bf16)
    hi, lo = split2(log_decay)
    rest = (log_decay - hi.astype(f32) - lo.astype(f32)).astype(bf16)
    cum = dot(cat([tri, tri, tri], 1), cat([hi, lo, rest], 0))
    mid = cum[63:64, :]
    last = cum[127:128, :]
    shrink = jnp.exp(cum - mid)
    grow = jnp.exp(mid - cum)
    alpha = jnp.exp(cum - log_decay - mid) * unit
    beta = removal * grow
    kappa = k * grow
    return alpha, shrink, beta, kappa, jnp.exp(mid), jnp.exp(last - mid), jnp.exp(last)


def pair_products(x, y_hi, y_lo):
    parts = [split2(keep(x, head)) for head in (0, 1)]
    lhs = cat([cat([hi, lo], 1) for hi, lo in parts], 0)
    return dot(lhs, cat([y_hi, y_hi], 0)) + dot(lhs[:, :128], y_lo)


def pick(x):
    first = (lax.broadcasted_iota(jnp.int32, (128, x.shape[1]), 1) & 127) < HD
    return jnp.where(first, x[:128], x[128:])


def inverses(lowers):
    i = lax.broadcasted_iota(jnp.int32, (128, 128), 0)
    j = lax.broadcasted_iota(jnp.int32, (128, 128), 1)
    apart = i ^ j
    eye = jnp.where(i == j, 1.0, 0.0)
    zero = jnp.zeros((128, 128), bf16)
    inv = [eye - jnp.where(apart == 1, low, zero).astype(f32) for low in lowers]
    for size in (2, 8, 32):
        inside = (apart >= size) & (apart < 4 * size)
        inv_b = [x.astype(bf16) for x in inv]
        hop = [
            dot(x, jnp.where(inside, low, zero)).astype(bf16) for x, low in zip(inv_b, lowers)
        ]
        both = [dot(h, cat([h, x], 1)) for h, x in zip(hop, inv_b)]
        once = [x - y[:, 128:] for x, y in zip(inv, both)]
        inv = [x + dot(y[:, :128].astype(bf16), x.astype(bf16)) for x, y in zip(once, both)]
    return [x.astype(bf16) for x in inv]


def solve_all(invs, lows, sides):
    first = [pick(dot(inv, side.astype(bf16))).astype(bf16) for inv, side in zip(invs, sides)]
    back = [pick(dot(low, x)) for low, x in zip(lows, first)]
    miss = [
        (side - x.astype(f32) - y).astype(bf16) for side, x, y in zip(sides, first, back)
    ]
    return [x.astype(f32) + pick(dot(inv, m)) for x, inv, m in zip(first, invs, miss)]


def maps_of(z, value, beta_end, kappa_end, gain_end):
    zero = jnp.zeros((128, 128), bf16)
    lhs = cat([z.astype(bf16), cat([zero, -value], 1)], 0)
    both = dot_tn(lhs, cat([beta_end, kappa_end], 0).astype(bf16))
    first = lane_first((64, 128))
    packed = [
        jnp.where(first, both[o : o + 64], both[o + 64 : o + 128]) for o in (0, 128)
    ]
    i = lax.broadcasted_iota(jnp.int32, (64, 128), 0)
    j = lax.broadcasted_iota(jnp.int32, (64, 128), 1) & 63
    transit = jnp.where(i == j, gain_end, 0.0) - packed[0]
    return transit.astype(bf16), (-packed[1]).astype(bf16)


def after(left, transit, written):
    l_hi, l_lo = split2(left)
    t_hi, t_lo = split2(transit)
    weights = two_heads(t_hi)
    moved = dot(cat([l_hi, l_lo], 1), cat([weights, weights], 0)) + dot(l_hi, two_heads(t_lo))
    return moved + written


def after_given(left, transit):
    hi, lo = split2(left)
    weights = two_heads(transit)
    return dot(cat([hi, lo], 1), cat([weights, weights], 0))


def state_reads(reads, state):
    both = dot_nt(cat(split2(reads), 0), two_heads(state))
    return both[:128] + both[128:]


def head_mean(x):
    ones = block_ones()
    ones2 = cat([ones, ones], 0)
    parts = [head_sums(x[:, o : o + 128], ones2) for o in range(0, x.shape[1], 128)]
    return cat(parts, 1) * (1.0 / HD)


def kernel(
    tok, gain, wr, wk, wv, wd, wa, wg, wp, wgp, dbase, rbase, hgain, mix, pscale, wor, wop, init,
    out,
    tok_v, gain_v, weight_v, acc_v, proj_v, norm_v, base_v, mix_v, pscale_v, wout_v, init_v,
    scale_v, pool_v, keys_v, turn_v, low_v, side_v, z_v, reads_v, local_v, map_v, maps_in,
    gate_v, state_v, states_in, merged_v, recout_v, part_v, part_in, part_own, out_v,
    w_sem, small_sem, tok_send, tok_recv, halo_send, halo_recv, map_send, map_recv,
    st_send, st_recv, part_send, part_recv, out_sem,
):
    sp = lax.axis_index("sp")
    tp = lax.axis_index("tp")
    other = 1 - tp
    weights = (wr, wk, wv, wd, wa, wg, wp, wgp)
    group_of = lax.div(sp, 2)
    is_owner = (lax.rem(sp, 2) == tp) & (sp < 2 * GROUPS)

    barrier = pltpu.get_barrier_semaphore()
    pl.semaphore_signal(barrier, inc=1, device_id={"tp": other}, device_id_type=MESH)

    @pl.loop(1, N_SP)
    def _(step):
        pl.semaphore_signal(
            barrier, inc=1, device_id={"sp": lax.rem(sp + step, N_SP)}, device_id_type=MESH
        )

    mine = pl.multiple_of(tp * HALF, HALF)
    theirs = pl.multiple_of(other * HALF, HALF)
    pool_at = pl.multiple_of(tp * PCOLS, 128)
    small = [
        pltpu.make_async_copy(tok, tok_v.at[0], small_sem.at[0]),
        pltpu.make_async_copy(gain.at[:, pl.ds(mine, HALF)], gain_v.at[0], small_sem.at[1]),
        pltpu.make_async_copy(gain.at[:, pl.ds(theirs, HALF)], gain_v.at[1], small_sem.at[2]),
        pltpu.make_async_copy(dbase, base_v.at[0], small_sem.at[3]),
        pltpu.make_async_copy(rbase, base_v.at[1], small_sem.at[4]),
        pltpu.make_async_copy(hgain, base_v.at[2], small_sem.at[5]),
        pltpu.make_async_copy(mix.at[pl.ds(tp * 2, 2)], mix_v, small_sem.at[6]),
        pltpu.make_async_copy(pscale.at[:, pl.ds(pool_at, PCOLS)], pscale_v, small_sem.at[7]),
        pltpu.make_async_copy(init, init_v, small_sem.at[8]),
        pltpu.make_async_copy(wor, wout_v.at[pl.ds(0, RCOLS)], small_sem.at[9]),
        pltpu.make_async_copy(wop, wout_v.at[pl.ds(RCOLS, PCOLS)], small_sem.at[10]),
    ]
    loads = [
        [
            pltpu.make_async_copy(
                w.at[pl.ds(at, HALF)],
                weight_v.at[half, :, pl.ds(OFFS[i], WIDTHS[i])],
                w_sem.at[half, i],
            )
            for i, w in ((i, weights[i]) for i in NEED)
        ]
        for half, at in ((0, mine), (1, theirs))
    ]
    def start(copies):
        for copy in copies:
            copy.start()

    start(small[:3])
    start(loads[0][:2])

    def take(half):
        wide = tok_v[half].reshape(TOK, HALF).astype(f32)
        norm_v[half] = (wide * gain_v[half]).astype(bf16)
        return jnp.sum(wide * wide, axis=1, keepdims=True)

    small[0].wait()
    start(loads[0][2:4] + loads[1][:4] + small[3:5])
    pl.semaphore_wait(barrier, N_SP)
    send_tok = pltpu.make_async_remote_copy(
        src_ref=tok_v.at[0],
        dst_ref=tok_v.at[1],
        send_sem=tok_send,
        recv_sem=tok_recv,
        device_id={"tp": other},
        device_id_type=MESH,
    )
    send_tok.start()
    small[1].wait()
    squares = take(0)

    early = (slice(0, EARLY // 2), slice(EARLY // 2, EARLY))
    for step, at in enumerate(early):
        for copy in loads[0][2 * step : 2 * step + 2]:
            copy.wait()
        acc_v[:, at] = dot(norm_v[0], weight_v[0, :, at])
        if step == 0:
            start(loads[0][4:] + loads[1][4:] + small[5:])

    send_tok.wait_recv()
    small[2].wait()
    squares = squares + take(1)
    scale_v[...] = jnp.broadcast_to(lax.rsqrt(squares * (1.0 / D) + 0.25), (TOK, 128))

    def scaled(total):
        return (total * cat([scale_v[...]] * (total.shape[1] // 128), 1)).astype(bf16)

    for step, at in enumerate(early):
        for copy in loads[1][2 * step : 2 * step + 2]:
            copy.wait()
        total = acc_v[:, at] + dot(norm_v[1], weight_v[1, :, at])
        proj_v[:, at] = scaled(total)

    for copy in small[3:5]:
        copy.wait()
    groups = [(b, p) for b in range(SEQ) for p in range(PAIRS)]

    def part(index, b, p):
        at = OFFS[index] + 128 * p
        return proj_v[b * ROWS : (b + 1) * ROWS, at : at + 128]

    row = lax.broadcasted_iota(jnp.int32, (256, 128), 0) & 127
    col = lax.broadcasted_iota(jnp.int32, (256, 128), 1)
    strict = row > col
    inclusive = row >= col

    def rows_of(index, b):
        at = OFFS[index]
        return proj_v[b * ROWS : (b + 1) * ROWS, at : at + WIDTHS[index]].astype(f32)

    def local_row(index):
        return cat([base_v[index, pl.ds(3 * tp + p, 1), :] for p in range(PAIRS)], 1)

    ends = []
    for b in range(SEQ):
        alpha, shrink, beta, kappa, e_mid, e_tail, e_last = prepare(
            rows_of(1, b), rows_of(3, b), rows_of(4, b), local_row(0), local_row(1)
        )
        keys_v[b, 0] = alpha
        keys_v[b, 1] = shrink
        keys_v[b, 2] = beta
        keys_v[b, 3] = kappa
        ends.append((e_mid, e_tail, e_last))

    def pair_of(index, g):
        b, p = groups[g]
        return keys_v[b, index, :, 128 * p : 128 * p + 128]

    def end_of(index, g):
        b, p = groups[g]
        return ends[b][index][:, 128 * p : 128 * p + 128]

    every = range(GROUPS)
    for g in every:
        turned = cat([pair_of(2, g).T, pair_of(3, g).T], 1)
        y_hi, y_lo = split2(turned)
        turn_v[g, 0] = y_hi
        turn_v[g, 1] = y_lo
        pairs = pair_products(pair_of(0, g), y_hi, y_lo)
        low_v[g] = jnp.where(strict, pairs[:, :128], 0.0).astype(bf16)
        cross = jnp.where(strict, pairs[:, 128:], 0.0).astype(bf16)
        side_v[g, :, :128] = pair_of(0, g) * end_of(0, g)
        side_v[g, :, 128:] = pick(dot(cross, part(2, *groups[g])))
    by_head = inverses([low_v[g, 128 * h : 128 * h + 128, :] for g in every for h in (0, 1)])
    invs = [cat(by_head[2 * g : 2 * g + 2], 0) for g in every]
    map_copies = []
    for some in (range(0, 3), range(3, 6)):
        solved = solve_all(
            [invs[g] for g in some], [low_v[g] for g in some], [side_v[g] for g in some]
        )
        for g, z in zip(some, solved):
            z_v[g] = z.astype(bf16)
            tail = end_of(1, g)
            transit, written = maps_of(
                z, part(2, *groups[g]), pair_of(2, g) * tail, pair_of(3, g) * tail, end_of(2, g)
            )
            map_v[g, 0] = transit
            map_v[g, 1] = written
        for g in some:
            owner = 2 * g + tp
            copy = pltpu.make_async_remote_copy(
                src_ref=map_v.at[g],
                dst_ref=maps_in.at[sp],
                send_sem=map_send.at[g],
                recv_sem=map_recv.at[sp],
                device_id={"sp": owner},
                device_id_type=MESH,
            )
            map_copies.append(copy)

            @pl.when((sp != owner) & (sp < N_SP - 1))
            def _():
                copy.start()

            @pl.when(sp == owner)
            def _():
                pltpu.make_async_copy(map_v.at[g], maps_in.at[sp], map_recv.at[sp]).start()

    def late(index, copies, at):
        for half in (0, 1):
            for copy in loads[half][copies]:
                copy.wait()
        total = dot(norm_v[0], weight_v[0, :, at]) + dot(norm_v[1], weight_v[1, :, at])
        proj_v[:, at] = scaled(total)

    late(6, slice(6, 8), slice(OFFS[6], COLS))
    for b in range(SEQ):
        pool_v[b, 16:, :] = proj_v[b * ROWS : (b + 1) * ROWS, OFFS[6] : OFFS[7]]
    halo = pltpu.make_async_remote_copy(
        src_ref=pool_v.at[:, pl.ds(ROWS, 16), :],
        dst_ref=pool_v.at[:, pl.ds(0, 16), :],
        send_sem=halo_send,
        recv_sem=halo_recv,
        device_id={"sp": lax.rem(sp + 1, N_SP)},
        device_id_type=MESH,
    )

    @pl.when(sp < N_SP - 1)
    def _():
        halo.start()

    @pl.when(sp == 0)
    def _():
        pool_v[:, 0:16, :] = jnp.zeros((SEQ, 16, PCOLS), bf16)

    late(0, slice(4, 6), slice(OFFS[0], OFFS[6]))
    for copy in small[5:]:
        copy.wait()

    def send_state(j):
        return pltpu.make_async_remote_copy(
            src_ref=state_v.at[j],
            dst_ref=states_in.at[group_of],
            send_sem=st_send.at[j],
            recv_sem=st_recv.at[group_of],
            device_id={"sp": j},
            device_id_type=MESH,
        )

    def wait_map(j):
        pltpu.make_async_copy(map_v.at[0], maps_in.at[j], map_recv.at[j]).wait()

    def centred(state):
        return (state - jnp.mean(state, axis=0, keepdims=True)).astype(bf16)

    @pl.when(is_owner)
    def _():
        seq = lax.div(group_of, PAIRS)
        pair = lax.rem(group_of, PAIRS)
        state = cat([init_v[seq, 2 * pair], init_v[seq, 2 * pair + 1]], 1)
        for j in range(N_SP - 1):
            wait_map(j)
        zero = jnp.zeros((HD, 128), f32)
        prefixes = []
        for block in range(4):
            held = [cat([maps_in[4 * block, 0], maps_in[4 * block, 1]], 0).astype(f32)]
            prefixes.append(held)
        for y in (1, 2, 3):
            for block in range(4):
                j = 4 * block + y
                if j < N_SP - 1:
                    held = prefixes[block]
                    moved = after_given(held[-1], maps_in[j, 0])
                    held.append(moved + cat([zero, maps_in[j, 1].astype(f32)], 0))
        for block in range(4):
            held = prefixes[block]
            state_v[4 * block] = centred(state)
            for y in (1, 2, 3):
                inside = held[y - 1]
                state_v[4 * block + y] = centred(after(state, inside[:HD], inside[HD:]))
            if block < 3:
                state = after(state, held[3][:HD], held[3][HD:])

        @pl.loop(0, N_SP)
        def _(j):
            @pl.when(j != sp)
            def _():
                send_state(j).start()

            @pl.when(j == sp)
            def _():
                pltpu.make_async_copy(
                    state_v.at[j], states_in.at[group_of], st_recv.at[group_of]
                ).start()

    for g in every:
        rho = part(0, *groups[g]).astype(f32) * pair_of(1, g)
        pairs = pair_products(rho, turn_v[g, 0], turn_v[g, 1])
        within_beta = jnp.where(inclusive, pairs[:, :128], 0.0).astype(bf16)
        within_kappa = jnp.where(inclusive, pairs[:, 128:], 0.0).astype(bf16)
        drop = pick(dot(within_beta, z_v[g]))
        reads_v[g] = rho * end_of(0, g) - drop[:, :128]
        local = pick(dot(within_kappa, part(2, *groups[g]))) - drop[:, 128:]
        local_v[g] = local - head_mean(local)
    for b in range(SEQ):
        gate = rows_of(5, b)
        gate_v[b] = local_row(2) * (gate * sig(gate))

    @pl.when(sp > 0)
    def _():
        halo.wait_recv()

    places = (sp * ROWS + 1 + lax.broadcasted_iota(jnp.int32, (ROWS, 128), 0)).astype(f32)
    for b in range(SEQ):
        outs = []
        for s in range(2):
            at = slice(128 * s, 128 * s + 128)
            own = pool_v[b, :, at].astype(f32)
            total = own + pltpu.roll(own, 1, 0)
            if s == 1:
                total = total + pltpu.roll(total, 2, 0)
            wide = total + pltpu.roll(total, 2 if s == 0 else 4, 0)
            wide = wide + pltpu.roll(wide, 4 if s == 0 else 8, 0)
            trail = jnp.where(tp == 0, total, wide)[16:]
            window = jnp.where(tp == 0, float(2 << s), float(8 << s))
            diff = (trail / jnp.minimum(places, window) - own[16:]).astype(bf16)
            pooled = dot(diff, mix_v[s])
            gate = proj_v[b * ROWS : (b + 1) * ROWS, OFFS[7] + 128 * s : OFFS[7] + 128 * s + 128]
            gate = gate.astype(f32)
            outs.append((pooled * pscale_v[:, at] * (gate * sig(gate))).astype(bf16))
        recout_v[b * ROWS : (b + 1) * ROWS, RCOLS:] = cat(outs, 1)

    for at in (slice(0, 1024), slice(1024, D)):
        merged_v[:, at] = dot(recout_v[:, RCOLS:], wout_v[RCOLS:, at])

    for g in every:
        pltpu.make_async_copy(state_v.at[0], states_in.at[g], st_recv.at[g]).wait()
    centre = [state_reads(reads_v[g], states_in[g]) + local_v[g] for g in every]
    for b in range(SEQ):
        rec = cat(centre[PAIRS * b : PAIRS * b + PAIRS], 1)
        spread = head_mean(rec * rec)
        recout_v[b * ROWS : (b + 1) * ROWS, :RCOLS] = (
            rec * lax.rsqrt(spread + 1.0) * gate_v[b]
        ).astype(bf16)

    def product(at):
        return (merged_v[:, at] + dot(recout_v[:, :RCOLS], wout_v[:RCOLS, at])).astype(bf16)

    def send_part(tile):
        return pltpu.make_async_remote_copy(
            src_ref=part_v.at[tile],
            dst_ref=part_in.at[tile],
            send_sem=part_send.at[tile],
            recv_sem=part_recv.at[tile],
            device_id={"tp": other},
            device_id_type=MESH,
        )

    def store_out(tile):
        at = pl.ds(512 * tile, 512)
        return pltpu.make_async_copy(out_v.at[:, :, at], out.at[:, :, at], out_sem.at[tile])

    for tile in range(2):
        part_v[tile] = product(pl.ds(pl.multiple_of(theirs + tile * 512, 512), 512))
        send_part(tile).start()
    for tile in range(2):
        part_own[tile] = product(pl.ds(pl.multiple_of(mine + tile * 512, 512), 512))
    for tile in range(2):
        send_part(tile).wait_recv()
        total = part_own[tile].astype(f32) + part_in[tile].astype(f32)
        out_v[:, :, 512 * tile : 512 * tile + 512] = total.astype(bf16).reshape(SEQ, ROWS, 512)
        store_out(tile).start()

    send_tok.wait_send()

    @pl.when(sp < N_SP - 1)
    def _():
        halo.wait_send()

    for g, copy in enumerate(map_copies):
        @pl.when((sp != 2 * g + tp) & (sp < N_SP - 1))
        def _():
            copy.wait_send()

    @pl.when(is_owner)
    def _():
        @pl.loop(0, N_SP)
        def _(j):
            @pl.when(j != sp)
            def _():
                send_state(j).wait_send()

    for tile in range(2):
        send_part(tile).wait_send()
        store_out(tile).wait()


def shards(
    tokens, norm_gain, w_recept, w_key, w_value, w_decay, w_rate, w_gate_rec, w_pool, w_gate_pool,
    decay_base, rate_base, head_gain, pool_mix, pool_scale, w_out_rec, w_out_pool, init_state,
):
    vmem, sem = pltpu.VMEM, pltpu.SemaphoreType.DMA
    row = lambda x: x.reshape(1, -1)
    tile = lambda x: x.reshape(6, 128)
    scratch = [
        vmem((2, SEQ, ROWS, HALF), bf16),
        vmem((2, 1, HALF), f32),
        vmem((2, HALF, COLS), bf16),
        vmem((TOK, EARLY), f32),
        vmem((TOK, COLS), bf16),
        vmem((2, TOK, HALF), bf16),
        vmem((3, 6, 128), f32),
        vmem((2, 128, 128), bf16),
        vmem((1, PCOLS), f32),
        vmem((RCOLS + PCOLS, D), bf16),
        vmem((SEQ, 2 * PAIRS, HD, HD), f32),
        vmem((TOK, 128), f32),
        vmem((SEQ, 16 + ROWS, PCOLS), bf16),
        vmem((SEQ, 4, ROWS, RCOLS), f32),
        vmem((GROUPS, 2, 128, 256), bf16),
        vmem((GROUPS, 256, 128), bf16),
        vmem((GROUPS, 128, 256), f32),
        vmem((GROUPS, 128, 256), bf16),
        vmem((GROUPS, 128, 128), f32),
        vmem((GROUPS, 128, 128), f32),
        vmem((GROUPS, 2, HD, 128), bf16),
        vmem((N_SP, 2, HD, 128), bf16),
        vmem((SEQ, ROWS, RCOLS), f32),
        vmem((N_SP, HD, 128), bf16),
        vmem((GROUPS, HD, 128), bf16),
        vmem((TOK, D), f32),
        vmem((TOK, RCOLS + PCOLS), bf16),
        vmem((2, TOK, 512), bf16),
        vmem((2, TOK, 512), bf16),
        vmem((2, TOK, 512), bf16),
        vmem((SEQ, ROWS, HALF), bf16),
        sem((2, 8)),
        sem((11,)),
        sem,
        sem,
        sem,
        sem,
        sem((GROUPS,)),
        sem((N_SP,)),
        sem((N_SP,)),
        sem((GROUPS,)),
        sem((2,)),
        sem((2,)),
        sem((2,)),
    ]
    return pl.pallas_call(
        kernel,
        out_shape=jax.ShapeDtypeStruct((SEQ, ROWS, HALF), bf16),
        in_specs=[pl.BlockSpec(memory_space=pl.ANY)] * 18,
        out_specs=pl.BlockSpec(memory_space=pl.ANY),
        scratch_shapes=scratch,
        compiler_params=pltpu.CompilerParams(
            collective_id=0, has_side_effects=True, vmem_limit_bytes=56 << 20
        ),
        name="layer",
    )(
        tokens, row(norm_gain), w_recept, w_key, w_value, w_decay, w_rate, w_gate_rec, w_pool,
        w_gate_pool, tile(decay_base), tile(rate_base), tile(head_gain), pool_mix, row(pool_scale),
        w_out_rec, w_out_pool, init_state,
    )


def solution(mesh):
    split = P(None, "tp")
    placed = (
        P("fs", "sp", "tp"), P(),
        split, split, split, split, split, split, split, split,
        P(), P(), P(), P(), P(),
        P("tp", None), P("tp", None), P("fs", "tp", None, None),
    )
    return jax.shard_map(
        shards, mesh=mesh, in_specs=placed, out_specs=P("fs", "sp", "tp"), check_vma=False
    )
```

```python
import math

import jax
import jax.numpy as jnp
from jax import lax
from jax.experimental import pallas as pl
from jax.experimental.pallas import tpu as pltpu
from jax.sharding import PartitionSpec as P

D = 2048
HALF = 1024
SEQ = 2
ROWS = 128
TOK = SEQ * ROWS
RCOLS = 384
PCOLS = 256
PAIRS = 3
GROUPS = SEQ * PAIRS
HD = 64
N_SP = 16
COLS = 6 * RCOLS + 2 * PCOLS
OFFS = (1536, 0, 1152, 384, 768, 1920, 2304, 2560)
NEED = (1, 3, 4, 2, 0, 5, 6, 7)
EARLY = 4 * RCOLS
WIDTHS = (384, 384, 384, 384, 384, 384, 256, 256)
MESH = pl.DeviceIdType.MESH
f32 = jnp.float32
bf16 = jnp.bfloat16


def dot(a, b):
    return lax.dot_general(a, b, (((1,), (0,)), ((), ())), preferred_element_type=f32)


def dot_nt(a, b):
    return lax.dot_general(a, b, (((1,), (1,)), ((), ())), preferred_element_type=f32)


def dot_tn(a, b):
    return lax.dot_general(a, b, (((0,), (0,)), ((), ())), preferred_element_type=f32)


def split2(x):
    hi = x.astype(bf16)
    return hi, (x - hi.astype(f32)).astype(bf16)


def cat(parts, axis):
    return jnp.concatenate(parts, axis=axis)


def sig(x):
    e = jnp.exp(-jnp.abs(x))
    return jnp.where(x >= 0, 1.0, e) / (1.0 + e)


def lane_first(shape):
    return lax.broadcasted_iota(jnp.int32, shape, len(shape) - 1) < HD


def keep(x, head):
    first = lane_first(x.shape)
    zero = jnp.zeros_like(x)
    return jnp.where(first, x, zero) if head == 0 else jnp.where(first, zero, x)


def two_heads(x):
    return cat([keep(x, 0), keep(x, 1)], 0)


def block_ones():
    i = lax.broadcasted_iota(jnp.int32, (128, 128), 0) < HD
    j = lax.broadcasted_iota(jnp.int32, (128, 128), 1) < HD
    return jnp.where(i == j, 1.0, 0.0).astype(bf16)


def head_sums(x, ones2):
    hi, lo = split2(x)
    return dot(cat([hi, lo], 1), ones2)


def prepare(k, d_in, a_in, d_base, a_base):
    ones = block_ones()
    ones2 = cat([ones, ones], 0)
    x = d_base + d_in
    log_decay = -math.exp(-0.5) * sig(x)
    rate = sig(a_base + a_in)
    squares = k * k
    sums = cat([head_sums(squares[:, o : o + 128], ones2) for o in range(0, RCOLS, 128)], 1)
    unit = k * lax.rsqrt(sums + 1.0)
    removal = unit * rate
    i = lax.broadcasted_iota(jnp.int32, (128, 128), 0)
    j = lax.broadcasted_iota(jnp.int32, (128, 128), 1)
    tri = jnp.where(i >= j, 1.0, 0.0).astype(bf16)
    hi, lo = split2(log_decay)
    rest = (log_decay - hi.astype(f32) - lo.astype(f32)).astype(bf16)
    cum = dot(cat([tri, tri, tri], 1), cat([hi, lo, rest], 0))
    mid = cum[63:64, :]
    last = cum[127:128, :]
    shrink = jnp.exp(cum - mid)
    grow = jnp.exp(mid - cum)
    alpha = jnp.exp(cum - log_decay - mid) * unit
    beta = removal * grow
    kappa = k * grow
    return alpha, shrink, beta, kappa, jnp.exp(mid), jnp.exp(last - mid), jnp.exp(last)


def pair_products(x, y_hi, y_lo):
    parts = [split2(keep(x, head)) for head in (0, 1)]
    lhs = cat([cat([hi, lo], 1) for hi, lo in parts], 0)
    return dot(lhs, cat([y_hi, y_hi], 0)) + dot(lhs[:, :128], y_lo)


def pick(x):
    first = (lax.broadcasted_iota(jnp.int32, (128, x.shape[1]), 1) & 127) < HD
    return jnp.where(first, x[:128], x[128:])


def inverses(lowers):
    i = lax.broadcasted_iota(jnp.int32, (128, 128), 0)
    j = lax.broadcasted_iota(jnp.int32, (128, 128), 1)
    apart = i ^ j
    eye = jnp.where(i == j, 1.0, 0.0)
    zero = jnp.zeros((128, 128), bf16)
    inv = [eye - jnp.where(apart == 1, low, zero).astype(f32) for low in lowers]
    for size in (2, 8, 32):
        inside = (apart >= size) & (apart < 4 * size)
        inv_b = [x.astype(bf16) for x in inv]
        hop = [
            dot(x, jnp.where(inside, low, zero)).astype(bf16) for x, low in zip(inv_b, lowers)
        ]
        both = [dot(h, cat([h, x], 1)) for h, x in zip(hop, inv_b)]
        once = [x - y[:, 128:] for x, y in zip(inv, both)]
        inv = [x + dot(y[:, :128].astype(bf16), x.astype(bf16)) for x, y in zip(once, both)]
    return [x.astype(bf16) for x in inv]


def solve_all(invs, lows, sides):
    first = [pick(dot(inv, side.astype(bf16))).astype(bf16) for inv, side in zip(invs, sides)]
    back = [pick(dot(low, x)) for low, x in zip(lows, first)]
    miss = [
        (side - x.astype(f32) - y).astype(bf16) for side, x, y in zip(sides, first, back)
    ]
    return [x.astype(f32) + pick(dot(inv, m)) for x, inv, m in zip(first, invs, miss)]


def maps_of(z, value, beta_end, kappa_end, gain_end):
    zero = jnp.zeros((128, 128), bf16)
    lhs = cat([z.astype(bf16), cat([zero, -value], 1)], 0)
    both = dot_tn(lhs, cat([beta_end, kappa_end], 0).astype(bf16))
    first = lane_first((64, 128))
    packed = [
        jnp.where(first, both[o : o + 64], both[o + 64 : o + 128]) for o in (0, 128)
    ]
    i = lax.broadcasted_iota(jnp.int32, (64, 128), 0)
    j = lax.broadcasted_iota(jnp.int32, (64, 128), 1) & 63
    transit = jnp.where(i == j, gain_end, 0.0) - packed[0]
    return transit.astype(bf16), (-packed[1]).astype(bf16)


def after(left, transit, written):
    l_hi, l_lo = split2(left)
    t_hi, t_lo = split2(transit)
    weights = two_heads(t_hi)
    moved = dot(cat([l_hi, l_lo], 1), cat([weights, weights], 0)) + dot(l_hi, two_heads(t_lo))
    return moved + written


def after_given(left, transit):
    hi, lo = split2(left)
    weights = two_heads(transit)
    return dot(cat([hi, lo], 1), cat([weights, weights], 0))


def state_reads(reads, state):
    both = dot_nt(cat(split2(reads), 0), two_heads(state))
    return both[:128] + both[128:]


def head_mean(x):
    ones = block_ones()
    ones2 = cat([ones, ones], 0)
    parts = [head_sums(x[:, o : o + 128], ones2) for o in range(0, x.shape[1], 128)]
    return cat(parts, 1) * (1.0 / HD)


def kernel(
    tok, gain, wr, wk, wv, wd, wa, wg, wp, wgp, dbase, rbase, hgain, mix, pscale, wor, wop, init,
    own_out, arrived_out,
    tok_v, gain_v, weight_v, acc_v, proj_v, norm_v, square_v, base_v, mix_v, pscale_v, wout_v, init_v, init_in,
    scale_v, pool_v, keys_v, turn_v, low_v, side_v, z_v, reads_v, local_v, map_v, maps_in,
    gate_v, state_v, states_in, merged_v, recout_v, part_v, part_own,
    w_sem, small_sem, tok_send, tok_recv, halo_send, halo_recv, map_send, map_recv,
    st_send, st_recv, part_send, part_recv, own_sem, init_send, init_recv,
):
    sp = lax.axis_index("sp")
    tp = lax.axis_index("tp")
    other = 1 - tp
    weights = (wr, wk, wv, wd, wa, wg, wp, wgp)
    group_of = lax.div(sp, 2)
    side = lax.rem(sp, 2)
    is_owner = (tp == 1) & (sp < 2 * GROUPS)
    gives_init = (tp == 0) & (side == 0) & (sp < 2 * GROUPS)
    keeps_init = (tp == 1) & (side == 1) & (sp < 2 * GROUPS)

    barrier = pltpu.get_barrier_semaphore()
    pl.semaphore_signal(barrier, inc=1, device_id={"tp": other}, device_id_type=MESH)

    @pl.loop(1, N_SP)
    def _(step):
        peer = lax.rem(sp + step, N_SP)
        for core in (0, 1):
            pl.semaphore_signal(
                barrier, inc=1, device_id={"sp": peer, "tp": core}, device_id_type=MESH
            )

    mine = pl.multiple_of(tp * HALF, HALF)
    theirs = pl.multiple_of(other * HALF, HALF)
    pool_at = pl.multiple_of(tp * PCOLS, 128)
    held = jnp.minimum(group_of, GROUPS - 1)
    small = [
        pltpu.make_async_copy(tok, tok_v, small_sem.at[0]),
        pltpu.make_async_copy(gain.at[:, pl.ds(mine, HALF)], gain_v, small_sem.at[1]),
        pltpu.make_async_copy(dbase, base_v.at[0], small_sem.at[2]),
        pltpu.make_async_copy(rbase, base_v.at[1], small_sem.at[3]),
        pltpu.make_async_copy(hgain, base_v.at[2], small_sem.at[4]),
        pltpu.make_async_copy(mix.at[pl.ds(tp * 2, 2)], mix_v, small_sem.at[5]),
        pltpu.make_async_copy(pscale.at[:, pl.ds(pool_at, PCOLS)], pscale_v, small_sem.at[6]),
        pltpu.make_async_copy(
            init.at[lax.div(held, PAIRS), pl.ds(2 * lax.rem(held, PAIRS), 2)],
            init_v,
            small_sem.at[7],
        ),
        pltpu.make_async_copy(wor, wout_v.at[pl.ds(0, RCOLS)], small_sem.at[8]),
        pltpu.make_async_copy(wop, wout_v.at[pl.ds(RCOLS, PCOLS)], small_sem.at[9]),
    ]
    loads = [
        [
            pltpu.make_async_copy(
                w.at[pl.ds(at, HALF)],
                weight_v.at[half, :, pl.ds(OFFS[i], WIDTHS[i])],
                w_sem.at[half, i],
            )
            for i, w in ((i, weights[i]) for i in NEED)
        ]
        for half, at in ((0, mine), (1, theirs))
    ]
    def start(copies):
        for copy in copies:
            copy.start()

    start(small[:2])
    start(loads[0][:2])

    small[0].wait()
    start(loads[0][2:4] + loads[1][:4] + small[2:4])
    small[1].wait()
    wide = tok_v[...].reshape(TOK, HALF).astype(f32)
    norm_v[0] = (wide * gain_v[...]).astype(bf16)
    squares = wide * wide
    square_v[0] = sum(squares[:, o : o + 128] for o in range(0, HALF, 128))

    pl.semaphore_wait(barrier, 2 * N_SP - 1)
    send_tok = [
        pltpu.make_async_remote_copy(
            src_ref=ref.at[0],
            dst_ref=ref.at[1],
            send_sem=tok_send.at[i],
            recv_sem=tok_recv.at[i],
            device_id={"tp": other},
            device_id_type=MESH,
        )
        for i, ref in enumerate((norm_v, square_v))
    ]
    start(send_tok)
    early = (slice(0, EARLY // 2), slice(EARLY // 2, EARLY))
    for step, at in enumerate(early):
        for copy in loads[0][2 * step : 2 * step + 2]:
            copy.wait()
        acc_v[:, at] = dot(norm_v[0], weight_v[0, :, at])
        if step == 0:
            start(loads[0][4:] + loads[1][4:] + small[4:])

    send_tok[0].wait_recv()

    def scaled(total):
        return (total * cat([scale_v[...]] * (total.shape[1] // 128), 1)).astype(bf16)

    for step, at in enumerate(early):
        for copy in loads[1][2 * step : 2 * step + 2]:
            copy.wait()
        total = acc_v[:, at] + dot(norm_v[1], weight_v[1, :, at])
        if step == 0:
            send_tok[1].wait_recv()
            squares = jnp.sum(square_v[0] + square_v[1], axis=1, keepdims=True)
            scale = lax.rsqrt(squares * (1.0 / D) + 0.25)
            scale_v[...] = jnp.broadcast_to(scale, (TOK, 128))
        proj_v[:, at] = scaled(total)

    for copy in small[2:4]:
        copy.wait()
    groups = [(b, p) for b in range(SEQ) for p in range(PAIRS)]

    def part(index, b, p):
        at = OFFS[index] + 128 * p
        return proj_v[b * ROWS : (b + 1) * ROWS, at : at + 128]

    row = lax.broadcasted_iota(jnp.int32, (256, 128), 0) & 127
    col = lax.broadcasted_iota(jnp.int32, (256, 128), 1)
    strict = row > col
    inclusive = row >= col

    def rows_of(index, b):
        at = OFFS[index]
        return proj_v[b * ROWS : (b + 1) * ROWS, at : at + WIDTHS[index]].astype(f32)

    def local_row(index):
        return cat([base_v[index, pl.ds(3 * tp + p, 1), :] for p in range(PAIRS)], 1)

    ends = []
    for b in range(SEQ):
        alpha, shrink, beta, kappa, e_mid, e_tail, e_last = prepare(
            rows_of(1, b), rows_of(3, b), rows_of(4, b), local_row(0), local_row(1)
        )
        keys_v[b, 0] = alpha
        keys_v[b, 1] = shrink
        keys_v[b, 2] = beta
        keys_v[b, 3] = kappa
        ends.append((e_mid, e_tail, e_last))

    def pair_of(index, g):
        b, p = groups[g]
        return keys_v[b, index, :, 128 * p : 128 * p + 128]

    def end_of(index, g):
        b, p = groups[g]
        return ends[b][index][:, 128 * p : 128 * p + 128]

    every = range(GROUPS)
    for g in every:
        turned = cat([pair_of(2, g).T, pair_of(3, g).T], 1)
        y_hi, y_lo = split2(turned)
        turn_v[g, 0] = y_hi
        turn_v[g, 1] = y_lo
        pairs = pair_products(pair_of(0, g), y_hi, y_lo)
        low_v[g] = jnp.where(strict, pairs[:, :128], 0.0).astype(bf16)
        cross = jnp.where(strict, pairs[:, 128:], 0.0).astype(bf16)
        side_v[g, :, :128] = pair_of(0, g) * end_of(0, g)
        side_v[g, :, 128:] = pick(dot(cross, part(2, *groups[g])))
    by_head = inverses([low_v[g, 128 * h : 128 * h + 128, :] for g in every for h in (0, 1)])
    invs = [cat(by_head[2 * g : 2 * g + 2], 0) for g in every]
    map_copies = []
    solved = solve_all(invs, [low_v[g] for g in every], [side_v[g] for g in every])
    for g, z in zip(every, solved):
        z_v[g] = z.astype(bf16)
        tail = end_of(1, g)
        transit, written = maps_of(
            z, part(2, *groups[g]), pair_of(2, g) * tail, pair_of(3, g) * tail, end_of(2, g)
        )
        map_v[g, 0] = transit
        map_v[g, 1] = written
    own_map = [(tp == 1) & (sp == 2 * g + 1) for g in every]
    for g in every:
        copy = pltpu.make_async_remote_copy(
            src_ref=map_v.at[g],
            dst_ref=maps_in.at[sp],
            send_sem=map_send.at[g],
            recv_sem=map_recv.at[sp],
            device_id={"sp": 2 * g + tp, "tp": 1},
            device_id_type=MESH,
        )
        map_copies.append(copy)

        @pl.when(jnp.logical_not(own_map[g]) & (sp < N_SP - 1))
        def _():
            copy.start()

        @pl.when(own_map[g])
        def _():
            pltpu.make_async_copy(map_v.at[g], maps_in.at[sp], map_recv.at[sp]).start()

    def late(index, copies, at):
        for half in (0, 1):
            for copy in loads[half][copies]:
                copy.wait()
        total = dot(norm_v[0], weight_v[0, :, at]) + dot(norm_v[1], weight_v[1, :, at])
        proj_v[:, at] = scaled(total)

    late(6, slice(6, 8), slice(OFFS[6], COLS))
    for b in range(SEQ):
        pool_v[b, 16:, :] = proj_v[b * ROWS : (b + 1) * ROWS, OFFS[6] : OFFS[7]]
    halo = pltpu.make_async_remote_copy(
        src_ref=pool_v.at[:, pl.ds(ROWS, 16), :],
        dst_ref=pool_v.at[:, pl.ds(0, 16), :],
        send_sem=halo_send,
        recv_sem=halo_recv,
        device_id={"sp": lax.rem(sp + 1, N_SP)},
        device_id_type=MESH,
    )

    @pl.when(sp < N_SP - 1)
    def _():
        halo.start()

    @pl.when(sp == 0)
    def _():
        pool_v[:, 0:16, :] = jnp.zeros((SEQ, 16, PCOLS), bf16)

    def send_state(j):
        return pltpu.make_async_remote_copy(
            src_ref=state_v.at[j],
            dst_ref=states_in.at[group_of],
            send_sem=st_send.at[j],
            recv_sem=st_recv.at[group_of],
            device_id={"sp": j, "tp": side},
            device_id_type=MESH,
        )

    def wait_map(j):
        pltpu.make_async_copy(map_v.at[0], maps_in.at[j], map_recv.at[j]).wait()

    def centred(state):
        return (state - jnp.mean(state, axis=0, keepdims=True)).astype(bf16)

    small[7].wait()
    give = pltpu.make_async_remote_copy(
        src_ref=init_v,
        dst_ref=init_in,
        send_sem=init_send,
        recv_sem=init_recv,
        device_id={"tp": other},
        device_id_type=MESH,
    )

    @pl.when(gives_init)
    def _():
        give.start()

    @pl.when(keeps_init)
    def _():
        pltpu.make_async_copy(init_v, init_in, init_recv).start()

    @pl.when(is_owner)
    def _():
        pltpu.make_async_copy(init_v, init_in, init_recv).wait()
        start_state = cat([init_in[0], init_in[1]], 1)
        for j in range(N_SP - 1):
            wait_map(j)
        zero = jnp.zeros((HD, 128), f32)

        def then(left, transit, written):
            return after_given(left, transit) + cat([zero, written.astype(f32)], 0)

        def apply(state, held):
            return after(state, held[:HD], held[HD:])

        prefixes = []
        for block in range(4):
            prefixes.append([cat([maps_in[4 * block, 0], maps_in[4 * block, 1]], 0).astype(f32)])
        for y in (1, 2, 3):
            for block in range(4):
                j = 4 * block + y
                if j < N_SP - 1:
                    prefixes[block].append(then(prefixes[block][-1], maps_in[j, 0], maps_in[j, 1]))
        totals = [prefixes[block][3] for block in range(3)]
        ahead = after(totals[1], totals[2][:HD], cat([zero, totals[2][HD:]], 0))
        fourth = apply(start_state, totals[0])
        starts = [start_state, fourth, apply(fourth, totals[1]), apply(fourth, ahead)]
        for block in range(4):
            state_v[4 * block] = centred(starts[block])
            for y in (1, 2, 3):
                inside = prefixes[block][y - 1]
                moved = after_given(starts[block], inside[:HD].astype(bf16)) + inside[HD:]
                state_v[4 * block + y] = centred(moved)

        @pl.loop(0, N_SP)
        def _(j):
            @pl.when((j != sp) | (side == 0))
            def _():
                send_state(j).start()

            @pl.when((j == sp) & (side == 1))
            def _():
                pltpu.make_async_copy(
                    state_v.at[j], states_in.at[group_of], st_recv.at[group_of]
                ).start()

    late(0, slice(4, 6), slice(OFFS[0], OFFS[6]))
    for copy in small[4:7] + small[8:]:
        copy.wait()

    for g in every:
        rho = part(0, *groups[g]).astype(f32) * pair_of(1, g)
        pairs = pair_products(rho, turn_v[g, 0], turn_v[g, 1])
        within_beta = jnp.where(inclusive, pairs[:, :128], 0.0).astype(bf16)
        within_kappa = jnp.where(inclusive, pairs[:, 128:], 0.0).astype(bf16)
        drop = pick(dot(within_beta, z_v[g]))
        reads_v[g] = rho * end_of(0, g) - drop[:, :128]
        local = pick(dot(within_kappa, part(2, *groups[g]))) - drop[:, 128:]
        local_v[g] = local - head_mean(local)
    for b in range(SEQ):
        gate = rows_of(5, b)
        gate_v[b] = local_row(2) * (gate * sig(gate))

    @pl.when(sp > 0)
    def _():
        halo.wait_recv()

    places = (sp * ROWS + 1 + lax.broadcasted_iota(jnp.int32, (ROWS, 128), 0)).astype(f32)
    for b in range(SEQ):
        outs = []
        for s in range(2):
            at = slice(128 * s, 128 * s + 128)
            own = pool_v[b, :, at].astype(f32)
            total = own + pltpu.roll(own, 1, 0)
            if s == 1:
                total = total + pltpu.roll(total, 2, 0)
            wide = total + pltpu.roll(total, 2 if s == 0 else 4, 0)
            wide = wide + pltpu.roll(wide, 4 if s == 0 else 8, 0)
            trail = jnp.where(tp == 0, total, wide)[16:]
            window = jnp.where(tp == 0, float(2 << s), float(8 << s))
            diff = (trail / jnp.minimum(places, window) - own[16:]).astype(bf16)
            pooled = dot(diff, mix_v[s])
            gate = proj_v[b * ROWS : (b + 1) * ROWS, OFFS[7] + 128 * s : OFFS[7] + 128 * s + 128]
            gate = gate.astype(f32)
            outs.append((pooled * pscale_v[:, at] * (gate * sig(gate))).astype(bf16))
        recout_v[b * ROWS : (b + 1) * ROWS, RCOLS:] = cat(outs, 1)

    for at in (slice(0, 1024), slice(1024, D)):
        merged_v[:, at] = dot(recout_v[:, RCOLS:], wout_v[RCOLS:, at])

    for g in every:
        pltpu.make_async_copy(state_v.at[0], states_in.at[g], st_recv.at[g]).wait()
    centre = [state_reads(reads_v[g], states_in[g]) + local_v[g] for g in every]
    for b in range(SEQ):
        rec = cat(centre[PAIRS * b : PAIRS * b + PAIRS], 1)
        spread = head_mean(rec * rec)
        recout_v[b * ROWS : (b + 1) * ROWS, :RCOLS] = (
            rec * lax.rsqrt(spread + 1.0) * gate_v[b]
        ).astype(bf16)

    def product(at):
        total = merged_v[:, at] + dot(recout_v[:, :RCOLS], wout_v[:RCOLS, at])
        return total.astype(bf16).reshape(SEQ, ROWS, 512)

    def columns(ref, tile):
        return ref.at[:, :, pl.ds(512 * tile, 512)]

    def send_part(tile):
        return pltpu.make_async_remote_copy(
            src_ref=part_v.at[tile],
            dst_ref=columns(arrived_out, tile),
            send_sem=part_send.at[tile],
            recv_sem=part_recv.at[tile],
            device_id={"tp": other},
            device_id_type=MESH,
        )

    def keep_part(tile):
        return pltpu.make_async_copy(part_own.at[tile], columns(own_out, tile), own_sem.at[tile])

    for tile in range(2):
        part_v[tile] = product(pl.ds(pl.multiple_of(theirs + tile * 512, 512), 512))
        send_part(tile).start()
    for tile in range(2):
        part_own[tile] = product(pl.ds(pl.multiple_of(mine + tile * 512, 512), 512))
        keep_part(tile).start()

    for copy in send_tok:
        copy.wait_send()

    @pl.when(sp < N_SP - 1)
    def _():
        halo.wait_send()

    for g, copy in enumerate(map_copies):
        @pl.when(jnp.logical_not(own_map[g]) & (sp < N_SP - 1))
        def _():
            copy.wait_send()

    @pl.when(gives_init)
    def _():
        give.wait_send()

    @pl.when(is_owner)
    def _():
        @pl.loop(0, N_SP)
        def _(j):
            @pl.when((j != sp) | (side == 0))
            def _():
                send_state(j).wait_send()

    for tile in range(2):
        send_part(tile).wait()
        keep_part(tile).wait()


def shards(
    tokens, norm_gain, w_recept, w_key, w_value, w_decay, w_rate, w_gate_rec, w_pool, w_gate_pool,
    decay_base, rate_base, head_gain, pool_mix, pool_scale, w_out_rec, w_out_pool, init_state,
):
    vmem, sem = pltpu.VMEM, pltpu.SemaphoreType.DMA
    row = lambda x: x.reshape(1, -1)
    tile = lambda x: x.reshape(6, 128)
    scratch = [
        vmem((SEQ, ROWS, HALF), bf16),
        vmem((1, HALF), f32),
        vmem((2, HALF, COLS), bf16),
        vmem((TOK, EARLY), f32),
        vmem((TOK, COLS), bf16),
        vmem((2, TOK, HALF), bf16),
        vmem((2, TOK, 128), f32),
        vmem((3, 6, 128), f32),
        vmem((2, 128, 128), bf16),
        vmem((1, PCOLS), f32),
        vmem((RCOLS + PCOLS, D), bf16),
        vmem((2, HD, HD), f32),
        vmem((2, HD, HD), f32),
        vmem((TOK, 128), f32),
        vmem((SEQ, 16 + ROWS, PCOLS), bf16),
        vmem((SEQ, 4, ROWS, RCOLS), f32),
        vmem((GROUPS, 2, 128, 256), bf16),
        vmem((GROUPS, 256, 128), bf16),
        vmem((GROUPS, 128, 256), f32),
        vmem((GROUPS, 128, 256), bf16),
        vmem((GROUPS, 128, 128), f32),
        vmem((GROUPS, 128, 128), f32),
        vmem((GROUPS, 2, HD, 128), bf16),
        vmem((N_SP, 2, HD, 128), bf16),
        vmem((SEQ, ROWS, RCOLS), f32),
        vmem((N_SP, HD, 128), bf16),
        vmem((GROUPS, HD, 128), bf16),
        vmem((TOK, D), f32),
        vmem((TOK, RCOLS + PCOLS), bf16),
        vmem((2, SEQ, ROWS, 512), bf16),
        vmem((2, SEQ, ROWS, 512), bf16),
        sem((2, 8)),
        sem((10,)),
        sem((2,)),
        sem((2,)),
        sem,
        sem,
        sem((GROUPS,)),
        sem((N_SP,)),
        sem((N_SP,)),
        sem((GROUPS,)),
        sem((2,)),
        sem((2,)),
        sem((2,)),
        sem,
        sem,
    ]
    own, arrived = pl.pallas_call(
        kernel,
        out_shape=[jax.ShapeDtypeStruct((SEQ, ROWS, HALF), bf16)] * 2,
        in_specs=[pl.BlockSpec(memory_space=pl.ANY)] * 18,
        out_specs=[pl.BlockSpec(memory_space=pl.ANY)] * 2,
        scratch_shapes=scratch,
        compiler_params=pltpu.CompilerParams(
            collective_id=0, has_side_effects=True, vmem_limit_bytes=56 << 20
        ),
        name="layer",
    )(
        tokens, row(norm_gain), w_recept, w_key, w_value, w_decay, w_rate, w_gate_rec, w_pool,
        w_gate_pool, tile(decay_base), tile(rate_base), tile(head_gain), pool_mix, row(pool_scale),
        w_out_rec, w_out_pool, init_state,
    )
    return (own.astype(f32) + arrived.astype(f32)).astype(bf16)


def solution(mesh):
    split = P(None, "tp")
    placed = (
        P("fs", "sp", "tp"), P(),
        split, split, split, split, split, split, split, split,
        P(), P(), P(), P(), P(),
        P("tp", None), P("tp", None), P("fs", "tp", None, None),
    )
    return jax.shard_map(
        shards, mesh=mesh, in_specs=placed, out_specs=P("fs", "sp", "tp"), check_vma=False
    )
```

```python
import math

import jax
import jax.numpy as jnp
from jax import lax
from jax.experimental import pallas as pl
from jax.experimental.pallas import tpu as pltpu
from jax.sharding import PartitionSpec as P

D = 2048
HALF = 1024
SEQ = 2
ROWS = 128
TOK = SEQ * ROWS
RCOLS = 384
PCOLS = 256
PAIRS = 3
GROUPS = SEQ * PAIRS
HD = 64
N_SP = 16
COLS = 6 * RCOLS + 2 * PCOLS
OFFS = (1536, 0, 1152, 384, 768, 1920, 2304, 2560)
NEED = (1, 3, 4, 2, 0, 5, 6, 7)
EARLY = 4 * RCOLS
WIDTHS = (384, 384, 384, 384, 384, 384, 256, 256)
MESH = pl.DeviceIdType.MESH
f32 = jnp.float32
bf16 = jnp.bfloat16


def dot(a, b):
    return lax.dot_general(a, b, (((1,), (0,)), ((), ())), preferred_element_type=f32)


def dot_nt(a, b):
    return lax.dot_general(a, b, (((1,), (1,)), ((), ())), preferred_element_type=f32)


def dot_tn(a, b):
    return lax.dot_general(a, b, (((0,), (0,)), ((), ())), preferred_element_type=f32)


def split2(x):
    hi = x.astype(bf16)
    return hi, (x - hi.astype(f32)).astype(bf16)


def cat(parts, axis):
    return jnp.concatenate(parts, axis=axis)


def sig(x):
    e = jnp.exp(-jnp.abs(x))
    return jnp.where(x >= 0, 1.0, e) / (1.0 + e)


def lane_first(shape):
    return lax.broadcasted_iota(jnp.int32, shape, len(shape) - 1) < HD


def keep(x, head):
    first = lane_first(x.shape)
    zero = jnp.zeros_like(x)
    return jnp.where(first, x, zero) if head == 0 else jnp.where(first, zero, x)


def two_heads(x):
    return cat([keep(x, 0), keep(x, 1)], 0)


def block_ones():
    i = lax.broadcasted_iota(jnp.int32, (128, 128), 0) < HD
    j = lax.broadcasted_iota(jnp.int32, (128, 128), 1) < HD
    return jnp.where(i == j, 1.0, 0.0).astype(bf16)


def head_sums(x, ones2):
    hi, lo = split2(x)
    return dot(cat([hi, lo], 1), ones2)


def prepare(k, d_in, a_in, d_base, a_base):
    ones = block_ones()
    ones2 = cat([ones, ones], 0)
    x = d_base + d_in
    log_decay = -math.exp(-0.5) * sig(x)
    rate = sig(a_base + a_in)
    squares = k * k
    sums = cat([head_sums(squares[:, o : o + 128], ones2) for o in range(0, RCOLS, 128)], 1)
    unit = k * lax.rsqrt(sums + 1.0)
    removal = unit * rate
    i = lax.broadcasted_iota(jnp.int32, (128, 128), 0)
    j = lax.broadcasted_iota(jnp.int32, (128, 128), 1)
    tri = jnp.where(i >= j, 1.0, 0.0).astype(bf16)
    hi, lo = split2(log_decay)
    rest = (log_decay - hi.astype(f32) - lo.astype(f32)).astype(bf16)
    cum = dot(cat([tri, tri, tri], 1), cat([hi, lo, rest], 0))
    mid = cum[63:64, :]
    last = cum[127:128, :]
    shrink = jnp.exp(cum - mid)
    grow = jnp.exp(mid - cum)
    alpha = jnp.exp(cum - log_decay - mid) * unit
    beta = removal * grow
    kappa = k * grow
    return alpha, shrink, beta, kappa, jnp.exp(mid), jnp.exp(last - mid), jnp.exp(last)


def pair_products(x, y_hi, y_lo):
    parts = [split2(keep(x, head)) for head in (0, 1)]
    lhs = cat([cat([hi, lo], 1) for hi, lo in parts], 0)
    return dot(lhs, cat([y_hi, y_hi], 0)) + dot(lhs[:, :128], y_lo)


def pick(x):
    first = (lax.broadcasted_iota(jnp.int32, (128, x.shape[1]), 1) & 127) < HD
    return jnp.where(first, x[:128], x[128:])


def inverses(lowers):
    i = lax.broadcasted_iota(jnp.int32, (128, 128), 0)
    j = lax.broadcasted_iota(jnp.int32, (128, 128), 1)
    apart = i ^ j
    eye = jnp.where(i == j, 1.0, 0.0)
    zero = jnp.zeros((128, 128), bf16)
    inv = [eye - jnp.where(apart == 1, low, zero).astype(f32) for low in lowers]
    for size in (2, 8, 32):
        inside = (apart >= size) & (apart < 4 * size)
        inv_b = [x.astype(bf16) for x in inv]
        hop = [
            dot(x, jnp.where(inside, low, zero)).astype(bf16) for x, low in zip(inv_b, lowers)
        ]
        both = [dot(h, cat([h, x], 1)) for h, x in zip(hop, inv_b)]
        once = [x - y[:, 128:] for x, y in zip(inv, both)]
        inv = [x + dot(y[:, :128].astype(bf16), x.astype(bf16)) for x, y in zip(once, both)]
    return [x.astype(bf16) for x in inv]


def solve_all(invs, lows, sides):
    first = [pick(dot(inv, side.astype(bf16))).astype(bf16) for inv, side in zip(invs, sides)]
    back = [pick(dot(low, x)) for low, x in zip(lows, first)]
    miss = [
        (side - x.astype(f32) - y).astype(bf16) for side, x, y in zip(sides, first, back)
    ]
    return [x.astype(f32) + pick(dot(inv, m)) for x, inv, m in zip(first, invs, miss)]


def maps_of(z, value, beta_end, kappa_end, gain_end):
    zero = jnp.zeros((128, 128), bf16)
    lhs = cat([z.astype(bf16), cat([zero, -value], 1)], 0)
    both = dot_tn(lhs, cat([beta_end, kappa_end], 0).astype(bf16))
    first = lane_first((64, 128))
    packed = [
        jnp.where(first, both[o : o + 64], both[o + 64 : o + 128]) for o in (0, 128)
    ]
    i = lax.broadcasted_iota(jnp.int32, (64, 128), 0)
    j = lax.broadcasted_iota(jnp.int32, (64, 128), 1) & 63
    transit = jnp.where(i == j, gain_end, 0.0) - packed[0]
    return transit.astype(bf16), (-packed[1]).astype(bf16)


def after(left, transit, written):
    l_hi, l_lo = split2(left)
    t_hi, t_lo = split2(transit)
    weights = two_heads(t_hi)
    moved = dot(cat([l_hi, l_lo], 1), cat([weights, weights], 0)) + dot(l_hi, two_heads(t_lo))
    return moved + written


def after_given(left, transit):
    hi, lo = split2(left)
    weights = two_heads(transit)
    return dot(cat([hi, lo], 1), cat([weights, weights], 0))


def state_reads(reads, state):
    both = dot_nt(cat(split2(reads), 0), two_heads(state))
    return both[:128] + both[128:]


def head_mean(x):
    ones = block_ones()
    ones2 = cat([ones, ones], 0)
    parts = [head_sums(x[:, o : o + 128], ones2) for o in range(0, x.shape[1], 128)]
    return cat(parts, 1) * (1.0 / HD)


def kernel(
    tok, gain, wr, wk, wv, wd, wa, wg, wp, wgp, dbase, rbase, hgain, mix, pscale, wor, wop, init,
    own_out, arrived_out,
    tok_v, gain_v, weight_v, acc_v, proj_v, norm_v, square_v, base_v, mix_v, pscale_v, wout_v, init_v, init_in,
    scale_v, pool_v, keys_v, turn_v, low_v, side_v, z_v, reads_v, local_v, map_v, maps_in,
    gate_v, state_v, states_in, merged_v, recout_v, part_v, part_own,
    w_sem, small_sem, tok_send, tok_recv, halo_send, halo_recv, map_send, map_recv,
    st_send, st_recv, part_send, part_recv, own_sem, init_send, init_recv, pair_sem, go_sem,
):
    sp = lax.axis_index("sp")
    tp = lax.axis_index("tp")
    other = 1 - tp
    weights = (wr, wk, wv, wd, wa, wg, wp, wgp)
    group_of = lax.div(sp, 2)
    side = lax.rem(sp, 2)
    is_owner = (tp == 1) & (sp < 2 * GROUPS)
    gives_init = (tp == 0) & (side == 0) & (sp < 2 * GROUPS)
    keeps_init = (tp == 1) & (side == 1) & (sp < 2 * GROUPS)

    barrier = pltpu.get_barrier_semaphore()

    def tell(semaphore, **device):
        pl.semaphore_signal(semaphore, inc=1, device_id=device, device_id_type=MESH)

    @pl.when(tp == 1)
    def _():
        tell(barrier, tp=other)

    mine = pl.multiple_of(tp * HALF, HALF)
    theirs = pl.multiple_of(other * HALF, HALF)
    pool_at = pl.multiple_of(tp * PCOLS, 128)
    held = jnp.minimum(group_of, GROUPS - 1)
    small = [
        pltpu.make_async_copy(tok, tok_v, small_sem.at[0]),
        pltpu.make_async_copy(gain.at[:, pl.ds(mine, HALF)], gain_v, small_sem.at[1]),
        pltpu.make_async_copy(dbase, base_v.at[0], small_sem.at[2]),
        pltpu.make_async_copy(rbase, base_v.at[1], small_sem.at[3]),
        pltpu.make_async_copy(hgain, base_v.at[2], small_sem.at[4]),
        pltpu.make_async_copy(mix.at[pl.ds(tp * 2, 2)], mix_v, small_sem.at[5]),
        pltpu.make_async_copy(pscale.at[:, pl.ds(pool_at, PCOLS)], pscale_v, small_sem.at[6]),
        pltpu.make_async_copy(
            init.at[lax.div(held, PAIRS), pl.ds(2 * lax.rem(held, PAIRS), 2)],
            init_v,
            small_sem.at[7],
        ),
        pltpu.make_async_copy(wor, wout_v.at[pl.ds(0, RCOLS)], small_sem.at[8]),
        pltpu.make_async_copy(wop, wout_v.at[pl.ds(RCOLS, PCOLS)], small_sem.at[9]),
    ]
    loads = [
        [
            pltpu.make_async_copy(
                w.at[pl.ds(at, HALF)],
                weight_v.at[half, :, pl.ds(OFFS[i], WIDTHS[i])],
                w_sem.at[half, i],
            )
            for i, w in ((i, weights[i]) for i in NEED)
        ]
        for half, at in ((0, mine), (1, theirs))
    ]
    def start(copies):
        for copy in copies:
            copy.start()

    start(small[:2])
    start(loads[0][:2])

    small[0].wait()

    @pl.when(tp == 0)
    def _():
        pl.semaphore_wait(barrier, 1)
        tell(pair_sem, tp=other)

    start(loads[0][2:4] + loads[1][:4] + small[2:4])
    small[1].wait()
    wide = tok_v[...].reshape(TOK, HALF).astype(f32)
    norm_v[0] = (wide * gain_v[...]).astype(bf16)
    squares = wide * wide
    square_v[0] = sum(squares[:, o : o + 128] for o in range(0, HALF, 128))

    @pl.when(tp == 1)
    def _():
        pl.semaphore_wait(pair_sem, 1)

        @pl.loop(1, N_SP)
        def _(step):
            tell(barrier, sp=lax.rem(sp + step, N_SP))

    send_tok = [
        pltpu.make_async_remote_copy(
            src_ref=ref.at[0],
            dst_ref=ref.at[1],
            send_sem=tok_send.at[i],
            recv_sem=tok_recv.at[i],
            device_id={"tp": other},
            device_id_type=MESH,
        )
        for i, ref in enumerate((norm_v, square_v))
    ]
    start(send_tok)
    early = (slice(0, EARLY // 2), slice(EARLY // 2, EARLY))
    for step, at in enumerate(early):
        for copy in loads[0][2 * step : 2 * step + 2]:
            copy.wait()
        acc_v[:, at] = dot(norm_v[0], weight_v[0, :, at])
        if step == 0:
            start(loads[0][4:] + loads[1][4:] + small[4:])

    send_tok[0].wait_recv()

    def scaled(total):
        return (total * cat([scale_v[...]] * (total.shape[1] // 128), 1)).astype(bf16)

    for step, at in enumerate(early):
        for copy in loads[1][2 * step : 2 * step + 2]:
            copy.wait()
        total = acc_v[:, at] + dot(norm_v[1], weight_v[1, :, at])
        if step == 0:
            send_tok[1].wait_recv()
            squares = jnp.sum(square_v[0] + square_v[1], axis=1, keepdims=True)
            scale = lax.rsqrt(squares * (1.0 / D) + 0.25)
            scale_v[...] = jnp.broadcast_to(scale, (TOK, 128))
        proj_v[:, at] = scaled(total)

    for copy in small[2:4]:
        copy.wait()
    groups = [(b, p) for b in range(SEQ) for p in range(PAIRS)]

    def part(index, b, p):
        at = OFFS[index] + 128 * p
        return proj_v[b * ROWS : (b + 1) * ROWS, at : at + 128]

    row = lax.broadcasted_iota(jnp.int32, (256, 128), 0) & 127
    col = lax.broadcasted_iota(jnp.int32, (256, 128), 1)
    strict = row > col
    inclusive = row >= col

    def rows_of(index, b):
        at = OFFS[index]
        return proj_v[b * ROWS : (b + 1) * ROWS, at : at + WIDTHS[index]].astype(f32)

    def local_row(index):
        return cat([base_v[index, pl.ds(3 * tp + p, 1), :] for p in range(PAIRS)], 1)

    ends = []
    for b in range(SEQ):
        alpha, shrink, beta, kappa, e_mid, e_tail, e_last = prepare(
            rows_of(1, b), rows_of(3, b), rows_of(4, b), local_row(0), local_row(1)
        )
        keys_v[b, 0] = alpha
        keys_v[b, 1] = shrink
        keys_v[b, 2] = beta
        keys_v[b, 3] = kappa
        ends.append((e_mid, e_tail, e_last))

    def pair_of(index, g):
        b, p = groups[g]
        return keys_v[b, index, :, 128 * p : 128 * p + 128]

    def end_of(index, g):
        b, p = groups[g]
        return ends[b][index][:, 128 * p : 128 * p + 128]

    every = range(GROUPS)
    for g in every:
        turned = cat([pair_of(2, g).T, pair_of(3, g).T], 1)
        y_hi, y_lo = split2(turned)
        turn_v[g, 0] = y_hi
        turn_v[g, 1] = y_lo
        pairs = pair_products(pair_of(0, g), y_hi, y_lo)
        low_v[g] = jnp.where(strict, pairs[:, :128], 0.0).astype(bf16)
        cross = jnp.where(strict, pairs[:, 128:], 0.0).astype(bf16)
        side_v[g, :, :128] = pair_of(0, g) * end_of(0, g)
        side_v[g, :, 128:] = pick(dot(cross, part(2, *groups[g])))
    @pl.when(tp == 1)
    def _():
        pl.semaphore_wait(barrier, N_SP - 1)
        tell(go_sem, tp=other)

    by_head = inverses([low_v[g, 128 * h : 128 * h + 128, :] for g in every for h in (0, 1)])
    invs = [cat(by_head[2 * g : 2 * g + 2], 0) for g in every]
    map_copies = []
    solved = solve_all(invs, [low_v[g] for g in every], [side_v[g] for g in every])
    for g, z in zip(every, solved):
        z_v[g] = z.astype(bf16)
        tail = end_of(1, g)
        transit, written = maps_of(
            z, part(2, *groups[g]), pair_of(2, g) * tail, pair_of(3, g) * tail, end_of(2, g)
        )
        map_v[g, 0] = transit
        map_v[g, 1] = written
    @pl.when(tp == 0)
    def _():
        pl.semaphore_wait(go_sem, 1)

    own_map = [(tp == 1) & (sp == 2 * g + 1) for g in every]
    for g in every:
        copy = pltpu.make_async_remote_copy(
            src_ref=map_v.at[g],
            dst_ref=maps_in.at[sp],
            send_sem=map_send.at[g],
            recv_sem=map_recv.at[sp],
            device_id={"sp": 2 * g + tp, "tp": 1},
            device_id_type=MESH,
        )
        map_copies.append(copy)

        @pl.when(jnp.logical_not(own_map[g]) & (sp < N_SP - 1))
        def _():
            copy.start()

        @pl.when(own_map[g])
        def _():
            pltpu.make_async_copy(map_v.at[g], maps_in.at[sp], map_recv.at[sp]).start()

    def late(index, copies, at):
        for half in (0, 1):
            for copy in loads[half][copies]:
                copy.wait()
        total = dot(norm_v[0], weight_v[0, :, at]) + dot(norm_v[1], weight_v[1, :, at])
        proj_v[:, at] = scaled(total)

    late(6, slice(6, 8), slice(OFFS[6], COLS))
    for b in range(SEQ):
        pool_v[b, 16:, :] = proj_v[b * ROWS : (b + 1) * ROWS, OFFS[6] : OFFS[7]]
    halo = pltpu.make_async_remote_copy(
        src_ref=pool_v.at[:, pl.ds(ROWS, 16), :],
        dst_ref=pool_v.at[:, pl.ds(0, 16), :],
        send_sem=halo_send,
        recv_sem=halo_recv,
        device_id={"sp": lax.rem(sp + 1, N_SP)},
        device_id_type=MESH,
    )

    @pl.when(sp < N_SP - 1)
    def _():
        halo.start()

    @pl.when(sp == 0)
    def _():
        pool_v[:, 0:16, :] = jnp.zeros((SEQ, 16, PCOLS), bf16)

    def send_state(j):
        return pltpu.make_async_remote_copy(
            src_ref=state_v.at[j],
            dst_ref=states_in.at[group_of],
            send_sem=st_send.at[j],
            recv_sem=st_recv.at[group_of],
            device_id={"sp": j, "tp": side},
            device_id_type=MESH,
        )

    def wait_map(j):
        pltpu.make_async_copy(map_v.at[0], maps_in.at[j], map_recv.at[j]).wait()

    def centred(state):
        return (state - jnp.mean(state, axis=0, keepdims=True)).astype(bf16)

    small[7].wait()
    give = pltpu.make_async_remote_copy(
        src_ref=init_v,
        dst_ref=init_in,
        send_sem=init_send,
        recv_sem=init_recv,
        device_id={"tp": other},
        device_id_type=MESH,
    )

    @pl.when(gives_init)
    def _():
        give.start()

    @pl.when(keeps_init)
    def _():
        pltpu.make_async_copy(init_v, init_in, init_recv).start()

    @pl.when(is_owner)
    def _():
        pltpu.make_async_copy(init_v, init_in, init_recv).wait()
        start_state = cat([init_in[0], init_in[1]], 1)
        for j in range(N_SP - 1):
            wait_map(j)
        zero = jnp.zeros((HD, 128), f32)

        def then(left, transit, written):
            return after_given(left, transit) + cat([zero, written.astype(f32)], 0)

        def apply(state, held):
            return after(state, held[:HD], held[HD:])

        prefixes = []
        for block in range(4):
            prefixes.append([cat([maps_in[4 * block, 0], maps_in[4 * block, 1]], 0).astype(f32)])
        for y in (1, 2, 3):
            for block in range(4):
                j = 4 * block + y
                if j < N_SP - 1:
                    prefixes[block].append(then(prefixes[block][-1], maps_in[j, 0], maps_in[j, 1]))
        totals = [prefixes[block][3] for block in range(3)]
        ahead = after(totals[1], totals[2][:HD], cat([zero, totals[2][HD:]], 0))
        fourth = apply(start_state, totals[0])
        starts = [start_state, fourth, apply(fourth, totals[1]), apply(fourth, ahead)]
        for block in range(4):
            state_v[4 * block] = centred(starts[block])
            for y in (1, 2, 3):
                inside = prefixes[block][y - 1]
                moved = after_given(starts[block], inside[:HD].astype(bf16)) + inside[HD:]
                state_v[4 * block + y] = centred(moved)

        @pl.loop(0, N_SP)
        def _(j):
            @pl.when((j != sp) | (side == 0))
            def _():
                send_state(j).start()

            @pl.when((j == sp) & (side == 1))
            def _():
                pltpu.make_async_copy(
                    state_v.at[j], states_in.at[group_of], st_recv.at[group_of]
                ).start()

    late(0, slice(4, 6), slice(OFFS[0], OFFS[6]))
    for copy in small[4:7] + small[8:]:
        copy.wait()

    for g in every:
        rho = part(0, *groups[g]).astype(f32) * pair_of(1, g)
        pairs = pair_products(rho, turn_v[g, 0], turn_v[g, 1])
        within_beta = jnp.where(inclusive, pairs[:, :128], 0.0).astype(bf16)
        within_kappa = jnp.where(inclusive, pairs[:, 128:], 0.0).astype(bf16)
        drop = pick(dot(within_beta, z_v[g]))
        reads_v[g] = rho * end_of(0, g) - drop[:, :128]
        local = pick(dot(within_kappa, part(2, *groups[g]))) - drop[:, 128:]
        local_v[g] = local - head_mean(local)
    for b in range(SEQ):
        gate = rows_of(5, b)
        gate_v[b] = local_row(2) * (gate * sig(gate))

    @pl.when(sp > 0)
    def _():
        halo.wait_recv()

    places = (sp * ROWS + 1 + lax.broadcasted_iota(jnp.int32, (ROWS, 128), 0)).astype(f32)
    for b in range(SEQ):
        outs = []
        for s in range(2):
            at = slice(128 * s, 128 * s + 128)
            own = pool_v[b, :, at].astype(f32)
            total = own + pltpu.roll(own, 1, 0)
            if s == 1:
                total = total + pltpu.roll(total, 2, 0)
            wide = total + pltpu.roll(total, 2 if s == 0 else 4, 0)
            wide = wide + pltpu.roll(wide, 4 if s == 0 else 8, 0)
            trail = jnp.where(tp == 0, total, wide)[16:]
            window = jnp.where(tp == 0, float(2 << s), float(8 << s))
            diff = (trail / jnp.minimum(places, window) - own[16:]).astype(bf16)
            pooled = dot(diff, mix_v[s])
            gate = proj_v[b * ROWS : (b + 1) * ROWS, OFFS[7] + 128 * s : OFFS[7] + 128 * s + 128]
            gate = gate.astype(f32)
            outs.append((pooled * pscale_v[:, at] * (gate * sig(gate))).astype(bf16))
        recout_v[b * ROWS : (b + 1) * ROWS, RCOLS:] = cat(outs, 1)

    for at in (slice(0, 1024), slice(1024, D)):
        merged_v[:, at] = dot(recout_v[:, RCOLS:], wout_v[RCOLS:, at])

    for g in every:
        pltpu.make_async_copy(state_v.at[0], states_in.at[g], st_recv.at[g]).wait()
    centre = [state_reads(reads_v[g], states_in[g]) + local_v[g] for g in every]
    for b in range(SEQ):
        rec = cat(centre[PAIRS * b : PAIRS * b + PAIRS], 1)
        spread = head_mean(rec * rec)
        recout_v[b * ROWS : (b + 1) * ROWS, :RCOLS] = (
            rec * lax.rsqrt(spread + 1.0) * gate_v[b]
        ).astype(bf16)

    def product(at):
        total = merged_v[:, at] + dot(recout_v[:, :RCOLS], wout_v[:RCOLS, at])
        return total.astype(bf16).reshape(SEQ, ROWS, 512)

    def columns(ref, tile):
        return ref.at[:, :, pl.ds(512 * tile, 512)]

    def send_part(tile):
        return pltpu.make_async_remote_copy(
            src_ref=part_v.at[tile],
            dst_ref=columns(arrived_out, tile),
            send_sem=part_send.at[tile],
            recv_sem=part_recv.at[tile],
            device_id={"tp": other},
            device_id_type=MESH,
        )

    def keep_part(tile):
        return pltpu.make_async_copy(part_own.at[tile], columns(own_out, tile), own_sem.at[tile])

    for tile in range(2):
        part_v[tile] = product(pl.ds(pl.multiple_of(theirs + tile * 512, 512), 512))
        send_part(tile).start()
    for tile in range(2):
        part_own[tile] = product(pl.ds(pl.multiple_of(mine + tile * 512, 512), 512))
        keep_part(tile).start()

    for copy in send_tok:
        copy.wait_send()

    @pl.when(sp < N_SP - 1)
    def _():
        halo.wait_send()

    for g, copy in enumerate(map_copies):
        @pl.when(jnp.logical_not(own_map[g]) & (sp < N_SP - 1))
        def _():
            copy.wait_send()

    @pl.when(gives_init)
    def _():
        give.wait_send()

    @pl.when(is_owner)
    def _():
        @pl.loop(0, N_SP)
        def _(j):
            @pl.when((j != sp) | (side == 0))
            def _():
                send_state(j).wait_send()

    for tile in range(2):
        send_part(tile).wait()
        keep_part(tile).wait()


def shards(
    tokens, norm_gain, w_recept, w_key, w_value, w_decay, w_rate, w_gate_rec, w_pool, w_gate_pool,
    decay_base, rate_base, head_gain, pool_mix, pool_scale, w_out_rec, w_out_pool, init_state,
):
    vmem, sem = pltpu.VMEM, pltpu.SemaphoreType.DMA
    row = lambda x: x.reshape(1, -1)
    tile = lambda x: x.reshape(6, 128)
    scratch = [
        vmem((SEQ, ROWS, HALF), bf16),
        vmem((1, HALF), f32),
        vmem((2, HALF, COLS), bf16),
        vmem((TOK, EARLY), f32),
        vmem((TOK, COLS), bf16),
        vmem((2, TOK, HALF), bf16),
        vmem((2, TOK, 128), f32),
        vmem((3, 6, 128), f32),
        vmem((2, 128, 128), bf16),
        vmem((1, PCOLS), f32),
        vmem((RCOLS + PCOLS, D), bf16),
        vmem((2, HD, HD), f32),
        vmem((2, HD, HD), f32),
        vmem((TOK, 128), f32),
        vmem((SEQ, 16 + ROWS, PCOLS), bf16),
        vmem((SEQ, 4, ROWS, RCOLS), f32),
        vmem((GROUPS, 2, 128, 256), bf16),
        vmem((GROUPS, 256, 128), bf16),
        vmem((GROUPS, 128, 256), f32),
        vmem((GROUPS, 128, 256), bf16),
        vmem((GROUPS, 128, 128), f32),
        vmem((GROUPS, 128, 128), f32),
        vmem((GROUPS, 2, HD, 128), bf16),
        vmem((N_SP, 2, HD, 128), bf16),
        vmem((SEQ, ROWS, RCOLS), f32),
        vmem((N_SP, HD, 128), bf16),
        vmem((GROUPS, HD, 128), bf16),
        vmem((TOK, D), f32),
        vmem((TOK, RCOLS + PCOLS), bf16),
        vmem((2, SEQ, ROWS, 512), bf16),
        vmem((2, SEQ, ROWS, 512), bf16),
        sem((2, 8)),
        sem((10,)),
        sem((2,)),
        sem((2,)),
        sem,
        sem,
        sem((GROUPS,)),
        sem((N_SP,)),
        sem((N_SP,)),
        sem((GROUPS,)),
        sem((2,)),
        sem((2,)),
        sem((2,)),
        sem,
        sem,
        pltpu.SemaphoreType.REGULAR,
        pltpu.SemaphoreType.REGULAR,
    ]
    own, arrived = pl.pallas_call(
        kernel,
        out_shape=[jax.ShapeDtypeStruct((SEQ, ROWS, HALF), bf16)] * 2,
        in_specs=[pl.BlockSpec(memory_space=pl.ANY)] * 18,
        out_specs=[pl.BlockSpec(memory_space=pl.ANY)] * 2,
        scratch_shapes=scratch,
        compiler_params=pltpu.CompilerParams(
            collective_id=0, has_side_effects=True, vmem_limit_bytes=56 << 20
        ),
        name="layer",
    )(
        tokens, row(norm_gain), w_recept, w_key, w_value, w_decay, w_rate, w_gate_rec, w_pool,
        w_gate_pool, tile(decay_base), tile(rate_base), tile(head_gain), pool_mix, row(pool_scale),
        w_out_rec, w_out_pool, init_state,
    )
    return (own.astype(f32) + arrived.astype(f32)).astype(bf16)


def solution(mesh):
    split = P(None, "tp")
    placed = (
        P("fs", "sp", "tp"), P(),
        split, split, split, split, split, split, split, split,
        P(), P(), P(), P(), P(),
        P("tp", None), P("tp", None), P("fs", "tp", None, None),
    )
    return jax.shard_map(
        shards, mesh=mesh, in_specs=placed, out_specs=P("fs", "sp", "tp"), check_vma=False
    )
```

```python
import math

import jax
import jax.numpy as jnp
from jax import lax
from jax.experimental import pallas as pl
from jax.experimental.pallas import tpu as pltpu
from jax.sharding import PartitionSpec as P

D = 2048
HALF = 1024
SEQ = 2
ROWS = 128
TOK = SEQ * ROWS
RCOLS = 384
PCOLS = 256
PAIRS = 3
GROUPS = SEQ * PAIRS
HD = 64
N_SP = 16
COLS = 6 * RCOLS + 2 * PCOLS
OFFS = (1536, 0, 1152, 384, 768, 1920, 2304, 2560)
NEED = (1, 3, 4, 2, 0, 5, 6, 7)
EARLY = 4 * RCOLS
WIDTHS = (384, 384, 384, 384, 384, 384, 256, 256)
MESH = pl.DeviceIdType.MESH
f32 = jnp.float32
bf16 = jnp.bfloat16


def dot(a, b):
    return lax.dot_general(a, b, (((1,), (0,)), ((), ())), preferred_element_type=f32)


def dot_nt(a, b):
    return lax.dot_general(a, b, (((1,), (1,)), ((), ())), preferred_element_type=f32)


def dot_tn(a, b):
    return lax.dot_general(a, b, (((0,), (0,)), ((), ())), preferred_element_type=f32)


def split2(x):
    hi = x.astype(bf16)
    return hi, (x - hi.astype(f32)).astype(bf16)


def cat(parts, axis):
    return jnp.concatenate(parts, axis=axis)


def sig(x):
    e = jnp.exp(-jnp.abs(x))
    return jnp.where(x >= 0, 1.0, e) / (1.0 + e)


def lane_first(shape):
    return lax.broadcasted_iota(jnp.int32, shape, len(shape) - 1) < HD


def keep(x, head):
    first = lane_first(x.shape)
    zero = jnp.zeros_like(x)
    return jnp.where(first, x, zero) if head == 0 else jnp.where(first, zero, x)


def two_heads(x):
    return cat([keep(x, 0), keep(x, 1)], 0)


def block_ones():
    i = lax.broadcasted_iota(jnp.int32, (128, 128), 0) < HD
    j = lax.broadcasted_iota(jnp.int32, (128, 128), 1) < HD
    return jnp.where(i == j, 1.0, 0.0).astype(bf16)


def head_sums(x, ones2):
    hi, lo = split2(x)
    return dot(cat([hi, lo], 1), ones2)


def prepare(k, d_in, a_in, d_base, a_base):
    ones = block_ones()
    ones2 = cat([ones, ones], 0)
    x = d_base + d_in
    log_decay = -math.exp(-0.5) * sig(x)
    rate = sig(a_base + a_in)
    squares = k * k
    sums = cat([head_sums(squares[:, o : o + 128], ones2) for o in range(0, RCOLS, 128)], 1)
    unit = k * lax.rsqrt(sums + 1.0)
    removal = unit * rate
    i = lax.broadcasted_iota(jnp.int32, (128, 128), 0)
    j = lax.broadcasted_iota(jnp.int32, (128, 128), 1)
    tri = jnp.where(i >= j, 1.0, 0.0).astype(bf16)
    hi, lo = split2(log_decay)
    rest = (log_decay - hi.astype(f32) - lo.astype(f32)).astype(bf16)
    cum = dot(cat([tri, tri, tri], 1), cat([hi, lo, rest], 0))
    mid = cum[63:64, :]
    last = cum[127:128, :]
    shrink = jnp.exp(cum - mid)
    grow = jnp.exp(mid - cum)
    alpha = jnp.exp(cum - log_decay - mid) * unit
    beta = removal * grow
    kappa = k * grow
    return alpha, shrink, beta, kappa, jnp.exp(mid), jnp.exp(last - mid), jnp.exp(last)


def pair_products(x, y_hi, y_lo):
    parts = [split2(keep(x, head)) for head in (0, 1)]
    lhs = cat([cat([hi, lo], 1) for hi, lo in parts], 0)
    return dot(lhs, cat([y_hi, y_hi], 0)) + dot(lhs[:, :128], y_lo)


def pick(x):
    first = (lax.broadcasted_iota(jnp.int32, (128, x.shape[1]), 1) & 127) < HD
    return jnp.where(first, x[:128], x[128:])


def inverses(lowers):
    i = lax.broadcasted_iota(jnp.int32, (128, 128), 0)
    j = lax.broadcasted_iota(jnp.int32, (128, 128), 1)
    apart = i ^ j
    eye = jnp.where(i == j, 1.0, 0.0)
    zero = jnp.zeros((128, 128), bf16)
    inv = [eye - jnp.where(apart == 1, low, zero).astype(f32) for low in lowers]
    for size in (2, 8, 32):
        inside = (apart >= size) & (apart < 4 * size)
        inv_b = [x.astype(bf16) for x in inv]
        hop = [
            dot(x, jnp.where(inside, low, zero)).astype(bf16) for x, low in zip(inv_b, lowers)
        ]
        both = [dot(h, cat([h, x], 1)) for h, x in zip(hop, inv_b)]
        once = [x - y[:, 128:] for x, y in zip(inv, both)]
        inv = [x + dot(y[:, :128].astype(bf16), x.astype(bf16)) for x, y in zip(once, both)]
    return [x.astype(bf16) for x in inv]


def solve_all(invs, lows, sides):
    first = [pick(dot(inv, side.astype(bf16))).astype(bf16) for inv, side in zip(invs, sides)]
    back = [pick(dot(low, x)) for low, x in zip(lows, first)]
    miss = [
        (side - x.astype(f32) - y).astype(bf16) for side, x, y in zip(sides, first, back)
    ]
    return [x.astype(f32) + pick(dot(inv, m)) for x, inv, m in zip(first, invs, miss)]


def maps_of(z, value, beta_end, kappa_end, gain_end):
    zero = jnp.zeros((128, 128), bf16)
    lhs = cat([z.astype(bf16), cat([zero, -value], 1)], 0)
    both = dot_tn(lhs, cat([beta_end, kappa_end], 0).astype(bf16))
    first = lane_first((64, 128))
    packed = [
        jnp.where(first, both[o : o + 64], both[o + 64 : o + 128]) for o in (0, 128)
    ]
    i = lax.broadcasted_iota(jnp.int32, (64, 128), 0)
    j = lax.broadcasted_iota(jnp.int32, (64, 128), 1) & 63
    transit = jnp.where(i == j, gain_end, 0.0) - packed[0]
    return transit.astype(bf16), (-packed[1]).astype(bf16)


def after_given(state, transit):
    both = dot(cat(split2(state), 0), two_heads(transit))
    return both[:HD] + both[HD:]


def state_reads(reads, state):
    both = dot_nt(cat(split2(reads), 0), two_heads(state))
    return both[:128] + both[128:]


def head_mean(x):
    ones = block_ones()
    ones2 = cat([ones, ones], 0)
    parts = [head_sums(x[:, o : o + 128], ones2) for o in range(0, x.shape[1], 128)]
    return cat(parts, 1) * (1.0 / HD)


def kernel(
    tok, gain, wr, wk, wv, wd, wa, wg, wp, wgp, dbase, rbase, hgain, mix, pscale, wor, wop, init,
    own_out, arrived_out,
    tok_v, gain_v, weight_v, acc_v, proj_v, norm_v, square_v, base_v, mix_v, pscale_v, wout_v, init_v, init_in,
    scale_v, pool_v, keys_v, turn_v, low_v, side_v, z_v, reads_v, local_v, map_v, maps_in,
    gate_v, state_v, states_in, merged_v, recout_v, part_v, part_own,
    w_sem, small_sem, tok_send, tok_recv, halo_send, halo_recv, map_send, map_recv,
    st_send, st_recv, part_send, part_recv, own_sem, init_send, init_recv, pair_sem, go_sem,
):
    sp = lax.axis_index("sp")
    tp = lax.axis_index("tp")
    other = 1 - tp
    weights = (wr, wk, wv, wd, wa, wg, wp, wgp)
    group_of = lax.div(sp, 2)
    side = lax.rem(sp, 2)
    is_owner = (tp == 1) & (sp < 2 * GROUPS)
    gives_init = (tp == 0) & (side == 0) & (sp < 2 * GROUPS)
    keeps_init = (tp == 1) & (side == 1) & (sp < 2 * GROUPS)

    barrier = pltpu.get_barrier_semaphore()

    def tell(semaphore, **device):
        pl.semaphore_signal(semaphore, inc=1, device_id=device, device_id_type=MESH)

    @pl.when(tp == 1)
    def _():
        tell(barrier, tp=other)

    mine = pl.multiple_of(tp * HALF, HALF)
    theirs = pl.multiple_of(other * HALF, HALF)
    pool_at = pl.multiple_of(tp * PCOLS, 128)
    held = jnp.minimum(group_of, GROUPS - 1)
    small = [
        pltpu.make_async_copy(tok, tok_v, small_sem.at[0]),
        pltpu.make_async_copy(gain.at[:, pl.ds(mine, HALF)], gain_v, small_sem.at[1]),
        pltpu.make_async_copy(dbase, base_v.at[0], small_sem.at[2]),
        pltpu.make_async_copy(rbase, base_v.at[1], small_sem.at[3]),
        pltpu.make_async_copy(hgain, base_v.at[2], small_sem.at[4]),
        pltpu.make_async_copy(mix.at[pl.ds(tp * 2, 2)], mix_v, small_sem.at[5]),
        pltpu.make_async_copy(pscale.at[:, pl.ds(pool_at, PCOLS)], pscale_v, small_sem.at[6]),
        pltpu.make_async_copy(
            init.at[lax.div(held, PAIRS), pl.ds(2 * lax.rem(held, PAIRS), 2)],
            init_v,
            small_sem.at[7],
        ),
        pltpu.make_async_copy(wor, wout_v.at[pl.ds(0, RCOLS)], small_sem.at[8]),
        pltpu.make_async_copy(wop, wout_v.at[pl.ds(RCOLS, PCOLS)], small_sem.at[9]),
    ]
    loads = [
        [
            pltpu.make_async_copy(
                w.at[pl.ds(at, HALF)],
                weight_v.at[half, :, pl.ds(OFFS[i], WIDTHS[i])],
                w_sem.at[half, i],
            )
            for i, w in ((i, weights[i]) for i in NEED)
        ]
        for half, at in ((0, mine), (1, theirs))
    ]
    def start(copies):
        for copy in copies:
            copy.start()

    start(small[:2])
    start(loads[0][:2])

    small[0].wait()

    @pl.when(tp == 0)
    def _():
        pl.semaphore_wait(barrier, 1)
        tell(pair_sem, tp=other)

    start(loads[0][2:4] + loads[1][:4] + small[2:4])
    small[1].wait()
    wide = tok_v[...].reshape(TOK, HALF).astype(f32)
    norm_v[0] = (wide * gain_v[...]).astype(bf16)
    squares = wide * wide
    square_v[0] = sum(squares[:, o : o + 128] for o in range(0, HALF, 128))

    @pl.when(tp == 1)
    def _():
        pl.semaphore_wait(pair_sem, 1)

        @pl.loop(1, N_SP)
        def _(step):
            tell(barrier, sp=lax.rem(sp + step, N_SP))

    send_tok = [
        pltpu.make_async_remote_copy(
            src_ref=ref.at[0],
            dst_ref=ref.at[1],
            send_sem=tok_send.at[i],
            recv_sem=tok_recv.at[i],
            device_id={"tp": other},
            device_id_type=MESH,
        )
        for i, ref in enumerate((norm_v, square_v))
    ]
    start(send_tok)
    early = (slice(0, EARLY // 2), slice(EARLY // 2, EARLY))
    for step, at in enumerate(early):
        for copy in loads[0][2 * step : 2 * step + 2]:
            copy.wait()
        acc_v[:, at] = dot(norm_v[0], weight_v[0, :, at])
        if step == 0:
            start(loads[0][4:] + loads[1][4:] + small[4:])

    send_tok[0].wait_recv()

    def scaled(total):
        return (total * cat([scale_v[...]] * (total.shape[1] // 128), 1)).astype(bf16)

    for step, at in enumerate(early):
        for copy in loads[1][2 * step : 2 * step + 2]:
            copy.wait()
        total = acc_v[:, at] + dot(norm_v[1], weight_v[1, :, at])
        if step == 0:
            send_tok[1].wait_recv()
            squares = jnp.sum(square_v[0] + square_v[1], axis=1, keepdims=True)
            scale = lax.rsqrt(squares * (1.0 / D) + 0.25)
            scale_v[...] = jnp.broadcast_to(scale, (TOK, 128))
        proj_v[:, at] = scaled(total)

    for copy in small[2:4]:
        copy.wait()
    groups = [(b, p) for b in range(SEQ) for p in range(PAIRS)]

    def part(index, b, p):
        at = OFFS[index] + 128 * p
        return proj_v[b * ROWS : (b + 1) * ROWS, at : at + 128]

    row = lax.broadcasted_iota(jnp.int32, (256, 128), 0) & 127
    col = lax.broadcasted_iota(jnp.int32, (256, 128), 1)
    strict = row > col
    inclusive = row >= col

    def rows_of(index, b):
        at = OFFS[index]
        return proj_v[b * ROWS : (b + 1) * ROWS, at : at + WIDTHS[index]].astype(f32)

    def local_row(index):
        return cat([base_v[index, pl.ds(3 * tp + p, 1), :] for p in range(PAIRS)], 1)

    ends = []
    for b in range(SEQ):
        alpha, shrink, beta, kappa, e_mid, e_tail, e_last = prepare(
            rows_of(1, b), rows_of(3, b), rows_of(4, b), local_row(0), local_row(1)
        )
        keys_v[b, 0] = alpha
        keys_v[b, 1] = shrink
        keys_v[b, 2] = beta
        keys_v[b, 3] = kappa
        ends.append((e_mid, e_tail, e_last))

    def pair_of(index, g):
        b, p = groups[g]
        return keys_v[b, index, :, 128 * p : 128 * p + 128]

    def end_of(index, g):
        b, p = groups[g]
        return ends[b][index][:, 128 * p : 128 * p + 128]

    every = range(GROUPS)
    for g in every:
        turned = cat([pair_of(2, g).T, pair_of(3, g).T], 1)
        y_hi, y_lo = split2(turned)
        turn_v[g, 0] = y_hi
        turn_v[g, 1] = y_lo
        pairs = pair_products(pair_of(0, g), y_hi, y_lo)
        low_v[g] = jnp.where(strict, pairs[:, :128], 0.0).astype(bf16)
        cross = jnp.where(strict, pairs[:, 128:], 0.0).astype(bf16)
        side_v[g, :, :128] = pair_of(0, g) * end_of(0, g)
        side_v[g, :, 128:] = pick(dot(cross, part(2, *groups[g])))
    @pl.when(tp == 1)
    def _():
        pl.semaphore_wait(barrier, N_SP - 1)
        tell(go_sem, tp=other)

    by_head = inverses([low_v[g, 128 * h : 128 * h + 128, :] for g in every for h in (0, 1)])
    invs = [cat(by_head[2 * g : 2 * g + 2], 0) for g in every]
    map_copies = []
    solved = solve_all(invs, [low_v[g] for g in every], [side_v[g] for g in every])
    for g, z in zip(every, solved):
        z_v[g] = z.astype(bf16)
        tail = end_of(1, g)
        transit, written = maps_of(
            z, part(2, *groups[g]), pair_of(2, g) * tail, pair_of(3, g) * tail, end_of(2, g)
        )
        map_v[g, 0] = transit
        map_v[g, 1] = written
    @pl.when(tp == 0)
    def _():
        pl.semaphore_wait(go_sem, 1)

    own_map = [(tp == 1) & (sp == 2 * g + 1) for g in every]
    for g in every:
        copy = pltpu.make_async_remote_copy(
            src_ref=map_v.at[g],
            dst_ref=maps_in.at[sp],
            send_sem=map_send.at[g],
            recv_sem=map_recv.at[sp],
            device_id={"sp": 2 * g + tp, "tp": 1},
            device_id_type=MESH,
        )
        map_copies.append(copy)

        @pl.when(jnp.logical_not(own_map[g]) & (sp < N_SP - 1))
        def _():
            copy.start()

        @pl.when(own_map[g])
        def _():
            pltpu.make_async_copy(map_v.at[g], maps_in.at[sp], map_recv.at[sp]).start()

    def late(index, copies, at):
        for half in (0, 1):
            for copy in loads[half][copies]:
                copy.wait()
        total = dot(norm_v[0], weight_v[0, :, at]) + dot(norm_v[1], weight_v[1, :, at])
        proj_v[:, at] = scaled(total)

    late(6, slice(6, 8), slice(OFFS[6], COLS))
    for b in range(SEQ):
        pool_v[b, 16:, :] = proj_v[b * ROWS : (b + 1) * ROWS, OFFS[6] : OFFS[7]]
    halo = pltpu.make_async_remote_copy(
        src_ref=pool_v.at[:, pl.ds(ROWS, 16), :],
        dst_ref=pool_v.at[:, pl.ds(0, 16), :],
        send_sem=halo_send,
        recv_sem=halo_recv,
        device_id={"sp": lax.rem(sp + 1, N_SP)},
        device_id_type=MESH,
    )

    @pl.when(sp < N_SP - 1)
    def _():
        halo.start()

    @pl.when(sp == 0)
    def _():
        pool_v[:, 0:16, :] = jnp.zeros((SEQ, 16, PCOLS), bf16)

    late(0, slice(4, 5), slice(OFFS[0], OFFS[5]))
    for g in every:
        rho = part(0, *groups[g]).astype(f32) * pair_of(1, g)
        pairs = pair_products(rho, turn_v[g, 0], turn_v[g, 1])
        within_beta = jnp.where(inclusive, pairs[:, :128], 0.0).astype(bf16)
        within_kappa = jnp.where(inclusive, pairs[:, 128:], 0.0).astype(bf16)
        drop = pick(dot(within_beta, z_v[g]))
        reads_v[g] = rho * end_of(0, g) - drop[:, :128]
        local = pick(dot(within_kappa, part(2, *groups[g]))) - drop[:, 128:]
        local_v[g] = local - head_mean(local)
    def send_state(j):
        return pltpu.make_async_remote_copy(
            src_ref=state_v.at[j],
            dst_ref=states_in.at[group_of],
            send_sem=st_send.at[j],
            recv_sem=st_recv.at[group_of],
            device_id={"sp": j, "tp": side},
            device_id_type=MESH,
        )

    def wait_map(j):
        pltpu.make_async_copy(map_v.at[0], maps_in.at[j], map_recv.at[j]).wait()

    def centred(state):
        return (state - jnp.mean(state, axis=0, keepdims=True)).astype(bf16)

    small[7].wait()
    give = pltpu.make_async_remote_copy(
        src_ref=init_v,
        dst_ref=init_in,
        send_sem=init_send,
        recv_sem=init_recv,
        device_id={"tp": other},
        device_id_type=MESH,
    )

    @pl.when(gives_init)
    def _():
        give.start()

    @pl.when(keeps_init)
    def _():
        pltpu.make_async_copy(init_v, init_in, init_recv).start()

    @pl.when(is_owner)
    def _():
        pltpu.make_async_copy(init_v, init_in, init_recv).wait()
        state = cat([init_in[0], init_in[1]], 1)
        def emit(j):
            @pl.when((j != sp) | (side == 0))
            def _():
                send_state(j).start()

            @pl.when((j == sp) & (side == 1))
            def _():
                pltpu.make_async_copy(
                    state_v.at[j], states_in.at[group_of], st_recv.at[group_of]
                ).start()

        state_v[0] = centred(state)
        emit(0)
        for block in (range(0, 4), range(4, 8), range(8, 12), range(12, 14), range(14, 15)):
            for j in block:
                wait_map(j)
            for j in block:
                state = after_given(state, maps_in[j, 0]) + maps_in[j, 1].astype(f32)
                state_v[j + 1] = centred(state)
            for j in block:
                emit(j + 1)

    late(5, slice(5, 6), slice(OFFS[5], OFFS[6]))
    for copy in small[4:7] + small[8:]:
        copy.wait()
    for b in range(SEQ):
        gate = rows_of(5, b)
        gate_v[b] = local_row(2) * (gate * sig(gate))

    @pl.when(sp > 0)
    def _():
        halo.wait_recv()

    places = (sp * ROWS + 1 + lax.broadcasted_iota(jnp.int32, (ROWS, 128), 0)).astype(f32)
    for b in range(SEQ):
        outs = []
        for s in range(2):
            at = slice(128 * s, 128 * s + 128)
            own = pool_v[b, :, at].astype(f32)
            total = own + pltpu.roll(own, 1, 0)
            if s == 1:
                total = total + pltpu.roll(total, 2, 0)
            wide = total + pltpu.roll(total, 2 if s == 0 else 4, 0)
            wide = wide + pltpu.roll(wide, 4 if s == 0 else 8, 0)
            trail = jnp.where(tp == 0, total, wide)[16:]
            window = jnp.where(tp == 0, float(2 << s), float(8 << s))
            diff = (trail / jnp.minimum(places, window) - own[16:]).astype(bf16)
            pooled = dot(diff, mix_v[s])
            gate = proj_v[b * ROWS : (b + 1) * ROWS, OFFS[7] + 128 * s : OFFS[7] + 128 * s + 128]
            gate = gate.astype(f32)
            outs.append((pooled * pscale_v[:, at] * (gate * sig(gate))).astype(bf16))
        recout_v[b * ROWS : (b + 1) * ROWS, RCOLS:] = cat(outs, 1)

    for at in (slice(0, 1024), slice(1024, D)):
        merged_v[:, at] = dot(recout_v[:, RCOLS:], wout_v[RCOLS:, at])

    for g in every:
        pltpu.make_async_copy(state_v.at[0], states_in.at[g], st_recv.at[g]).wait()
    centre = [state_reads(reads_v[g], states_in[g]) + local_v[g] for g in every]
    for b in range(SEQ):
        rec = cat(centre[PAIRS * b : PAIRS * b + PAIRS], 1)
        spread = head_mean(rec * rec)
        recout_v[b * ROWS : (b + 1) * ROWS, :RCOLS] = (
            rec * lax.rsqrt(spread + 1.0) * gate_v[b]
        ).astype(bf16)

    def product(at):
        total = merged_v[:, at] + dot(recout_v[:, :RCOLS], wout_v[:RCOLS, at])
        return total.astype(bf16).reshape(SEQ, ROWS, 512)

    def columns(ref, tile):
        return ref.at[:, :, pl.ds(512 * tile, 512)]

    def send_part(tile):
        return pltpu.make_async_remote_copy(
            src_ref=part_v.at[tile],
            dst_ref=columns(arrived_out, tile),
            send_sem=part_send.at[tile],
            recv_sem=part_recv.at[tile],
            device_id={"tp": other},
            device_id_type=MESH,
        )

    def keep_part(tile):
        return pltpu.make_async_copy(part_own.at[tile], columns(own_out, tile), own_sem.at[tile])

    for tile in range(2):
        part_v[tile] = product(pl.ds(pl.multiple_of(theirs + tile * 512, 512), 512))
        send_part(tile).start()
    for tile in range(2):
        part_own[tile] = product(pl.ds(pl.multiple_of(mine + tile * 512, 512), 512))
        keep_part(tile).start()

    for copy in send_tok:
        copy.wait_send()

    @pl.when(sp < N_SP - 1)
    def _():
        halo.wait_send()

    for g, copy in enumerate(map_copies):
        @pl.when(jnp.logical_not(own_map[g]) & (sp < N_SP - 1))
        def _():
            copy.wait_send()

    @pl.when(gives_init)
    def _():
        give.wait_send()

    @pl.when(is_owner)
    def _():
        @pl.loop(0, N_SP)
        def _(j):
            @pl.when((j != sp) | (side == 0))
            def _():
                send_state(j).wait_send()

    for tile in range(2):
        send_part(tile).wait()
        keep_part(tile).wait()


def shards(
    tokens, norm_gain, w_recept, w_key, w_value, w_decay, w_rate, w_gate_rec, w_pool, w_gate_pool,
    decay_base, rate_base, head_gain, pool_mix, pool_scale, w_out_rec, w_out_pool, init_state,
):
    vmem, sem = pltpu.VMEM, pltpu.SemaphoreType.DMA
    row = lambda x: x.reshape(1, -1)
    tile = lambda x: x.reshape(6, 128)
    scratch = [
        vmem((SEQ, ROWS, HALF), bf16),
        vmem((1, HALF), f32),
        vmem((2, HALF, COLS), bf16),
        vmem((TOK, EARLY), f32),
        vmem((TOK, COLS), bf16),
        vmem((2, TOK, HALF), bf16),
        vmem((2, TOK, 128), f32),
        vmem((3, 6, 128), f32),
        vmem((2, 128, 128), bf16),
        vmem((1, PCOLS), f32),
        vmem((RCOLS + PCOLS, D), bf16),
        vmem((2, HD, HD), f32),
        vmem((2, HD, HD), f32),
        vmem((TOK, 128), f32),
        vmem((SEQ, 16 + ROWS, PCOLS), bf16),
        vmem((SEQ, 4, ROWS, RCOLS), f32),
        vmem((GROUPS, 2, 128, 256), bf16),
        vmem((GROUPS, 256, 128), bf16),
        vmem((GROUPS, 128, 256), f32),
        vmem((GROUPS, 128, 256), bf16),
        vmem((GROUPS, 128, 128), f32),
        vmem((GROUPS, 128, 128), f32),
        vmem((GROUPS, 2, HD, 128), bf16),
        vmem((N_SP, 2, HD, 128), bf16),
        vmem((SEQ, ROWS, RCOLS), f32),
        vmem((N_SP, HD, 128), bf16),
        vmem((GROUPS, HD, 128), bf16),
        vmem((TOK, D), f32),
        vmem((TOK, RCOLS + PCOLS), bf16),
        vmem((2, SEQ, ROWS, 512), bf16),
        vmem((2, SEQ, ROWS, 512), bf16),
        sem((2, 8)),
        sem((10,)),
        sem((2,)),
        sem((2,)),
        sem,
        sem,
        sem((GROUPS,)),
        sem((N_SP,)),
        sem((N_SP,)),
        sem((GROUPS,)),
        sem((2,)),
        sem((2,)),
        sem((2,)),
        sem,
        sem,
        pltpu.SemaphoreType.REGULAR,
        pltpu.SemaphoreType.REGULAR,
    ]
    own, arrived = pl.pallas_call(
        kernel,
        out_shape=[jax.ShapeDtypeStruct((SEQ, ROWS, HALF), bf16)] * 2,
        in_specs=[pl.BlockSpec(memory_space=pl.ANY)] * 18,
        out_specs=[pl.BlockSpec(memory_space=pl.ANY)] * 2,
        scratch_shapes=scratch,
        compiler_params=pltpu.CompilerParams(
            collective_id=0, has_side_effects=True, vmem_limit_bytes=56 << 20
        ),
        name="layer",
    )(
        tokens, row(norm_gain), w_recept, w_key, w_value, w_decay, w_rate, w_gate_rec, w_pool,
        w_gate_pool, tile(decay_base), tile(rate_base), tile(head_gain), pool_mix, row(pool_scale),
        w_out_rec, w_out_pool, init_state,
    )
    return (own.astype(f32) + arrived.astype(f32)).astype(bf16)


def solution(mesh):
    split = P(None, "tp")
    placed = (
        P("fs", "sp", "tp"), P(),
        split, split, split, split, split, split, split, split,
        P(), P(), P(), P(), P(),
        P("tp", None), P("tp", None), P("fs", "tp", None, None),
    )
    return jax.shard_map(
        shards, mesh=mesh, in_specs=placed, out_specs=P("fs", "sp", "tp"), check_vma=False
    )
```

```python
import math

import jax
import jax.numpy as jnp
from jax import lax
from jax.experimental import pallas as pl
from jax.experimental.pallas import tpu as pltpu
from jax.sharding import PartitionSpec as P

D = 2048
HALF = 1024
SEQ = 2
ROWS = 128
TOK = SEQ * ROWS
RCOLS = 384
PCOLS = 256
PAIRS = 3
GROUPS = SEQ * PAIRS
HD = 64
N_SP = 16
COLS = 6 * RCOLS + 2 * PCOLS
OFFS = (1536, 0, 1152, 384, 768, 1920, 2304, 2560)
NEED = (1, 3, 4, 2, 0, 5, 6, 7)
EARLY = 4 * RCOLS
WIDTHS = (384, 384, 384, 384, 384, 384, 256, 256)
MESH = pl.DeviceIdType.MESH
f32 = jnp.float32
bf16 = jnp.bfloat16


def dot(a, b):
    return lax.dot_general(a, b, (((1,), (0,)), ((), ())), preferred_element_type=f32)


def dot_nt(a, b):
    return lax.dot_general(a, b, (((1,), (1,)), ((), ())), preferred_element_type=f32)


def dot_tn(a, b):
    return lax.dot_general(a, b, (((0,), (0,)), ((), ())), preferred_element_type=f32)


def split2(x):
    hi = x.astype(bf16)
    return hi, (x - hi.astype(f32)).astype(bf16)


def cat(parts, axis):
    return jnp.concatenate(parts, axis=axis)


def sig(x):
    e = jnp.exp(-jnp.abs(x))
    return jnp.where(x >= 0, 1.0, e) / (1.0 + e)


def lane_first(shape):
    return lax.broadcasted_iota(jnp.int32, shape, len(shape) - 1) < HD


def keep(x, head):
    first = lane_first(x.shape)
    zero = jnp.zeros_like(x)
    return jnp.where(first, x, zero) if head == 0 else jnp.where(first, zero, x)


def two_heads(x):
    return cat([keep(x, 0), keep(x, 1)], 0)


def block_ones():
    i = lax.broadcasted_iota(jnp.int32, (128, 128), 0) < HD
    j = lax.broadcasted_iota(jnp.int32, (128, 128), 1) < HD
    return jnp.where(i == j, 1.0, 0.0).astype(bf16)


def head_sums(x, ones2):
    hi, lo = split2(x)
    return dot(cat([hi, lo], 1), ones2)


def prepare(k, d_in, a_in, d_base, a_base):
    ones = block_ones()
    ones2 = cat([ones, ones], 0)
    x = d_base + d_in
    log_decay = -math.exp(-0.5) * sig(x)
    rate = sig(a_base + a_in)
    squares = k * k
    sums = cat([head_sums(squares[:, o : o + 128], ones2) for o in range(0, RCOLS, 128)], 1)
    unit = k * lax.rsqrt(sums + 1.0)
    removal = unit * rate
    i = lax.broadcasted_iota(jnp.int32, (128, 128), 0)
    j = lax.broadcasted_iota(jnp.int32, (128, 128), 1)
    tri = jnp.where(i >= j, 1.0, 0.0).astype(bf16)
    hi, lo = split2(log_decay)
    rest = (log_decay - hi.astype(f32) - lo.astype(f32)).astype(bf16)
    cum = dot(cat([tri, tri, tri], 1), cat([hi, lo, rest], 0))
    mid = cum[63:64, :]
    last = cum[127:128, :]
    shrink = jnp.exp(cum - mid)
    grow = jnp.exp(mid - cum)
    alpha = jnp.exp(cum - log_decay - mid) * unit
    beta = removal * grow
    kappa = k * grow
    return alpha, shrink, beta, kappa, jnp.exp(mid), jnp.exp(last - mid), jnp.exp(last)


def pair_products(x, y_hi, y_lo):
    parts = [split2(keep(x, head)) for head in (0, 1)]
    lhs = cat([cat([hi, lo], 1) for hi, lo in parts], 0)
    return dot(lhs, cat([y_hi, y_hi], 0)) + dot(lhs[:, :128], y_lo)


def pick(x):
    first = (lax.broadcasted_iota(jnp.int32, (128, x.shape[1]), 1) & 127) < HD
    return jnp.where(first, x[:128], x[128:])


def inverses(lowers):
    i = lax.broadcasted_iota(jnp.int32, (128, 128), 0)
    j = lax.broadcasted_iota(jnp.int32, (128, 128), 1)
    apart = i ^ j
    eye = jnp.where(i == j, 1.0, 0.0)
    zero = jnp.zeros((128, 128), bf16)
    inv = [eye - jnp.where(apart == 1, low, zero).astype(f32) for low in lowers]
    for size in (2, 8, 32):
        inside = (apart >= size) & (apart < 4 * size)
        inv_b = [x.astype(bf16) for x in inv]
        hop = [
            dot(x, jnp.where(inside, low, zero)).astype(bf16) for x, low in zip(inv_b, lowers)
        ]
        both = [dot(h, cat([h, x], 1)) for h, x in zip(hop, inv_b)]
        once = [x - y[:, 128:] for x, y in zip(inv, both)]
        inv = [x + dot(y[:, :128].astype(bf16), x.astype(bf16)) for x, y in zip(once, both)]
    return [x.astype(bf16) for x in inv]


def solve_all(invs, lows, sides):
    first = [pick(dot(inv, side.astype(bf16))).astype(bf16) for inv, side in zip(invs, sides)]
    back = [pick(dot(low, x)) for low, x in zip(lows, first)]
    miss = [
        (side - x.astype(f32) - y).astype(bf16) for side, x, y in zip(sides, first, back)
    ]
    return [x.astype(f32) + pick(dot(inv, m)) for x, inv, m in zip(first, invs, miss)]


def maps_of(z, value, beta_end, kappa_end, gain_end):
    zero = jnp.zeros((128, 128), bf16)
    lhs = cat([z.astype(bf16), cat([zero, -value], 1)], 0)
    both = dot_tn(lhs, cat([beta_end, kappa_end], 0).astype(bf16))
    first = lane_first((64, 128))
    packed = [
        jnp.where(first, both[o : o + 64], both[o + 64 : o + 128]) for o in (0, 128)
    ]
    i = lax.broadcasted_iota(jnp.int32, (64, 128), 0)
    j = lax.broadcasted_iota(jnp.int32, (64, 128), 1) & 63
    transit = jnp.where(i == j, gain_end, 0.0) - packed[0]
    return transit.astype(bf16), (-packed[1]).astype(bf16)


def after_given(state, transit):
    both = dot(cat(split2(state), 0), two_heads(transit))
    return both[:HD] + both[HD:]


def state_reads(reads, state):
    both = dot_nt(cat(split2(reads), 0), two_heads(state))
    return both[:128] + both[128:]


def head_mean(x):
    ones = block_ones()
    ones2 = cat([ones, ones], 0)
    parts = [head_sums(x[:, o : o + 128], ones2) for o in range(0, x.shape[1], 128)]
    return cat(parts, 1) * (1.0 / HD)


def kernel(
    tok, gain, wr, wk, wv, wd, wa, wg, wp, wgp, dbase, rbase, hgain, mix, pscale, wor, wop, init,
    own_out, arrived_out,
    tok_v, gain_v, weight_v, acc_v, proj_v, norm_v, square_v, base_v, mix_v, pscale_v, wout_v, init_v, init_in,
    scale_v, pool_v, keys_v, turn_v, low_v, side_v, z_v, reads_v, local_v, map_v, maps_in,
    gate_v, state_v, states_in, merged_v, recout_v, part_v,
    w_sem, small_sem, tok_send, tok_recv, halo_send, halo_recv, map_send, map_recv,
    st_send, st_recv, part_send, part_recv, init_send, init_recv, pair_sem, go_sem,
):
    sp = lax.axis_index("sp")
    tp = lax.axis_index("tp")
    other = 1 - tp
    weights = (wr, wk, wv, wd, wa, wg, wp, wgp)
    group_of = lax.div(sp, 2)
    side = lax.rem(sp, 2)
    is_owner = (tp == 1) & (sp < 2 * GROUPS)
    gives_init = (tp == 0) & (side == 0) & (sp < 2 * GROUPS)
    keeps_init = (tp == 1) & (side == 1) & (sp < 2 * GROUPS)

    barrier = pltpu.get_barrier_semaphore()

    def tell(semaphore, **device):
        pl.semaphore_signal(semaphore, inc=1, device_id=device, device_id_type=MESH)

    @pl.when(tp == 1)
    def _():
        tell(barrier, tp=other)

    mine = pl.multiple_of(tp * HALF, HALF)
    theirs = pl.multiple_of(other * HALF, HALF)
    pool_at = pl.multiple_of(tp * PCOLS, 128)
    held = jnp.minimum(group_of, GROUPS - 1)
    small = [
        pltpu.make_async_copy(tok, tok_v, small_sem.at[0]),
        pltpu.make_async_copy(gain.at[:, pl.ds(mine, HALF)], gain_v, small_sem.at[1]),
        pltpu.make_async_copy(dbase, base_v.at[0], small_sem.at[2]),
        pltpu.make_async_copy(rbase, base_v.at[1], small_sem.at[3]),
        pltpu.make_async_copy(hgain, base_v.at[2], small_sem.at[4]),
        pltpu.make_async_copy(mix.at[pl.ds(tp * 2, 2)], mix_v, small_sem.at[5]),
        pltpu.make_async_copy(pscale.at[:, pl.ds(pool_at, PCOLS)], pscale_v, small_sem.at[6]),
        pltpu.make_async_copy(
            init.at[lax.div(held, PAIRS), pl.ds(2 * lax.rem(held, PAIRS), 2)],
            init_v,
            small_sem.at[7],
        ),
        pltpu.make_async_copy(wor, wout_v.at[pl.ds(0, RCOLS)], small_sem.at[8]),
        pltpu.make_async_copy(wop, wout_v.at[pl.ds(RCOLS, PCOLS)], small_sem.at[9]),
    ]
    loads = [
        [
            pltpu.make_async_copy(
                w.at[pl.ds(at, HALF)],
                weight_v.at[half, :, pl.ds(OFFS[i], WIDTHS[i])],
                w_sem.at[half, i],
            )
            for i, w in ((i, weights[i]) for i in NEED)
        ]
        for half, at in ((0, mine), (1, theirs))
    ]
    def start(copies):
        for copy in copies:
            copy.start()

    start(small[:2])
    start(loads[0][:2])

    small[0].wait()

    @pl.when(tp == 0)
    def _():
        pl.semaphore_wait(barrier, 1)
        tell(pair_sem, tp=other)

    start(loads[0][2:4] + loads[1][:4] + small[2:4])
    small[1].wait()
    wide = tok_v[...].reshape(TOK, HALF).astype(f32)
    norm_v[0] = (wide * gain_v[...]).astype(bf16)
    squares = wide * wide
    square_v[0] = sum(squares[:, o : o + 128] for o in range(0, HALF, 128))

    @pl.when(tp == 1)
    def _():
        pl.semaphore_wait(pair_sem, 1)

        @pl.loop(1, N_SP)
        def _(step):
            tell(barrier, sp=lax.rem(sp + step, N_SP))

    send_tok = [
        pltpu.make_async_remote_copy(
            src_ref=ref.at[0],
            dst_ref=ref.at[1],
            send_sem=tok_send.at[i],
            recv_sem=tok_recv.at[i],
            device_id={"tp": other},
            device_id_type=MESH,
        )
        for i, ref in enumerate((norm_v, square_v))
    ]
    start(send_tok)
    early = (slice(0, EARLY // 2), slice(EARLY // 2, EARLY))
    for step, at in enumerate(early):
        for copy in loads[0][2 * step : 2 * step + 2]:
            copy.wait()
        acc_v[:, at] = dot(norm_v[0], weight_v[0, :, at])
        if step == 0:
            start(loads[0][4:] + loads[1][4:] + small[4:])

    send_tok[0].wait_recv()

    def scaled(total):
        return (total * cat([scale_v[...]] * (total.shape[1] // 128), 1)).astype(bf16)

    for step, at in enumerate(early):
        for copy in loads[1][2 * step : 2 * step + 2]:
            copy.wait()
        total = acc_v[:, at] + dot(norm_v[1], weight_v[1, :, at])
        if step == 0:
            send_tok[1].wait_recv()
            squares = jnp.sum(square_v[0] + square_v[1], axis=1, keepdims=True)
            scale = lax.rsqrt(squares * (1.0 / D) + 0.25)
            scale_v[...] = jnp.broadcast_to(scale, (TOK, 128))
        proj_v[:, at] = scaled(total)

    for copy in small[2:4]:
        copy.wait()
    groups = [(b, p) for b in range(SEQ) for p in range(PAIRS)]

    def part(index, b, p):
        at = OFFS[index] + 128 * p
        return proj_v[b * ROWS : (b + 1) * ROWS, at : at + 128]

    row = lax.broadcasted_iota(jnp.int32, (256, 128), 0) & 127
    col = lax.broadcasted_iota(jnp.int32, (256, 128), 1)
    strict = row > col
    inclusive = row >= col

    def rows_of(index, b):
        at = OFFS[index]
        return proj_v[b * ROWS : (b + 1) * ROWS, at : at + WIDTHS[index]].astype(f32)

    def local_row(index):
        return cat([base_v[index, pl.ds(3 * tp + p, 1), :] for p in range(PAIRS)], 1)

    ends = []
    for b in range(SEQ):
        alpha, shrink, beta, kappa, e_mid, e_tail, e_last = prepare(
            rows_of(1, b), rows_of(3, b), rows_of(4, b), local_row(0), local_row(1)
        )
        keys_v[b, 0] = alpha
        keys_v[b, 1] = shrink
        keys_v[b, 2] = beta
        keys_v[b, 3] = kappa
        ends.append((e_mid, e_tail, e_last))

    def pair_of(index, g):
        b, p = groups[g]
        return keys_v[b, index, :, 128 * p : 128 * p + 128]

    def end_of(index, g):
        b, p = groups[g]
        return ends[b][index][:, 128 * p : 128 * p + 128]

    every = range(GROUPS)
    for g in every:
        turned = cat([pair_of(2, g).T, pair_of(3, g).T], 1)
        y_hi, y_lo = split2(turned)
        turn_v[g, 0] = y_hi
        turn_v[g, 1] = y_lo
        pairs = pair_products(pair_of(0, g), y_hi, y_lo)
        low_v[g] = jnp.where(strict, pairs[:, :128], 0.0).astype(bf16)
        cross = jnp.where(strict, pairs[:, 128:], 0.0).astype(bf16)
        side_v[g, :, :128] = pair_of(0, g) * end_of(0, g)
        side_v[g, :, 128:] = pick(dot(cross, part(2, *groups[g])))
    @pl.when(tp == 1)
    def _():
        pl.semaphore_wait(barrier, N_SP - 1)
        tell(go_sem, tp=other)

    by_head = inverses([low_v[g, 128 * h : 128 * h + 128, :] for g in every for h in (0, 1)])
    invs = [cat(by_head[2 * g : 2 * g + 2], 0) for g in every]
    map_copies = []
    solved = solve_all(invs, [low_v[g] for g in every], [side_v[g] for g in every])
    for g, z in zip(every, solved):
        z_v[g] = z.astype(bf16)
        tail = end_of(1, g)
        transit, written = maps_of(
            z, part(2, *groups[g]), pair_of(2, g) * tail, pair_of(3, g) * tail, end_of(2, g)
        )
        map_v[g, 0] = transit
        map_v[g, 1] = written
    @pl.when(tp == 0)
    def _():
        pl.semaphore_wait(go_sem, 1)

    own_map = [(tp == 1) & (sp == 2 * g + 1) for g in every]
    for g in every:
        copy = pltpu.make_async_remote_copy(
            src_ref=map_v.at[g],
            dst_ref=maps_in.at[sp],
            send_sem=map_send.at[g],
            recv_sem=map_recv.at[sp],
            device_id={"sp": 2 * g + tp, "tp": 1},
            device_id_type=MESH,
        )
        map_copies.append(copy)

        @pl.when(jnp.logical_not(own_map[g]) & (sp < N_SP - 1))
        def _():
            copy.start()

        @pl.when(own_map[g])
        def _():
            pltpu.make_async_copy(map_v.at[g], maps_in.at[sp], map_recv.at[sp]).start()

    def late(index, copies, at):
        for half in (0, 1):
            for copy in loads[half][copies]:
                copy.wait()
        total = dot(norm_v[0], weight_v[0, :, at]) + dot(norm_v[1], weight_v[1, :, at])
        proj_v[:, at] = scaled(total)

    late(6, slice(6, 8), slice(OFFS[6], COLS))
    for b in range(SEQ):
        pool_v[b, 16:, :] = proj_v[b * ROWS : (b + 1) * ROWS, OFFS[6] : OFFS[7]]
    halo = pltpu.make_async_remote_copy(
        src_ref=pool_v.at[:, pl.ds(ROWS, 16), :],
        dst_ref=pool_v.at[:, pl.ds(0, 16), :],
        send_sem=halo_send,
        recv_sem=halo_recv,
        device_id={"sp": lax.rem(sp + 1, N_SP)},
        device_id_type=MESH,
    )

    @pl.when(sp < N_SP - 1)
    def _():
        halo.start()

    @pl.when(sp == 0)
    def _():
        pool_v[:, 0:16, :] = jnp.zeros((SEQ, 16, PCOLS), bf16)

    late(0, slice(4, 5), slice(OFFS[0], OFFS[5]))
    for g in every:
        rho = part(0, *groups[g]).astype(f32) * pair_of(1, g)
        pairs = pair_products(rho, turn_v[g, 0], turn_v[g, 1])
        within_beta = jnp.where(inclusive, pairs[:, :128], 0.0).astype(bf16)
        within_kappa = jnp.where(inclusive, pairs[:, 128:], 0.0).astype(bf16)
        drop = pick(dot(within_beta, z_v[g]))
        reads_v[g] = rho * end_of(0, g) - drop[:, :128]
        local = pick(dot(within_kappa, part(2, *groups[g]))) - drop[:, 128:]
        local_v[g] = local - head_mean(local)
    def send_state(j):
        return pltpu.make_async_remote_copy(
            src_ref=state_v.at[j],
            dst_ref=states_in.at[group_of],
            send_sem=st_send.at[j],
            recv_sem=st_recv.at[group_of],
            device_id={"sp": j, "tp": side},
            device_id_type=MESH,
        )

    def wait_map(j):
        pltpu.make_async_copy(map_v.at[0], maps_in.at[j], map_recv.at[j]).wait()

    def centred(state):
        return (state - jnp.mean(state, axis=0, keepdims=True)).astype(bf16)

    small[7].wait()
    give = pltpu.make_async_remote_copy(
        src_ref=init_v,
        dst_ref=init_in,
        send_sem=init_send,
        recv_sem=init_recv,
        device_id={"tp": other},
        device_id_type=MESH,
    )

    @pl.when(gives_init)
    def _():
        give.start()

    @pl.when(keeps_init)
    def _():
        pltpu.make_async_copy(init_v, init_in, init_recv).start()

    @pl.when(is_owner)
    def _():
        pltpu.make_async_copy(init_v, init_in, init_recv).wait()
        state = cat([init_in[0], init_in[1]], 1)
        def emit(j):
            @pl.when((j != sp) | (side == 0))
            def _():
                send_state(j).start()

            @pl.when((j == sp) & (side == 1))
            def _():
                pltpu.make_async_copy(
                    state_v.at[j], states_in.at[group_of], st_recv.at[group_of]
                ).start()

        state_v[0] = centred(state)
        emit(0)
        for block in (range(0, 4), range(4, 8), range(8, 12), range(12, 14), range(14, 15)):
            for j in block:
                wait_map(j)
            for j in block:
                state = after_given(state, maps_in[j, 0]) + maps_in[j, 1].astype(f32)
                state_v[j + 1] = centred(state)
            for j in block:
                emit(j + 1)

    late(5, slice(5, 6), slice(OFFS[5], OFFS[6]))
    for copy in small[4:7] + small[8:]:
        copy.wait()
    for b in range(SEQ):
        gate = rows_of(5, b)
        gate_v[b] = local_row(2) * (gate * sig(gate))

    @pl.when(sp > 0)
    def _():
        halo.wait_recv()

    places = (sp * ROWS + 1 + lax.broadcasted_iota(jnp.int32, (ROWS, 128), 0)).astype(f32)
    for b in range(SEQ):
        outs = []
        for s in range(2):
            at = slice(128 * s, 128 * s + 128)
            own = pool_v[b, :, at].astype(f32)
            total = own + pltpu.roll(own, 1, 0)
            if s == 1:
                total = total + pltpu.roll(total, 2, 0)
            wide = total + pltpu.roll(total, 2 if s == 0 else 4, 0)
            wide = wide + pltpu.roll(wide, 4 if s == 0 else 8, 0)
            trail = jnp.where(tp == 0, total, wide)[16:]
            window = jnp.where(tp == 0, float(2 << s), float(8 << s))
            diff = (trail / jnp.minimum(places, window) - own[16:]).astype(bf16)
            pooled = dot(diff, mix_v[s])
            gate = proj_v[b * ROWS : (b + 1) * ROWS, OFFS[7] + 128 * s : OFFS[7] + 128 * s + 128]
            gate = gate.astype(f32)
            outs.append((pooled * pscale_v[:, at] * (gate * sig(gate))).astype(bf16))
        recout_v[b * ROWS : (b + 1) * ROWS, RCOLS:] = cat(outs, 1)

    for at in (slice(0, 1024), slice(1024, D)):
        merged_v[:, at] = dot(recout_v[:, RCOLS:], wout_v[RCOLS:, at])

    for g in every:
        pltpu.make_async_copy(state_v.at[0], states_in.at[g], st_recv.at[g]).wait()
    centre = [state_reads(reads_v[g], states_in[g]) + local_v[g] for g in every]
    for b in range(SEQ):
        rec = cat(centre[PAIRS * b : PAIRS * b + PAIRS], 1)
        spread = head_mean(rec * rec)
        recout_v[b * ROWS : (b + 1) * ROWS, :RCOLS] = (
            rec * lax.rsqrt(spread + 1.0) * gate_v[b]
        ).astype(bf16)

    def product(at):
        total = merged_v[:, at] + dot(recout_v[:, :RCOLS], wout_v[:RCOLS, at])
        return total.astype(bf16).reshape(SEQ, ROWS, 512)

    def columns(ref, tile):
        return ref.at[:, :, pl.ds(512 * tile, 512)]

    def send_part(tile):
        return pltpu.make_async_remote_copy(
            src_ref=part_v.at[tile],
            dst_ref=columns(arrived_out, tile),
            send_sem=part_send.at[tile],
            recv_sem=part_recv.at[tile],
            device_id={"tp": other},
            device_id_type=MESH,
        )

    for tile in range(2):
        part_v[tile] = product(pl.ds(pl.multiple_of(theirs + tile * 512, 512), 512))
        send_part(tile).start()
    for tile in range(2):
        at = pl.ds(pl.multiple_of(mine + tile * 512, 512), 512)
        own_out[:, :, 512 * tile : 512 * tile + 512] = product(at)

    for copy in send_tok:
        copy.wait_send()

    @pl.when(sp < N_SP - 1)
    def _():
        halo.wait_send()

    for g, copy in enumerate(map_copies):
        @pl.when(jnp.logical_not(own_map[g]) & (sp < N_SP - 1))
        def _():
            copy.wait_send()

    @pl.when(gives_init)
    def _():
        give.wait_send()

    @pl.when(is_owner)
    def _():
        @pl.loop(0, N_SP)
        def _(j):
            @pl.when((j != sp) | (side == 0))
            def _():
                send_state(j).wait_send()

    for tile in range(2):
        send_part(tile).wait()


def shards(
    tokens, norm_gain, w_recept, w_key, w_value, w_decay, w_rate, w_gate_rec, w_pool, w_gate_pool,
    decay_base, rate_base, head_gain, pool_mix, pool_scale, w_out_rec, w_out_pool, init_state,
):
    vmem, sem = pltpu.VMEM, pltpu.SemaphoreType.DMA
    row = lambda x: x.reshape(1, -1)
    tile = lambda x: x.reshape(6, 128)
    scratch = [
        vmem((SEQ, ROWS, HALF), bf16),
        vmem((1, HALF), f32),
        vmem((2, HALF, COLS), bf16),
        vmem((TOK, EARLY), f32),
        vmem((TOK, COLS), bf16),
        vmem((2, TOK, HALF), bf16),
        vmem((2, TOK, 128), f32),
        vmem((3, 6, 128), f32),
        vmem((2, 128, 128), bf16),
        vmem((1, PCOLS), f32),
        vmem((RCOLS + PCOLS, D), bf16),
        vmem((2, HD, HD), f32),
        vmem((2, HD, HD), f32),
        vmem((TOK, 128), f32),
        vmem((SEQ, 16 + ROWS, PCOLS), bf16),
        vmem((SEQ, 4, ROWS, RCOLS), f32),
        vmem((GROUPS, 2, 128, 256), bf16),
        vmem((GROUPS, 256, 128), bf16),
        vmem((GROUPS, 128, 256), f32),
        vmem((GROUPS, 128, 256), bf16),
        vmem((GROUPS, 128, 128), f32),
        vmem((GROUPS, 128, 128), f32),
        vmem((GROUPS, 2, HD, 128), bf16),
        vmem((N_SP, 2, HD, 128), bf16),
        vmem((SEQ, ROWS, RCOLS), f32),
        vmem((N_SP, HD, 128), bf16),
        vmem((GROUPS, HD, 128), bf16),
        vmem((TOK, D), f32),
        vmem((TOK, RCOLS + PCOLS), bf16),
        vmem((2, SEQ, ROWS, 512), bf16),
        sem((2, 8)),
        sem((10,)),
        sem((2,)),
        sem((2,)),
        sem,
        sem,
        sem((GROUPS,)),
        sem((N_SP,)),
        sem((N_SP,)),
        sem((GROUPS,)),
        sem((2,)),
        sem((2,)),
        sem,
        sem,
        pltpu.SemaphoreType.REGULAR,
        pltpu.SemaphoreType.REGULAR,
    ]
    pin = lambda x: pltpu.with_memory_space_constraint(x, pltpu.HBM)
    own, arrived = pl.pallas_call(
        kernel,
        out_shape=[jax.ShapeDtypeStruct((SEQ, ROWS, HALF), bf16)] * 2,
        in_specs=[pl.BlockSpec(memory_space=pl.ANY)] * 18,
        out_specs=[pl.BlockSpec(memory_space=pltpu.VMEM)] * 2,
        scratch_shapes=scratch,
        compiler_params=pltpu.CompilerParams(
            collective_id=0, has_side_effects=True, vmem_limit_bytes=48 << 20
        ),
        name="layer",
    )(*(pin(x) for x in (
        tokens, row(norm_gain), w_recept, w_key, w_value, w_decay, w_rate, w_gate_rec, w_pool,
        w_gate_pool, tile(decay_base), tile(rate_base), tile(head_gain), pool_mix, row(pool_scale),
        w_out_rec, w_out_pool, init_state,
    )))
    return (own.astype(f32) + arrived.astype(f32)).astype(bf16)


def solution(mesh):
    split = P(None, "tp")
    placed = (
        P("fs", "sp", "tp"), P(),
        split, split, split, split, split, split, split, split,
        P(), P(), P(), P(), P(),
        P("tp", None), P("tp", None), P("fs", "tp", None, None),
    )
    return jax.shard_map(
        shards, mesh=mesh, in_specs=placed, out_specs=P("fs", "sp", "tp"), check_vma=False
    )
```

```python
import math

import jax
import jax.numpy as jnp
from jax import lax
from jax.experimental import pallas as pl
from jax.experimental.pallas import tpu as pltpu
from jax.sharding import PartitionSpec as P

D = 2048
HALF = 1024
SEQ = 2
ROWS = 128
TOK = SEQ * ROWS
RCOLS = 384
PCOLS = 256
PAIRS = 3
GROUPS = SEQ * PAIRS
HD = 64
N_SP = 16
COLS = 6 * RCOLS + 2 * PCOLS
OFFS = (1536, 0, 1152, 384, 768, 1920, 2304, 2560)
NEED = (1, 3, 4, 2, 0, 5, 6, 7)
EARLY = 4 * RCOLS
WIDTHS = (384, 384, 384, 384, 384, 384, 256, 256)
MESH = pl.DeviceIdType.MESH
f32 = jnp.float32
bf16 = jnp.bfloat16


def dot(a, b):
    return lax.dot_general(a, b, (((1,), (0,)), ((), ())), preferred_element_type=f32)


def dot_nt(a, b):
    return lax.dot_general(a, b, (((1,), (1,)), ((), ())), preferred_element_type=f32)


def dot_tn(a, b):
    return lax.dot_general(a, b, (((0,), (0,)), ((), ())), preferred_element_type=f32)


def split2(x):
    hi = x.astype(bf16)
    return hi, (x - hi.astype(f32)).astype(bf16)


def cat(parts, axis):
    return jnp.concatenate(parts, axis=axis)


def sig(x):
    e = jnp.exp(-jnp.abs(x))
    return jnp.where(x >= 0, 1.0, e) / (1.0 + e)


def lane_first(shape):
    return lax.broadcasted_iota(jnp.int32, shape, len(shape) - 1) < HD


def keep(x, head):
    first = lane_first(x.shape)
    zero = jnp.zeros_like(x)
    return jnp.where(first, x, zero) if head == 0 else jnp.where(first, zero, x)


def two_heads(x):
    return cat([keep(x, 0), keep(x, 1)], 0)


def block_ones():
    i = lax.broadcasted_iota(jnp.int32, (128, 128), 0) < HD
    j = lax.broadcasted_iota(jnp.int32, (128, 128), 1) < HD
    return jnp.where(i == j, 1.0, 0.0).astype(bf16)


def head_sums(x, ones2):
    hi, lo = split2(x)
    return dot(cat([hi, lo], 1), ones2)


def prepare(k, d_in, a_in, d_base, a_base):
    ones = block_ones()
    ones2 = cat([ones, ones], 0)
    x = d_base + d_in
    log_decay = -math.exp(-0.5) * sig(x)
    rate = sig(a_base + a_in)
    squares = k * k
    sums = cat([head_sums(squares[:, o : o + 128], ones2) for o in range(0, RCOLS, 128)], 1)
    unit = k * lax.rsqrt(sums + 1.0)
    removal = unit * rate
    i = lax.broadcasted_iota(jnp.int32, (128, 128), 0)
    j = lax.broadcasted_iota(jnp.int32, (128, 128), 1)
    tri = jnp.where(i >= j, 1.0, 0.0).astype(bf16)
    hi, lo = split2(log_decay)
    rest = (log_decay - hi.astype(f32) - lo.astype(f32)).astype(bf16)
    cum = dot(cat([tri, tri, tri], 1), cat([hi, lo, rest], 0))
    mid = cum[63:64, :]
    last = cum[127:128, :]
    shrink = jnp.exp(cum - mid)
    grow = jnp.exp(mid - cum)
    alpha = jnp.exp(cum - log_decay - mid) * unit
    beta = removal * grow
    kappa = k * grow
    return alpha, shrink, beta, kappa, jnp.exp(mid), jnp.exp(last - mid), jnp.exp(last)


def pair_products(x, turned):
    parts = [split2(keep(x, head)) for head in (0, 1)]
    lhs = cat([cat([hi, lo], 1) for hi, lo in parts], 0)
    return dot(lhs, cat([turned, turned], 0))


def pick(x):
    first = (lax.broadcasted_iota(jnp.int32, (128, x.shape[1]), 1) & 127) < HD
    return jnp.where(first, x[:128], x[128:])


def inverses(lowers):
    i = lax.broadcasted_iota(jnp.int32, (128, 128), 0)
    j = lax.broadcasted_iota(jnp.int32, (128, 128), 1)
    apart = i ^ j
    same = apart < 32
    zero = jnp.zeros((128, 128), bf16)

    def packed(x):
        return (x[:32] + x[32:64]) + (x[64:96] + x[96:])

    def spread(x):
        return jnp.where(same, cat([x] * 4, 0), jnp.zeros((128, 128), x.dtype))

    eye = packed(jnp.where(i == j, 1.0, 0.0))
    inv = [eye - packed(jnp.where(apart == 1, low, zero).astype(f32)) for low in lowers]
    for size in (2, 8):
        inside = (apart >= size) & (apart < 4 * size)
        inv_b = [x.astype(bf16) for x in inv]
        hop = [
            dot(x, jnp.where(inside, low, zero)).astype(bf16) for x, low in zip(inv_b, lowers)
        ]
        both = [dot(h, cat([spread(h), spread(x)], 1)) for h, x in zip(hop, inv_b)]
        once = [x - y[:, 128:] for x, y in zip(inv, both)]
        inv = [
            x + dot(y[:, :128].astype(bf16), spread(x.astype(bf16))) for x, y in zip(once, both)
        ]
    inv = [spread(x) for x in inv]
    inv_b = [x.astype(bf16) for x in inv]
    outside = apart >= 32
    top = jnp.zeros((32, 128), bf16)
    hop = [
        dot(x[32:], jnp.where(outside, low, zero)).astype(bf16) for x, low in zip(inv_b, lowers)
    ]
    both = [dot(h, cat([cat([top, h], 0), x], 1)) for h, x in zip(hop, inv_b)]
    once = [cat([x[:32], x[32:] - y[:, 128:]], 0) for x, y in zip(inv, both)]
    last = [dot(y[32:, :128].astype(bf16), x.astype(bf16)) for x, y in zip(once, both)]
    return [cat([x[:64], x[64:] + y], 0).astype(bf16) for x, y in zip(once, last)]


def solve_all(invs, lows, sides):
    first = [pick(dot(inv, side.astype(bf16))).astype(bf16) for inv, side in zip(invs, sides)]
    back = [pick(dot(low, x)) for low, x in zip(lows, first)]
    miss = [
        (side - x.astype(f32) - y).astype(bf16) for side, x, y in zip(sides, first, back)
    ]
    return [x.astype(f32) + pick(dot(inv, m)) for x, inv, m in zip(first, invs, miss)]


def maps_of(z, value, beta_end, kappa_end, gain_end):
    zero = jnp.zeros((128, 128), bf16)
    lhs = cat([z.astype(bf16), cat([zero, -value], 1)], 0)
    both = dot_tn(lhs, cat([beta_end, kappa_end], 0).astype(bf16))
    first = lane_first((64, 128))
    packed = [
        jnp.where(first, both[o : o + 64], both[o + 64 : o + 128]) for o in (0, 128)
    ]
    i = lax.broadcasted_iota(jnp.int32, (64, 128), 0)
    j = lax.broadcasted_iota(jnp.int32, (64, 128), 1) & 63
    transit = jnp.where(i == j, gain_end, 0.0) - packed[0]
    return transit.astype(bf16), (-packed[1]).astype(bf16)


def after_given(state, transit):
    both = dot(cat(split2(state), 0), two_heads(transit))
    return both[:HD] + both[HD:]


def state_reads(reads, state):
    both = dot_nt(cat(split2(reads), 0), two_heads(state))
    return both[:128] + both[128:]


def head_mean(x):
    ones = block_ones()
    ones2 = cat([ones, ones], 0)
    parts = [head_sums(x[:, o : o + 128], ones2) for o in range(0, x.shape[1], 128)]
    return cat(parts, 1) * (1.0 / HD)


def kernel(
    tok, gain, wr, wk, wv, wd, wa, wg, wp, wgp, dbase, rbase, hgain, mix, pscale, wor, wop, init,
    own_out, arrived_out,
    tok_v, gain_v, weight_v, acc_v, proj_v, norm_v, square_v, base_v, mix_v, pscale_v, wout_v, init_v, init_in,
    scale_v, pool_v, keys_v, turn_v, low_v, side_v, z_v, reads_v, local_v, map_v, maps_in,
    gate_v, state_v, states_in, merged_v, recout_v, part_v,
    w_sem, small_sem, tok_send, tok_recv, halo_send, halo_recv, map_send, map_recv,
    st_send, st_recv, part_send, part_recv, init_send, init_recv, pair_sem, go_sem,
):
    sp = lax.axis_index("sp")
    tp = lax.axis_index("tp")
    other = 1 - tp
    weights = (wr, wk, wv, wd, wa, wg, wp, wgp)
    group_of = lax.div(sp, 2)
    side = lax.rem(sp, 2)
    is_owner = (tp == 1) & (sp < 2 * GROUPS)
    gives_init = (tp == 0) & (side == 0) & (sp < 2 * GROUPS)
    keeps_init = (tp == 1) & (side == 1) & (sp < 2 * GROUPS)

    barrier = pltpu.get_barrier_semaphore()

    def tell(semaphore, **device):
        pl.semaphore_signal(semaphore, inc=1, device_id=device, device_id_type=MESH)

    @pl.when(tp == 1)
    def _():
        tell(barrier, tp=other)

    mine = pl.multiple_of(tp * HALF, HALF)
    theirs = pl.multiple_of(other * HALF, HALF)
    pool_at = pl.multiple_of(tp * PCOLS, 128)
    held = jnp.minimum(group_of, GROUPS - 1)
    small = [
        pltpu.make_async_copy(tok, tok_v, small_sem.at[0]),
        pltpu.make_async_copy(gain.at[:, pl.ds(mine, HALF)], gain_v, small_sem.at[1]),
        pltpu.make_async_copy(dbase, base_v.at[0], small_sem.at[2]),
        pltpu.make_async_copy(rbase, base_v.at[1], small_sem.at[3]),
        pltpu.make_async_copy(hgain, base_v.at[2], small_sem.at[4]),
        pltpu.make_async_copy(mix.at[pl.ds(tp * 2, 2)], mix_v, small_sem.at[5]),
        pltpu.make_async_copy(pscale.at[:, pl.ds(pool_at, PCOLS)], pscale_v, small_sem.at[6]),
        pltpu.make_async_copy(
            init.at[lax.div(held, PAIRS), pl.ds(2 * lax.rem(held, PAIRS), 2)],
            init_v,
            small_sem.at[7],
        ),
        pltpu.make_async_copy(wor, wout_v.at[pl.ds(0, RCOLS)], small_sem.at[8]),
        pltpu.make_async_copy(wop, wout_v.at[pl.ds(RCOLS, PCOLS)], small_sem.at[9]),
    ]
    loads = [
        [
            pltpu.make_async_copy(
                w.at[pl.ds(at, HALF)],
                weight_v.at[half, :, pl.ds(OFFS[i], WIDTHS[i])],
                w_sem.at[half, i],
            )
            for i, w in ((i, weights[i]) for i in NEED)
        ]
        for half, at in ((0, mine), (1, theirs))
    ]
    def start(copies):
        for copy in copies:
            copy.start()

    start(small[:2])
    start(loads[0][:2])

    small[0].wait()

    @pl.when(tp == 0)
    def _():
        pl.semaphore_wait(barrier, 1)
        tell(pair_sem, tp=other)

    start(loads[0][2:4] + loads[1][:4] + small[2:4])
    small[1].wait()
    wide = tok_v[...].reshape(TOK, HALF).astype(f32)
    norm_v[0] = (wide * gain_v[...]).astype(bf16)
    squares = wide * wide
    square_v[0] = sum(squares[:, o : o + 128] for o in range(0, HALF, 128))

    @pl.when(tp == 1)
    def _():
        pl.semaphore_wait(pair_sem, 1)

        @pl.loop(1, N_SP)
        def _(step):
            tell(barrier, sp=lax.rem(sp + step, N_SP))

    send_tok = [
        pltpu.make_async_remote_copy(
            src_ref=ref.at[0],
            dst_ref=ref.at[1],
            send_sem=tok_send.at[i],
            recv_sem=tok_recv.at[i],
            device_id={"tp": other},
            device_id_type=MESH,
        )
        for i, ref in enumerate((norm_v, square_v))
    ]
    start(send_tok)
    early = (slice(0, EARLY // 2), slice(EARLY // 2, EARLY))
    for step, at in enumerate(early):
        for copy in loads[0][2 * step : 2 * step + 2]:
            copy.wait()
        acc_v[:, at] = dot(norm_v[0], weight_v[0, :, at])
        if step == 0:
            start(loads[0][4:] + loads[1][4:] + small[4:])

    send_tok[0].wait_recv()

    def scaled(total):
        return (total * cat([scale_v[...]] * (total.shape[1] // 128), 1)).astype(bf16)

    for step, at in enumerate(early):
        for copy in loads[1][2 * step : 2 * step + 2]:
            copy.wait()
        total = acc_v[:, at] + dot(norm_v[1], weight_v[1, :, at])
        if step == 0:
            send_tok[1].wait_recv()
            squares = jnp.sum(square_v[0] + square_v[1], axis=1, keepdims=True)
            scale = lax.rsqrt(squares * (1.0 / D) + 0.25)
            scale_v[...] = jnp.broadcast_to(scale, (TOK, 128))
        proj_v[:, at] = scaled(total)

    for copy in small[2:4]:
        copy.wait()
    groups = [(b, p) for b in range(SEQ) for p in range(PAIRS)]

    def part(index, b, p):
        at = OFFS[index] + 128 * p
        return proj_v[b * ROWS : (b + 1) * ROWS, at : at + 128]

    row = lax.broadcasted_iota(jnp.int32, (256, 128), 0) & 127
    col = lax.broadcasted_iota(jnp.int32, (256, 128), 1)
    strict = row > col
    inclusive = row >= col

    def rows_of(index, b):
        at = OFFS[index]
        return proj_v[b * ROWS : (b + 1) * ROWS, at : at + WIDTHS[index]].astype(f32)

    def local_row(index):
        return cat([base_v[index, pl.ds(3 * tp + p, 1), :] for p in range(PAIRS)], 1)

    ends = []
    for b in range(SEQ):
        alpha, shrink, beta, kappa, e_mid, e_tail, e_last = prepare(
            rows_of(1, b), rows_of(3, b), rows_of(4, b), local_row(0), local_row(1)
        )
        keys_v[b, 0] = alpha
        keys_v[b, 1] = shrink
        keys_v[b, 2] = beta
        keys_v[b, 3] = kappa
        ends.append((e_mid, e_tail, e_last))

    def pair_of(index, g):
        b, p = groups[g]
        return keys_v[b, index, :, 128 * p : 128 * p + 128]

    def end_of(index, g):
        b, p = groups[g]
        return ends[b][index][:, 128 * p : 128 * p + 128]

    every = range(GROUPS)
    for g in every:
        turned = cat([pair_of(2, g).astype(bf16).T, pair_of(3, g).astype(bf16).T], 1)
        turn_v[g] = turned
        pairs = pair_products(pair_of(0, g), turned)
        low_v[g] = jnp.where(strict, pairs[:, :128], 0.0).astype(bf16)
        cross = jnp.where(strict, pairs[:, 128:], 0.0).astype(bf16)
        side_v[g, :, :128] = pair_of(0, g) * end_of(0, g)
        side_v[g, :, 128:] = pick(dot(cross, part(2, *groups[g])))
    @pl.when(tp == 1)
    def _():
        pl.semaphore_wait(barrier, N_SP - 1)
        tell(go_sem, tp=other)

    by_head = inverses([low_v[g, 128 * h : 128 * h + 128, :] for g in every for h in (0, 1)])
    invs = [cat(by_head[2 * g : 2 * g + 2], 0) for g in every]
    map_copies = []
    solved = solve_all(invs, [low_v[g] for g in every], [side_v[g] for g in every])
    for g, z in zip(every, solved):
        z_v[g] = z.astype(bf16)
        tail = end_of(1, g)
        transit, written = maps_of(
            z, part(2, *groups[g]), pair_of(2, g) * tail, pair_of(3, g) * tail, end_of(2, g)
        )
        map_v[g, 0] = transit
        map_v[g, 1] = written
    @pl.when(tp == 0)
    def _():
        pl.semaphore_wait(go_sem, 1)

    own_map = [(tp == 1) & (sp == 2 * g + 1) for g in every]
    for g in every:
        copy = pltpu.make_async_remote_copy(
            src_ref=map_v.at[g],
            dst_ref=maps_in.at[sp],
            send_sem=map_send.at[g],
            recv_sem=map_recv.at[sp],
            device_id={"sp": 2 * g + tp, "tp": 1},
            device_id_type=MESH,
        )
        map_copies.append(copy)

        @pl.when(jnp.logical_not(own_map[g]) & (sp < N_SP - 1))
        def _():
            copy.start()

        @pl.when(own_map[g])
        def _():
            pltpu.make_async_copy(map_v.at[g], maps_in.at[sp], map_recv.at[sp]).start()

    def late(index, copies, at):
        for half in (0, 1):
            for copy in loads[half][copies]:
                copy.wait()
        total = dot(norm_v[0], weight_v[0, :, at]) + dot(norm_v[1], weight_v[1, :, at])
        proj_v[:, at] = scaled(total)

    late(6, slice(6, 8), slice(OFFS[6], COLS))
    for b in range(SEQ):
        pool_v[b, 16:, :] = proj_v[b * ROWS : (b + 1) * ROWS, OFFS[6] : OFFS[7]]
    halo = pltpu.make_async_remote_copy(
        src_ref=pool_v.at[:, pl.ds(ROWS, 16), :],
        dst_ref=pool_v.at[:, pl.ds(0, 16), :],
        send_sem=halo_send,
        recv_sem=halo_recv,
        device_id={"sp": lax.rem(sp + 1, N_SP)},
        device_id_type=MESH,
    )

    @pl.when(sp < N_SP - 1)
    def _():
        halo.start()

    @pl.when(sp == 0)
    def _():
        pool_v[:, 0:16, :] = jnp.zeros((SEQ, 16, PCOLS), bf16)

    late(0, slice(4, 5), slice(OFFS[0], OFFS[5]))
    for g in every:
        rho = part(0, *groups[g]).astype(f32) * pair_of(1, g)
        pairs = pair_products(rho, turn_v[g])
        within_beta = jnp.where(inclusive, pairs[:, :128], 0.0).astype(bf16)
        within_kappa = jnp.where(inclusive, pairs[:, 128:], 0.0).astype(bf16)
        drop = pick(dot(within_beta, z_v[g]))
        reads_v[g] = rho * end_of(0, g) - drop[:, :128]
        local = pick(dot(within_kappa, part(2, *groups[g]))) - drop[:, 128:]
        local_v[g] = local - head_mean(local)
    def send_state(j):
        return pltpu.make_async_remote_copy(
            src_ref=state_v.at[j],
            dst_ref=states_in.at[group_of],
            send_sem=st_send.at[j],
            recv_sem=st_recv.at[group_of],
            device_id={"sp": j, "tp": side},
            device_id_type=MESH,
        )

    def wait_map(j):
        pltpu.make_async_copy(map_v.at[0], maps_in.at[j], map_recv.at[j]).wait()

    def centred(state):
        return (state - jnp.mean(state, axis=0, keepdims=True)).astype(bf16)

    small[7].wait()
    give = pltpu.make_async_remote_copy(
        src_ref=init_v,
        dst_ref=init_in,
        send_sem=init_send,
        recv_sem=init_recv,
        device_id={"tp": other},
        device_id_type=MESH,
    )

    @pl.when(gives_init)
    def _():
        give.start()

    @pl.when(keeps_init)
    def _():
        pltpu.make_async_copy(init_v, init_in, init_recv).start()

    @pl.when(is_owner)
    def _():
        pltpu.make_async_copy(init_v, init_in, init_recv).wait()
        state = cat([init_in[0], init_in[1]], 1)
        def emit(j):
            @pl.when((j != sp) | (side == 0))
            def _():
                send_state(j).start()

        state_v[0] = centred(state)
        emit(0)
        for block in (range(0, 4), range(4, 8), range(8, 12), range(12, 14), range(14, 15)):
            for j in block:
                wait_map(j)
            for j in block:
                state = after_given(state, maps_in[j, 0]) + maps_in[j, 1].astype(f32)
                state_v[j + 1] = centred(state)
            for j in block:
                emit(j + 1)

        @pl.when(side == 1)
        def _():
            pltpu.make_async_copy(
                state_v.at[sp], states_in.at[group_of], st_recv.at[group_of]
            ).start()

    late(5, slice(5, 6), slice(OFFS[5], OFFS[6]))
    for copy in small[4:7] + small[8:]:
        copy.wait()
    for b in range(SEQ):
        gate = rows_of(5, b)
        gate_v[b] = local_row(2) * (gate * sig(gate))

    @pl.when(sp > 0)
    def _():
        halo.wait_recv()

    places = (sp * ROWS + 1 + lax.broadcasted_iota(jnp.int32, (ROWS, 128), 0)).astype(f32)
    for b in range(SEQ):
        outs = []
        for s in range(2):
            at = slice(128 * s, 128 * s + 128)
            own = pool_v[b, :, at].astype(f32)
            total = own + pltpu.roll(own, 1, 0)
            if s == 1:
                total = total + pltpu.roll(total, 2, 0)
            wide = total + pltpu.roll(total, 2 if s == 0 else 4, 0)
            wide = wide + pltpu.roll(wide, 4 if s == 0 else 8, 0)
            trail = jnp.where(tp == 0, total, wide)[16:]
            window = jnp.where(tp == 0, float(2 << s), float(8 << s))
            diff = (trail / jnp.minimum(places, window) - own[16:]).astype(bf16)
            pooled = dot(diff, mix_v[s])
            gate = proj_v[b * ROWS : (b + 1) * ROWS, OFFS[7] + 128 * s : OFFS[7] + 128 * s + 128]
            gate = gate.astype(f32)
            outs.append((pooled * pscale_v[:, at] * (gate * sig(gate))).astype(bf16))
        recout_v[b * ROWS : (b + 1) * ROWS, RCOLS:] = cat(outs, 1)

    for at in (slice(0, 1024), slice(1024, D)):
        merged_v[:, at] = dot(recout_v[:, RCOLS:], wout_v[RCOLS:, at])

    for g in every:
        pltpu.make_async_copy(state_v.at[0], states_in.at[g], st_recv.at[g]).wait()
    centre = [state_reads(reads_v[g], states_in[g]) + local_v[g] for g in every]
    for b in range(SEQ):
        rec = cat(centre[PAIRS * b : PAIRS * b + PAIRS], 1)
        spread = head_mean(rec * rec)
        recout_v[b * ROWS : (b + 1) * ROWS, :RCOLS] = (
            rec * lax.rsqrt(spread + 1.0) * gate_v[b]
        ).astype(bf16)

    def product(at):
        total = merged_v[:, at] + dot(recout_v[:, :RCOLS], wout_v[:RCOLS, at])
        return total.astype(bf16).reshape(SEQ, ROWS, 512)

    def columns(ref, tile):
        return ref.at[:, :, pl.ds(512 * tile, 512)]

    def send_part(tile):
        return pltpu.make_async_remote_copy(
            src_ref=part_v.at[tile],
            dst_ref=columns(arrived_out, tile),
            send_sem=part_send.at[tile],
            recv_sem=part_recv.at[tile],
            device_id={"tp": other},
            device_id_type=MESH,
        )

    for tile in range(2):
        part_v[tile] = product(pl.ds(pl.multiple_of(theirs + tile * 512, 512), 512))
        send_part(tile).start()
    for tile in range(2):
        at = pl.ds(pl.multiple_of(mine + tile * 512, 512), 512)
        own_out[:, :, 512 * tile : 512 * tile + 512] = product(at)

    for copy in send_tok:
        copy.wait_send()

    @pl.when(sp < N_SP - 1)
    def _():
        halo.wait_send()

    for g, copy in enumerate(map_copies):
        @pl.when(jnp.logical_not(own_map[g]) & (sp < N_SP - 1))
        def _():
            copy.wait_send()

    @pl.when(gives_init)
    def _():
        give.wait_send()

    @pl.when(is_owner)
    def _():
        @pl.loop(0, N_SP)
        def _(j):
            @pl.when((j != sp) | (side == 0))
            def _():
                send_state(j).wait_send()

    for tile in range(2):
        send_part(tile).wait()


def shards(
    tokens, norm_gain, w_recept, w_key, w_value, w_decay, w_rate, w_gate_rec, w_pool, w_gate_pool,
    decay_base, rate_base, head_gain, pool_mix, pool_scale, w_out_rec, w_out_pool, init_state,
):
    vmem, sem = pltpu.VMEM, pltpu.SemaphoreType.DMA
    row = lambda x: x.reshape(1, -1)
    tile = lambda x: x.reshape(6, 128)
    scratch = [
        vmem((SEQ, ROWS, HALF), bf16),
        vmem((1, HALF), f32),
        vmem((2, HALF, COLS), bf16),
        vmem((TOK, EARLY), f32),
        vmem((TOK, COLS), bf16),
        vmem((2, TOK, HALF), bf16),
        vmem((2, TOK, 128), f32),
        vmem((3, 6, 128), f32),
        vmem((2, 128, 128), bf16),
        vmem((1, PCOLS), f32),
        vmem((RCOLS + PCOLS, D), bf16),
        vmem((2, HD, HD), f32),
        vmem((2, HD, HD), f32),
        vmem((TOK, 128), f32),
        vmem((SEQ, 16 + ROWS, PCOLS), bf16),
        vmem((SEQ, 4, ROWS, RCOLS), f32),
        vmem((GROUPS, 128, 256), bf16),
        vmem((GROUPS, 256, 128), bf16),
        vmem((GROUPS, 128, 256), f32),
        vmem((GROUPS, 128, 256), bf16),
        vmem((GROUPS, 128, 128), f32),
        vmem((GROUPS, 128, 128), f32),
        vmem((GROUPS, 2, HD, 128), bf16),
        vmem((N_SP, 2, HD, 128), bf16),
        vmem((SEQ, ROWS, RCOLS), f32),
        vmem((N_SP, HD, 128), bf16),
        vmem((GROUPS, HD, 128), bf16),
        vmem((TOK, D), f32),
        vmem((TOK, RCOLS + PCOLS), bf16),
        vmem((2, SEQ, ROWS, 512), bf16),
        sem((2, 8)),
        sem((10,)),
        sem((2,)),
        sem((2,)),
        sem,
        sem,
        sem((GROUPS,)),
        sem((N_SP,)),
        sem((N_SP,)),
        sem((GROUPS,)),
        sem((2,)),
        sem((2,)),
        sem,
        sem,
        pltpu.SemaphoreType.REGULAR,
        pltpu.SemaphoreType.REGULAR,
    ]
    pin = lambda x: pltpu.with_memory_space_constraint(x, pltpu.HBM)
    own, arrived = pl.pallas_call(
        kernel,
        out_shape=[jax.ShapeDtypeStruct((SEQ, ROWS, HALF), bf16)] * 2,
        in_specs=[pl.BlockSpec(memory_space=pl.ANY)] * 18,
        out_specs=[pl.BlockSpec(memory_space=pltpu.VMEM)] * 2,
        scratch_shapes=scratch,
        compiler_params=pltpu.CompilerParams(
            collective_id=0, has_side_effects=True, vmem_limit_bytes=48 << 20
        ),
        name="layer",
    )(*(pin(x) for x in (
        tokens, row(norm_gain), w_recept, w_key, w_value, w_decay, w_rate, w_gate_rec, w_pool,
        w_gate_pool, tile(decay_base), tile(rate_base), tile(head_gain), pool_mix, row(pool_scale),
        w_out_rec, w_out_pool, init_state,
    )))
    return (own.astype(f32) + arrived.astype(f32)).astype(bf16)


def solution(mesh):
    split = P(None, "tp")
    placed = (
        P("fs", "sp", "tp"), P(),
        split, split, split, split, split, split, split, split,
        P(), P(), P(), P(), P(),
        P("tp", None), P("tp", None), P("fs", "tp", None, None),
    )
    return jax.shard_map(
        shards, mesh=mesh, in_specs=placed, out_specs=P("fs", "sp", "tp"), check_vma=False
    )
```

```python
import math

import jax
import jax.numpy as jnp
from jax import lax
from jax.experimental import pallas as pl
from jax.experimental.pallas import tpu as pltpu
from jax.sharding import PartitionSpec as P

D = 2048
HALF = 1024
SEQ = 2
ROWS = 128
TOK = SEQ * ROWS
RCOLS = 384
PCOLS = 256
PAIRS = 3
GROUPS = SEQ * PAIRS
HD = 64
N_SP = 16
COLS = 6 * RCOLS + 2 * PCOLS
OFFS = (1536, 0, 1152, 384, 768, 1920, 2304, 2560)
NEED = (1, 3, 4, 2, 0, 5, 6, 7)
EARLY = 4 * RCOLS
OWNERS = ((0, 2, 4, 6, 8, 10), (1, 3, 5, 7, 9, 11))
WIDTHS = (384, 384, 384, 384, 384, 384, 256, 256)
MESH = pl.DeviceIdType.MESH
f32 = jnp.float32
bf16 = jnp.bfloat16


def dot(a, b):
    return lax.dot_general(a, b, (((1,), (0,)), ((), ())), preferred_element_type=f32)


def dot_nt(a, b):
    return lax.dot_general(a, b, (((1,), (1,)), ((), ())), preferred_element_type=f32)


def dot_tn(a, b):
    return lax.dot_general(a, b, (((0,), (0,)), ((), ())), preferred_element_type=f32)


def split2(x):
    hi = x.astype(bf16)
    return hi, (x - hi.astype(f32)).astype(bf16)


def cat(parts, axis):
    return jnp.concatenate(parts, axis=axis)


def sig(x):
    e = jnp.exp(-jnp.abs(x))
    return jnp.where(x >= 0, 1.0, e) / (1.0 + e)


def lane_first(shape):
    return lax.broadcasted_iota(jnp.int32, shape, len(shape) - 1) < HD


def keep(x, head):
    first = lane_first(x.shape)
    zero = jnp.zeros_like(x)
    return jnp.where(first, x, zero) if head == 0 else jnp.where(first, zero, x)


def two_heads(x):
    return cat([keep(x, 0), keep(x, 1)], 0)


def block_ones():
    i = lax.broadcasted_iota(jnp.int32, (128, 128), 0) < HD
    j = lax.broadcasted_iota(jnp.int32, (128, 128), 1) < HD
    return jnp.where(i == j, 1.0, 0.0).astype(bf16)


def head_sums(x, ones2):
    hi, lo = split2(x)
    return dot(cat([hi, lo], 1), ones2)


def prepare(k, d_in, a_in, d_base, a_base):
    ones = block_ones()
    ones2 = cat([ones, ones], 0)
    x = d_base + d_in
    log_decay = -math.exp(-0.5) * sig(x)
    rate = sig(a_base + a_in)
    squares = k * k
    sums = cat([head_sums(squares[:, o : o + 128], ones2) for o in range(0, RCOLS, 128)], 1)
    unit = k * lax.rsqrt(sums + 1.0)
    removal = unit * rate
    i = lax.broadcasted_iota(jnp.int32, (128, 128), 0)
    j = lax.broadcasted_iota(jnp.int32, (128, 128), 1)
    tri = jnp.where(i >= j, 1.0, 0.0).astype(bf16)
    hi, lo = split2(log_decay)
    rest = (log_decay - hi.astype(f32) - lo.astype(f32)).astype(bf16)
    cum = dot(cat([tri, tri, tri], 1), cat([hi, lo, rest], 0))
    mid = cum[63:64, :]
    last = cum[127:128, :]
    shrink = jnp.exp(cum - mid)
    grow = jnp.exp(mid - cum)
    alpha = jnp.exp(cum - log_decay - mid) * unit
    beta = removal * grow
    kappa = k * grow
    return alpha, shrink, beta, kappa, jnp.exp(mid), jnp.exp(last - mid), jnp.exp(last)


def pair_products(x, turned):
    parts = [split2(keep(x, head)) for head in (0, 1)]
    lhs = cat([cat([hi, lo], 1) for hi, lo in parts], 0)
    return dot(lhs, cat([turned, turned], 0))


def pick(x):
    first = (lax.broadcasted_iota(jnp.int32, (128, x.shape[1]), 1) & 127) < HD
    return jnp.where(first, x[:128], x[128:])


def inverses(lowers):
    i = lax.broadcasted_iota(jnp.int32, (128, 128), 0)
    j = lax.broadcasted_iota(jnp.int32, (128, 128), 1)
    apart = i ^ j
    same = apart < 32
    zero = jnp.zeros((128, 128), bf16)

    def packed(x):
        return (x[:32] + x[32:64]) + (x[64:96] + x[96:])

    def spread(x):
        return jnp.where(same, cat([x] * 4, 0), jnp.zeros((128, 128), x.dtype))

    eye = packed(jnp.where(i == j, 1.0, 0.0))
    inv = [eye - packed(jnp.where(apart == 1, low, zero).astype(f32)) for low in lowers]
    for size in (2, 8):
        inside = (apart >= size) & (apart < 4 * size)
        inv_b = [x.astype(bf16) for x in inv]
        hop = [
            dot(x, jnp.where(inside, low, zero)).astype(bf16) for x, low in zip(inv_b, lowers)
        ]
        both = [dot(h, cat([spread(h), spread(x)], 1)) for h, x in zip(hop, inv_b)]
        once = [x - y[:, 128:] for x, y in zip(inv, both)]
        inv = [
            x + dot(y[:, :128].astype(bf16), spread(x.astype(bf16))) for x, y in zip(once, both)
        ]
    inv = [spread(x) for x in inv]
    inv_b = [x.astype(bf16) for x in inv]
    outside = apart >= 32
    top = jnp.zeros((32, 128), bf16)
    hop = [
        dot(x[32:], jnp.where(outside, low, zero)).astype(bf16) for x, low in zip(inv_b, lowers)
    ]
    both = [dot(h, cat([cat([top, h], 0), x], 1)) for h, x in zip(hop, inv_b)]
    once = [cat([x[:32], x[32:] - y[:, 128:]], 0) for x, y in zip(inv, both)]
    last = [dot(y[32:, :128].astype(bf16), x.astype(bf16)) for x, y in zip(once, both)]
    return [cat([x[:64], x[64:] + y], 0).astype(bf16) for x, y in zip(once, last)]


def solve_all(invs, lows, sides):
    first = [pick(dot(inv, side.astype(bf16))).astype(bf16) for inv, side in zip(invs, sides)]
    back = [pick(dot(low, x)) for low, x in zip(lows, first)]
    miss = [
        (side - x.astype(f32) - y).astype(bf16) for side, x, y in zip(sides, first, back)
    ]
    return [x.astype(f32) + pick(dot(inv, m)) for x, inv, m in zip(first, invs, miss)]


def maps_of(z, value, beta_end, kappa_end, gain_end):
    zero = jnp.zeros((128, 128), bf16)
    lhs = cat([z.astype(bf16), cat([zero, -value], 1)], 0)
    both = dot_tn(lhs, cat([beta_end, kappa_end], 0).astype(bf16))
    first = lane_first((64, 128))
    packed = [
        jnp.where(first, both[o : o + 64], both[o + 64 : o + 128]) for o in (0, 128)
    ]
    i = lax.broadcasted_iota(jnp.int32, (64, 128), 0)
    j = lax.broadcasted_iota(jnp.int32, (64, 128), 1) & 63
    transit = jnp.where(i == j, gain_end, 0.0) - packed[0]
    return transit.astype(bf16), (-packed[1]).astype(bf16)


def after_given(state, transit):
    both = dot(cat(split2(state), 0), two_heads(transit))
    return both[:HD] + both[HD:]


def state_reads(reads, state):
    both = dot_nt(cat(split2(reads), 0), two_heads(state))
    return both[:128] + both[128:]


def head_mean(x):
    ones = block_ones()
    ones2 = cat([ones, ones], 0)
    parts = [head_sums(x[:, o : o + 128], ones2) for o in range(0, x.shape[1], 128)]
    return cat(parts, 1) * (1.0 / HD)


def kernel(
    tok, gain, wr, wk, wv, wd, wa, wg, wp, wgp, dbase, rbase, hgain, mix, pscale, wor, wop, init,
    own_out, arrived_out,
    tok_v, gain_v, weight_v, acc_v, proj_v, norm_v, square_v, base_v, mix_v, pscale_v, wout_v, init_v, init_in,
    scale_v, pool_v, keys_v, turn_v, low_v, side_v, z_v, reads_v, local_v, map_v, maps_in,
    gate_v, state_v, states_in, merged_v, recout_v, part_v,
    w_sem, small_sem, tok_send, tok_recv, halo_send, halo_recv, map_send, map_recv,
    st_send, st_recv, part_send, part_recv, init_send, init_recv, pair_sem, go_sem,
):
    sp = lax.axis_index("sp")
    tp = lax.axis_index("tp")
    other = 1 - tp
    weights = (wr, wk, wv, wd, wa, wg, wp, wgp)
    group_of, side, owning = 0, 0, 0
    for core in (0, 1):
        for g, owner in enumerate(OWNERS[core]):
            here = (sp == owner).astype(jnp.int32)
            group_of, side, owning = group_of + here * g, side + here * core, owning + here
    is_owner = (tp == 1) & (owning == 1)
    gives_init = (tp == 0) & (side == 0) & (owning == 1)
    keeps_init = (tp == 1) & (side == 1) & (owning == 1)

    def owner_of(g):
        return OWNERS[0][g] + tp * (OWNERS[1][g] - OWNERS[0][g])


    barrier = pltpu.get_barrier_semaphore()

    def tell(semaphore, **device):
        pl.semaphore_signal(semaphore, inc=1, device_id=device, device_id_type=MESH)

    @pl.when(tp == 1)
    def _():
        tell(barrier, tp=other)

    mine = pl.multiple_of(tp * HALF, HALF)
    theirs = pl.multiple_of(other * HALF, HALF)
    pool_at = pl.multiple_of(tp * PCOLS, 128)
    held = group_of
    small = [
        pltpu.make_async_copy(tok, tok_v, small_sem.at[0]),
        pltpu.make_async_copy(gain.at[:, pl.ds(mine, HALF)], gain_v, small_sem.at[1]),
        pltpu.make_async_copy(dbase, base_v.at[0], small_sem.at[2]),
        pltpu.make_async_copy(rbase, base_v.at[1], small_sem.at[3]),
        pltpu.make_async_copy(hgain, base_v.at[2], small_sem.at[4]),
        pltpu.make_async_copy(mix.at[pl.ds(tp * 2, 2)], mix_v, small_sem.at[5]),
        pltpu.make_async_copy(pscale.at[:, pl.ds(pool_at, PCOLS)], pscale_v, small_sem.at[6]),
        pltpu.make_async_copy(
            init.at[lax.div(held, PAIRS), pl.ds(2 * lax.rem(held, PAIRS), 2)],
            init_v,
            small_sem.at[7],
        ),
        pltpu.make_async_copy(wor, wout_v.at[pl.ds(0, RCOLS)], small_sem.at[8]),
        pltpu.make_async_copy(wop, wout_v.at[pl.ds(RCOLS, PCOLS)], small_sem.at[9]),
    ]
    loads = [
        [
            pltpu.make_async_copy(
                w.at[pl.ds(at, HALF)],
                weight_v.at[half, :, pl.ds(OFFS[i], WIDTHS[i])],
                w_sem.at[half, i],
            )
            for i, w in ((i, weights[i]) for i in NEED)
        ]
        for half, at in ((0, mine), (1, theirs))
    ]
    def start(copies):
        for copy in copies:
            copy.start()

    start(small[:2])
    start(loads[0][:2])

    small[0].wait()

    @pl.when(tp == 0)
    def _():
        pl.semaphore_wait(barrier, 1)
        tell(pair_sem, tp=other)

    start(loads[0][2:4] + loads[1][:4] + small[2:4])
    small[1].wait()
    wide = tok_v[...].reshape(TOK, HALF).astype(f32)
    norm_v[0] = (wide * gain_v[...]).astype(bf16)
    squares = wide * wide
    square_v[0] = sum(squares[:, o : o + 128] for o in range(0, HALF, 128))

    @pl.when(tp == 1)
    def _():
        pl.semaphore_wait(pair_sem, 1)

        @pl.loop(1, N_SP)
        def _(step):
            tell(barrier, sp=lax.rem(sp + step, N_SP))

    send_tok = [
        pltpu.make_async_remote_copy(
            src_ref=ref.at[0],
            dst_ref=ref.at[1],
            send_sem=tok_send.at[i],
            recv_sem=tok_recv.at[i],
            device_id={"tp": other},
            device_id_type=MESH,
        )
        for i, ref in enumerate((norm_v, square_v))
    ]
    start(send_tok)
    early = (slice(0, EARLY // 2), slice(EARLY // 2, EARLY))
    for step, at in enumerate(early):
        for copy in loads[0][2 * step : 2 * step + 2]:
            copy.wait()
        acc_v[:, at] = dot(norm_v[0], weight_v[0, :, at])
        if step == 0:
            start(loads[0][4:] + loads[1][4:] + small[4:])

    send_tok[0].wait_recv()

    def scaled(total):
        return (total * cat([scale_v[...]] * (total.shape[1] // 128), 1)).astype(bf16)

    for step, at in enumerate(early):
        for copy in loads[1][2 * step : 2 * step + 2]:
            copy.wait()
        total = acc_v[:, at] + dot(norm_v[1], weight_v[1, :, at])
        if step == 0:
            send_tok[1].wait_recv()
            squares = jnp.sum(square_v[0] + square_v[1], axis=1, keepdims=True)
            scale = lax.rsqrt(squares * (1.0 / D) + 0.25)
            scale_v[...] = jnp.broadcast_to(scale, (TOK, 128))
        proj_v[:, at] = scaled(total)

    for copy in small[2:4]:
        copy.wait()
    groups = [(b, p) for b in range(SEQ) for p in range(PAIRS)]

    def part(index, b, p):
        at = OFFS[index] + 128 * p
        return proj_v[b * ROWS : (b + 1) * ROWS, at : at + 128]

    row = lax.broadcasted_iota(jnp.int32, (256, 128), 0) & 127
    col = lax.broadcasted_iota(jnp.int32, (256, 128), 1)
    strict = row > col
    inclusive = row >= col

    def rows_of(index, b):
        at = OFFS[index]
        return proj_v[b * ROWS : (b + 1) * ROWS, at : at + WIDTHS[index]].astype(f32)

    def local_row(index):
        return cat([base_v[index, pl.ds(3 * tp + p, 1), :] for p in range(PAIRS)], 1)

    small[7].wait()
    give = pltpu.make_async_remote_copy(
        src_ref=init_v,
        dst_ref=init_in,
        send_sem=init_send,
        recv_sem=init_recv,
        device_id={"tp": other},
        device_id_type=MESH,
    )

    @pl.when(gives_init)
    def _():
        give.start()

    @pl.when(keeps_init)
    def _():
        pltpu.make_async_copy(init_v, init_in, init_recv).start()

    ends = []
    for b in range(SEQ):
        alpha, shrink, beta, kappa, e_mid, e_tail, e_last = prepare(
            rows_of(1, b), rows_of(3, b), rows_of(4, b), local_row(0), local_row(1)
        )
        keys_v[b, 0] = alpha
        keys_v[b, 1] = shrink
        keys_v[b, 2] = beta
        keys_v[b, 3] = kappa
        ends.append((e_mid, e_tail, e_last))

    def pair_of(index, g):
        b, p = groups[g]
        return keys_v[b, index, :, 128 * p : 128 * p + 128]

    def end_of(index, g):
        b, p = groups[g]
        return ends[b][index][:, 128 * p : 128 * p + 128]

    every = range(GROUPS)
    for g in every:
        turned = cat([pair_of(2, g).astype(bf16).T, pair_of(3, g).astype(bf16).T], 1)
        turn_v[g] = turned
        pairs = pair_products(pair_of(0, g), turned)
        low_v[g] = jnp.where(strict, pairs[:, :128], 0.0).astype(bf16)
        cross = jnp.where(strict, pairs[:, 128:], 0.0).astype(bf16)
        side_v[g, :, :128] = pair_of(0, g) * end_of(0, g)
        side_v[g, :, 128:] = pick(dot(cross, part(2, *groups[g])))
    @pl.when(tp == 1)
    def _():
        pl.semaphore_wait(barrier, N_SP - 1)
        tell(go_sem, tp=other)

    by_head = inverses([low_v[g, 128 * h : 128 * h + 128, :] for g in every for h in (0, 1)])
    invs = [cat(by_head[2 * g : 2 * g + 2], 0) for g in every]
    map_copies = []
    solved = solve_all(invs, [low_v[g] for g in every], [side_v[g] for g in every])
    for g, z in zip(every, solved):
        z_v[g] = z.astype(bf16)
        tail = end_of(1, g)
        transit, written = maps_of(
            z, part(2, *groups[g]), pair_of(2, g) * tail, pair_of(3, g) * tail, end_of(2, g)
        )
        map_v[g, 0] = transit
        map_v[g, 1] = written
    @pl.when(tp == 0)
    def _():
        pl.semaphore_wait(go_sem, 1)

    own_map = [(tp == 1) & (sp == OWNERS[1][g]) for g in every]
    for g in every:
        copy = pltpu.make_async_remote_copy(
            src_ref=map_v.at[g],
            dst_ref=maps_in.at[sp],
            send_sem=map_send.at[g],
            recv_sem=map_recv.at[sp],
            device_id={"sp": owner_of(g), "tp": 1},
            device_id_type=MESH,
        )
        map_copies.append(copy)

        @pl.when(jnp.logical_not(own_map[g]) & (sp < N_SP - 1))
        def _():
            copy.start()

        @pl.when(own_map[g])
        def _():
            pltpu.make_async_copy(map_v.at[g], maps_in.at[sp], map_recv.at[sp]).start()

    def send_state(j):
        return pltpu.make_async_remote_copy(
            src_ref=state_v.at[j],
            dst_ref=states_in.at[group_of],
            send_sem=st_send.at[j],
            recv_sem=st_recv.at[group_of],
            device_id={"sp": j, "tp": side},
            device_id_type=MESH,
        )

    def wait_map(j):
        pltpu.make_async_copy(map_v.at[0], maps_in.at[j], map_recv.at[j]).wait()

    def centred(state):
        return (state - jnp.mean(state, axis=0, keepdims=True)).astype(bf16)

    def emit(j):
        @pl.when((j != sp) | (side == 0))
        def _():
            send_state(j).start()

    @pl.when(is_owner)
    def _():
        pltpu.make_async_copy(init_v, init_in, init_recv).wait()
        state_v[0] = centred(cat([init_in[0], init_in[1]], 1))
        emit(0)

    def late(index, copies, at):
        for half in (0, 1):
            for copy in loads[half][copies]:
                copy.wait()
        total = dot(norm_v[0], weight_v[0, :, at]) + dot(norm_v[1], weight_v[1, :, at])
        proj_v[:, at] = scaled(total)

    late(6, slice(6, 8), slice(OFFS[6], COLS))
    for b in range(SEQ):
        pool_v[b, 16:, :] = proj_v[b * ROWS : (b + 1) * ROWS, OFFS[6] : OFFS[7]]
    halo = pltpu.make_async_remote_copy(
        src_ref=pool_v.at[:, pl.ds(ROWS, 16), :],
        dst_ref=pool_v.at[:, pl.ds(0, 16), :],
        send_sem=halo_send,
        recv_sem=halo_recv,
        device_id={"sp": lax.rem(sp + 1, N_SP)},
        device_id_type=MESH,
    )

    @pl.when(sp < N_SP - 1)
    def _():
        halo.start()

    @pl.when(sp == 0)
    def _():
        pool_v[:, 0:16, :] = jnp.zeros((SEQ, 16, PCOLS), bf16)

    late(0, slice(4, 5), slice(OFFS[0], OFFS[5]))
    for g in every:
        rho = part(0, *groups[g]).astype(f32) * pair_of(1, g)
        pairs = pair_products(rho, turn_v[g])
        within_beta = jnp.where(inclusive, pairs[:, :128], 0.0).astype(bf16)
        within_kappa = jnp.where(inclusive, pairs[:, 128:], 0.0).astype(bf16)
        drop = pick(dot(within_beta, z_v[g]))
        reads_v[g] = rho * end_of(0, g) - drop[:, :128]
        local = pick(dot(within_kappa, part(2, *groups[g]))) - drop[:, 128:]
        local_v[g] = local - head_mean(local)
    def late_work():
        late(5, slice(5, 6), slice(OFFS[5], OFFS[6]))
        for copy in small[4:7] + small[8:]:
            copy.wait()
        for b in range(SEQ):
            gate = rows_of(5, b)
            gate_v[b] = local_row(2) * (gate * sig(gate))

        @pl.when(sp > 0)
        def _():
            halo.wait_recv()

        places = (sp * ROWS + 1 + lax.broadcasted_iota(jnp.int32, (ROWS, 128), 0)).astype(f32)
        for b in range(SEQ):
            outs = []
            for s in range(2):
                at = slice(128 * s, 128 * s + 128)
                own = pool_v[b, :, at].astype(f32)
                total = own + pltpu.roll(own, 1, 0)
                if s == 1:
                    total = total + pltpu.roll(total, 2, 0)
                wide = total + pltpu.roll(total, 2 if s == 0 else 4, 0)
                wide = wide + pltpu.roll(wide, 4 if s == 0 else 8, 0)
                trail = jnp.where(tp == 0, total, wide)[16:]
                window = jnp.where(tp == 0, float(2 << s), float(8 << s))
                diff = (trail / jnp.minimum(places, window) - own[16:]).astype(bf16)
                pooled = dot(diff, mix_v[s])
                gate = proj_v[b * ROWS : (b + 1) * ROWS, OFFS[7] + 128 * s : OFFS[7] + 128 * s + 128]
                gate = gate.astype(f32)
                outs.append((pooled * pscale_v[:, at] * (gate * sig(gate))).astype(bf16))
            recout_v[b * ROWS : (b + 1) * ROWS, RCOLS:] = cat(outs, 1)

        for at in (slice(0, 1024), slice(1024, D)):
            merged_v[:, at] = dot(recout_v[:, RCOLS:], wout_v[RCOLS:, at])

    @pl.when(sp < 8)
    def _():
        late_work()

    @pl.when(is_owner)
    def _():
        state = cat([init_in[0], init_in[1]], 1)
        for block in ((0,), (1,), (2,), (3,), (4, 5), (6, 7), (8, 9), (10, 11), (12,), (13,), (14,)):
            for j in block:
                wait_map(j)
            for j in block:
                state = after_given(state, maps_in[j, 0]) + maps_in[j, 1].astype(f32)
                state_v[j + 1] = centred(state)
            for j in block:
                emit(j + 1)

        @pl.when(side == 1)
        def _():
            pltpu.make_async_copy(
                state_v.at[sp], states_in.at[group_of], st_recv.at[group_of]
            ).start()

    @pl.when(sp >= 8)
    def _():
        late_work()

    for g in every:
        pltpu.make_async_copy(state_v.at[0], states_in.at[g], st_recv.at[g]).wait()
    centre = [state_reads(reads_v[g], states_in[g]) + local_v[g] for g in every]
    for b in range(SEQ):
        rec = cat(centre[PAIRS * b : PAIRS * b + PAIRS], 1)
        spread = head_mean(rec * rec)
        recout_v[b * ROWS : (b + 1) * ROWS, :RCOLS] = (
            rec * lax.rsqrt(spread + 1.0) * gate_v[b]
        ).astype(bf16)

    def product(at):
        total = merged_v[:, at] + dot(recout_v[:, :RCOLS], wout_v[:RCOLS, at])
        return total.astype(bf16).reshape(SEQ, ROWS, 512)

    def columns(ref, tile):
        return ref.at[:, :, pl.ds(512 * tile, 512)]

    def send_part(tile):
        return pltpu.make_async_remote_copy(
            src_ref=part_v.at[tile],
            dst_ref=columns(arrived_out, tile),
            send_sem=part_send.at[tile],
            recv_sem=part_recv.at[tile],
            device_id={"tp": other},
            device_id_type=MESH,
        )

    for tile in range(2):
        part_v[tile] = product(pl.ds(pl.multiple_of(theirs + tile * 512, 512), 512))
        send_part(tile).start()
    for tile in range(2):
        at = pl.ds(pl.multiple_of(mine + tile * 512, 512), 512)
        own_out[:, :, 512 * tile : 512 * tile + 512] = product(at)

    for copy in send_tok:
        copy.wait_send()

    @pl.when(sp < N_SP - 1)
    def _():
        halo.wait_send()

    for g, copy in enumerate(map_copies):
        @pl.when(jnp.logical_not(own_map[g]) & (sp < N_SP - 1))
        def _():
            copy.wait_send()

    @pl.when(gives_init)
    def _():
        give.wait_send()

    @pl.when(is_owner)
    def _():
        @pl.loop(0, N_SP)
        def _(j):
            @pl.when((j != sp) | (side == 0))
            def _():
                send_state(j).wait_send()

    for tile in range(2):
        send_part(tile).wait()


def shards(
    tokens, norm_gain, w_recept, w_key, w_value, w_decay, w_rate, w_gate_rec, w_pool, w_gate_pool,
    decay_base, rate_base, head_gain, pool_mix, pool_scale, w_out_rec, w_out_pool, init_state,
):
    vmem, sem = pltpu.VMEM, pltpu.SemaphoreType.DMA
    row = lambda x: x.reshape(1, -1)
    tile = lambda x: x.reshape(6, 128)
    scratch = [
        vmem((SEQ, ROWS, HALF), bf16),
        vmem((1, HALF), f32),
        vmem((2, HALF, COLS), bf16),
        vmem((TOK, EARLY), f32),
        vmem((TOK, COLS), bf16),
        vmem((2, TOK, HALF), bf16),
        vmem((2, TOK, 128), f32),
        vmem((3, 6, 128), f32),
        vmem((2, 128, 128), bf16),
        vmem((1, PCOLS), f32),
        vmem((RCOLS + PCOLS, D), bf16),
        vmem((2, HD, HD), f32),
        vmem((2, HD, HD), f32),
        vmem((TOK, 128), f32),
        vmem((SEQ, 16 + ROWS, PCOLS), bf16),
        vmem((SEQ, 4, ROWS, RCOLS), f32),
        vmem((GROUPS, 128, 256), bf16),
        vmem((GROUPS, 256, 128), bf16),
        vmem((GROUPS, 128, 256), f32),
        vmem((GROUPS, 128, 256), bf16),
        vmem((GROUPS, 128, 128), f32),
        vmem((GROUPS, 128, 128), f32),
        vmem((GROUPS, 2, HD, 128), bf16),
        vmem((N_SP, 2, HD, 128), bf16),
        vmem((SEQ, ROWS, RCOLS), f32),
        vmem((N_SP, HD, 128), bf16),
        vmem((GROUPS, HD, 128), bf16),
        vmem((TOK, D), f32),
        vmem((TOK, RCOLS + PCOLS), bf16),
        vmem((2, SEQ, ROWS, 512), bf16),
        sem((2, 8)),
        sem((10,)),
        sem((2,)),
        sem((2,)),
        sem,
        sem,
        sem((GROUPS,)),
        sem((N_SP,)),
        sem((N_SP,)),
        sem((GROUPS,)),
        sem((2,)),
        sem((2,)),
        sem,
        sem,
        pltpu.SemaphoreType.REGULAR,
        pltpu.SemaphoreType.REGULAR,
    ]
    pin = lambda x: pltpu.with_memory_space_constraint(x, pltpu.HBM)
    own, arrived = pl.pallas_call(
        kernel,
        out_shape=[jax.ShapeDtypeStruct((SEQ, ROWS, HALF), bf16)] * 2,
        in_specs=[pl.BlockSpec(memory_space=pl.ANY)] * 18,
        out_specs=[pl.BlockSpec(memory_space=pltpu.VMEM)] * 2,
        scratch_shapes=scratch,
        compiler_params=pltpu.CompilerParams(
            collective_id=0, has_side_effects=True, vmem_limit_bytes=48 << 20
        ),
        name="layer",
    )(*(pin(x) for x in (
        tokens, row(norm_gain), w_recept, w_key, w_value, w_decay, w_rate, w_gate_rec, w_pool,
        w_gate_pool, tile(decay_base), tile(rate_base), tile(head_gain), pool_mix, row(pool_scale),
        w_out_rec, w_out_pool, init_state,
    )))
    return (own.astype(f32) + arrived.astype(f32)).astype(bf16)


def solution(mesh):
    split = P(None, "tp")
    placed = (
        P("fs", "sp", "tp"), P(),
        split, split, split, split, split, split, split, split,
        P(), P(), P(), P(), P(),
        P("tp", None), P("tp", None), P("fs", "tp", None, None),
    )
    return jax.shard_map(
        shards, mesh=mesh, in_specs=placed, out_specs=P("fs", "sp", "tp"), check_vma=False
    )
```

```python
import math

import jax
import jax.numpy as jnp
from jax import lax
from jax.experimental import pallas as pl
from jax.experimental.pallas import tpu as pltpu
from jax.sharding import PartitionSpec as P

D = 2048
HALF = 1024
SEQ = 2
ROWS = 128
TOK = SEQ * ROWS
RCOLS = 384
PCOLS = 256
PAIRS = 3
GROUPS = SEQ * PAIRS
HD = 64
N_SP = 16
COLS = 6 * RCOLS + 2 * PCOLS
OFFS = (1536, 0, 1152, 384, 768, 1920, 2304, 2560)
NEED = (1, 3, 4, 2, 0, 5, 6, 7)
EARLY = 4 * RCOLS
OWNERS = ((0, 2, 4, 6, 8, 10), (1, 3, 5, 7, 9, 11))
WIDTHS = (384, 384, 384, 384, 384, 384, 256, 256)
MESH = pl.DeviceIdType.MESH
f32 = jnp.float32
bf16 = jnp.bfloat16


def dot(a, b):
    return lax.dot_general(a, b, (((1,), (0,)), ((), ())), preferred_element_type=f32)


def dot_nt(a, b):
    return lax.dot_general(a, b, (((1,), (1,)), ((), ())), preferred_element_type=f32)


def dot_tn(a, b):
    return lax.dot_general(a, b, (((0,), (0,)), ((), ())), preferred_element_type=f32)


def split2(x):
    hi = x.astype(bf16)
    return hi, (x - hi.astype(f32)).astype(bf16)


def cat(parts, axis):
    return jnp.concatenate(parts, axis=axis)


def sig(x):
    e = jnp.exp(-jnp.abs(x))
    return jnp.where(x >= 0, 1.0, e) / (1.0 + e)


def lane_first(shape):
    return lax.broadcasted_iota(jnp.int32, shape, len(shape) - 1) < HD


def keep(x, head):
    first = lane_first(x.shape)
    zero = jnp.zeros_like(x)
    return jnp.where(first, x, zero) if head == 0 else jnp.where(first, zero, x)


def two_heads(x):
    return cat([keep(x, 0), keep(x, 1)], 0)


def block_ones():
    i = lax.broadcasted_iota(jnp.int32, (128, 128), 0) < HD
    j = lax.broadcasted_iota(jnp.int32, (128, 128), 1) < HD
    return jnp.where(i == j, 1.0, 0.0).astype(bf16)


def head_sums(x, ones2):
    hi, lo = split2(x)
    return dot(cat([hi, lo], 1), ones2)


def prepare(k, d_in, a_in, d_base, a_base):
    ones = block_ones()
    ones2 = cat([ones, ones], 0)
    x = d_base + d_in
    log_decay = -math.exp(-0.5) * sig(x)
    rate = sig(a_base + a_in)
    squares = k * k
    sums = cat([head_sums(squares[:, o : o + 128], ones2) for o in range(0, RCOLS, 128)], 1)
    unit = k * lax.rsqrt(sums + 1.0)
    removal = unit * rate
    i = lax.broadcasted_iota(jnp.int32, (128, 128), 0)
    j = lax.broadcasted_iota(jnp.int32, (128, 128), 1)
    tri = jnp.where(i >= j, 1.0, 0.0).astype(bf16)
    hi, lo = split2(log_decay)
    rest = (log_decay - hi.astype(f32) - lo.astype(f32)).astype(bf16)
    cum = dot(cat([tri, tri, tri], 1), cat([hi, lo, rest], 0))
    mid = cum[63:64, :]
    last = cum[127:128, :]
    shrink = jnp.exp(cum - mid)
    grow = jnp.exp(mid - cum)
    alpha = jnp.exp(cum - log_decay - mid) * unit
    beta = removal * grow
    kappa = k * grow
    return alpha, shrink, beta, kappa, jnp.exp(mid), jnp.exp(last - mid), jnp.exp(last)


def pair_products(x, turned):
    parts = [split2(keep(x, head)) for head in (0, 1)]
    lhs = cat([cat([hi, lo], 1) for hi, lo in parts], 0)
    return dot(lhs, cat([turned, turned], 0))


def pick(x):
    first = (lax.broadcasted_iota(jnp.int32, (128, x.shape[1]), 1) & 127) < HD
    return jnp.where(first, x[:128], x[128:])


def inverses(lowers):
    i = lax.broadcasted_iota(jnp.int32, (128, 128), 0)
    j = lax.broadcasted_iota(jnp.int32, (128, 128), 1)
    apart = i ^ j
    same = apart < 32
    zero = jnp.zeros((128, 128), bf16)

    def packed(x):
        return (x[:32] + x[32:64]) + (x[64:96] + x[96:])

    def spread(x):
        return jnp.where(same, cat([x] * 4, 0), jnp.zeros((128, 128), x.dtype))

    eye = packed(jnp.where(i == j, 1.0, 0.0))
    inv = [eye - packed(jnp.where(apart == 1, low, zero).astype(f32)) for low in lowers]
    for size in (2, 8):
        inside = (apart >= size) & (apart < 4 * size)
        inv_b = [x.astype(bf16) for x in inv]
        hop = [
            dot(x, jnp.where(inside, low, zero)).astype(bf16) for x, low in zip(inv_b, lowers)
        ]
        both = [dot(h, cat([spread(h), spread(x)], 1)) for h, x in zip(hop, inv_b)]
        once = [x - y[:, 128:] for x, y in zip(inv, both)]
        inv = [
            x + dot(y[:, :128].astype(bf16), spread(x.astype(bf16))) for x, y in zip(once, both)
        ]
    inv = [spread(x) for x in inv]
    inv_b = [x.astype(bf16) for x in inv]
    outside = apart >= 32
    top = jnp.zeros((32, 128), bf16)
    hop = [
        dot(x[32:], jnp.where(outside, low, zero)).astype(bf16) for x, low in zip(inv_b, lowers)
    ]
    both = [dot(h, cat([cat([top, h], 0), x], 1)) for h, x in zip(hop, inv_b)]
    once = [cat([x[:32], x[32:] - y[:, 128:]], 0) for x, y in zip(inv, both)]
    last = [dot(y[32:, :128].astype(bf16), x.astype(bf16)) for x, y in zip(once, both)]
    return [cat([x[:64], x[64:] + y], 0).astype(bf16) for x, y in zip(once, last)]


def solve_all(invs, lows, sides):
    first = [pick(dot(inv, side.astype(bf16))).astype(bf16) for inv, side in zip(invs, sides)]
    back = [pick(dot(low, x)) for low, x in zip(lows, first)]
    miss = [
        (side - x.astype(f32) - y).astype(bf16) for side, x, y in zip(sides, first, back)
    ]
    return [x.astype(f32) + pick(dot(inv, m)) for x, inv, m in zip(first, invs, miss)]


def maps_of(z, value, beta_end, kappa_end, gain_end):
    zero = jnp.zeros((128, 128), bf16)
    lhs = cat([z.astype(bf16), cat([zero, -value], 1)], 0)
    both = dot_tn(lhs, cat([beta_end, kappa_end], 0).astype(bf16))
    first = lane_first((64, 128))
    packed = [
        jnp.where(first, both[o : o + 64], both[o + 64 : o + 128]) for o in (0, 128)
    ]
    i = lax.broadcasted_iota(jnp.int32, (64, 128), 0)
    j = lax.broadcasted_iota(jnp.int32, (64, 128), 1) & 63
    transit = jnp.where(i == j, gain_end, 0.0) - packed[0]
    return transit.astype(bf16), (-packed[1]).astype(bf16)


def after_given(state, transit):
    both = dot(cat(split2(state), 0), two_heads(transit))
    return both[:HD] + both[HD:]


def state_reads(reads, state):
    both = dot_nt(cat(split2(reads), 0), two_heads(state))
    return both[:128] + both[128:]


def head_mean(x):
    ones = block_ones()
    ones2 = cat([ones, ones], 0)
    parts = [head_sums(x[:, o : o + 128], ones2) for o in range(0, x.shape[1], 128)]
    return cat(parts, 1) * (1.0 / HD)


def kernel(
    tok, gain, wr, wk, wv, wd, wa, wg, wp, wgp, dbase, rbase, hgain, mix, pscale, wor, wop, init,
    own_out, arrived_out,
    tok_v, gain_v, weight_v, acc_v, proj_v, norm_v, square_v, base_v, mix_v, pscale_v, wout_v, init_v, init_in,
    scale_v, pool_v, keys_v, turn_v, low_v, side_v, z_v, reads_v, local_v, map_v, maps_in,
    gate_v, state_v, states_in, merged_v, recout_v, part_v,
    w_sem, small_sem, tok_send, tok_recv, halo_send, halo_recv, map_send, map_recv,
    st_send, st_recv, part_send, part_recv, init_send, init_recv, pair_sem, go_sem,
):
    sp = lax.axis_index("sp")
    tp = lax.axis_index("tp")
    other = 1 - tp
    weights = (wr, wk, wv, wd, wa, wg, wp, wgp)
    group_of, side, owning = 0, 0, 0
    for core in (0, 1):
        for g, owner in enumerate(OWNERS[core]):
            here = (sp == owner).astype(jnp.int32)
            group_of, side, owning = group_of + here * g, side + here * core, owning + here
    is_owner = (tp == 1) & (owning == 1)
    gives_init = (tp == 0) & (side == 0) & (owning == 1)
    keeps_init = (tp == 1) & (side == 1) & (owning == 1)

    def owner_of(g):
        return OWNERS[0][g] + tp * (OWNERS[1][g] - OWNERS[0][g])


    barrier = pltpu.get_barrier_semaphore()

    def tell(semaphore, **device):
        pl.semaphore_signal(semaphore, inc=1, device_id=device, device_id_type=MESH)

    @pl.when(tp == 1)
    def _():
        tell(barrier, tp=other)

    mine = pl.multiple_of(tp * HALF, HALF)
    theirs = pl.multiple_of(other * HALF, HALF)
    pool_at = pl.multiple_of(tp * PCOLS, 128)
    held = group_of
    small = [
        pltpu.make_async_copy(tok, tok_v, small_sem.at[0]),
        pltpu.make_async_copy(gain.at[:, pl.ds(mine, HALF)], gain_v, small_sem.at[1]),
        pltpu.make_async_copy(dbase, base_v.at[0], small_sem.at[2]),
        pltpu.make_async_copy(rbase, base_v.at[1], small_sem.at[3]),
        pltpu.make_async_copy(hgain, base_v.at[2], small_sem.at[4]),
        pltpu.make_async_copy(mix.at[pl.ds(tp * 2, 2)], mix_v, small_sem.at[5]),
        pltpu.make_async_copy(pscale.at[:, pl.ds(pool_at, PCOLS)], pscale_v, small_sem.at[6]),
        pltpu.make_async_copy(
            init.at[lax.div(held, PAIRS), pl.ds(2 * lax.rem(held, PAIRS), 2)],
            init_v,
            small_sem.at[7],
        ),
        pltpu.make_async_copy(wor, wout_v.at[pl.ds(0, RCOLS)], small_sem.at[8]),
        pltpu.make_async_copy(wop, wout_v.at[pl.ds(RCOLS, PCOLS)], small_sem.at[9]),
    ]
    loads = [
        [
            pltpu.make_async_copy(
                w.at[pl.ds(at, HALF)],
                weight_v.at[half, :, pl.ds(OFFS[i], WIDTHS[i])],
                w_sem.at[half, i],
            )
            for i, w in ((i, weights[i]) for i in NEED)
        ]
        for half, at in ((0, mine), (1, theirs))
    ]
    def start(copies):
        for copy in copies:
            copy.start()

    start(small[:2])
    start(loads[0][:2])

    small[0].wait()

    @pl.when(tp == 0)
    def _():
        pl.semaphore_wait(barrier, 1)
        tell(pair_sem, tp=other)

    start(loads[0][2:4])
    small[1].wait()
    wide = tok_v[...].reshape(TOK, HALF).astype(f32)
    norm_v[0] = (wide * gain_v[...]).astype(bf16)
    squares = wide * wide
    square_v[0] = sum(squares[:, o : o + 128] for o in range(0, HALF, 128))
    start(loads[1][:4] + small[2:4])

    @pl.when(tp == 1)
    def _():
        pl.semaphore_wait(pair_sem, 1)

        @pl.loop(1, N_SP)
        def _(step):
            tell(barrier, sp=lax.rem(sp + step, N_SP))

    send_tok = [
        pltpu.make_async_remote_copy(
            src_ref=ref.at[0],
            dst_ref=ref.at[1],
            send_sem=tok_send.at[i],
            recv_sem=tok_recv.at[i],
            device_id={"tp": other},
            device_id_type=MESH,
        )
        for i, ref in enumerate((norm_v, square_v))
    ]
    start(send_tok)
    early = (slice(0, EARLY // 2), slice(EARLY // 2, EARLY))
    for step, at in enumerate(early):
        for copy in loads[0][2 * step : 2 * step + 2]:
            copy.wait()
        acc_v[:, at] = dot(norm_v[0], weight_v[0, :, at])
        if step == 0:
            start(loads[0][4:] + loads[1][4:] + small[4:])

    send_tok[0].wait_recv()

    def scaled(total):
        return (total * cat([scale_v[...]] * (total.shape[1] // 128), 1)).astype(bf16)

    for step, at in enumerate(early):
        for copy in loads[1][2 * step : 2 * step + 2]:
            copy.wait()
        total = acc_v[:, at] + dot(norm_v[1], weight_v[1, :, at])
        if step == 0:
            send_tok[1].wait_recv()
            squares = jnp.sum(square_v[0] + square_v[1], axis=1, keepdims=True)
            scale = lax.rsqrt(squares * (1.0 / D) + 0.25)
            scale_v[...] = jnp.broadcast_to(scale, (TOK, 128))
        proj_v[:, at] = scaled(total)

    for copy in small[2:4]:
        copy.wait()
    groups = [(b, p) for b in range(SEQ) for p in range(PAIRS)]

    def part(index, b, p):
        at = OFFS[index] + 128 * p
        return proj_v[b * ROWS : (b + 1) * ROWS, at : at + 128]

    row = lax.broadcasted_iota(jnp.int32, (256, 128), 0) & 127
    col = lax.broadcasted_iota(jnp.int32, (256, 128), 1)
    strict = row > col
    inclusive = row >= col

    def rows_of(index, b):
        at = OFFS[index]
        return proj_v[b * ROWS : (b + 1) * ROWS, at : at + WIDTHS[index]].astype(f32)

    def local_row(index):
        return cat([base_v[index, pl.ds(3 * tp + p, 1), :] for p in range(PAIRS)], 1)

    small[7].wait()
    give = pltpu.make_async_remote_copy(
        src_ref=init_v,
        dst_ref=init_in,
        send_sem=init_send,
        recv_sem=init_recv,
        device_id={"tp": other},
        device_id_type=MESH,
    )

    @pl.when(gives_init)
    def _():
        give.start()

    @pl.when(keeps_init)
    def _():
        pltpu.make_async_copy(init_v, init_in, init_recv).start()

    ends = []
    for b in range(SEQ):
        alpha, shrink, beta, kappa, e_mid, e_tail, e_last = prepare(
            rows_of(1, b), rows_of(3, b), rows_of(4, b), local_row(0), local_row(1)
        )
        keys_v[b, 0] = alpha
        keys_v[b, 1] = shrink
        keys_v[b, 2] = beta
        keys_v[b, 3] = kappa
        ends.append((e_mid, e_tail, e_last))

    def pair_of(index, g):
        b, p = groups[g]
        return keys_v[b, index, :, 128 * p : 128 * p + 128]

    def end_of(index, g):
        b, p = groups[g]
        return ends[b][index][:, 128 * p : 128 * p + 128]

    every = range(GROUPS)
    for g in every:
        turned = cat([pair_of(2, g).astype(bf16).T, pair_of(3, g).astype(bf16).T], 1)
        turn_v[g] = turned
        pairs = pair_products(pair_of(0, g), turned)
        low_v[g] = jnp.where(strict, pairs[:, :128], 0.0).astype(bf16)
        cross = jnp.where(strict, pairs[:, 128:], 0.0).astype(bf16)
        side_v[g, :, :128] = pair_of(0, g) * end_of(0, g)
        side_v[g, :, 128:] = pick(dot(cross, part(2, *groups[g])))
    @pl.when(tp == 1)
    def _():
        pl.semaphore_wait(barrier, N_SP - 1)
        tell(go_sem, tp=other)

    by_head = inverses([low_v[g, 128 * h : 128 * h + 128, :] for g in every for h in (0, 1)])
    invs = [cat(by_head[2 * g : 2 * g + 2], 0) for g in every]
    map_copies = []
    solved = solve_all(invs, [low_v[g] for g in every], [side_v[g] for g in every])
    for g, z in zip(every, solved):
        z_v[g] = z.astype(bf16)
        tail = end_of(1, g)
        transit, written = maps_of(
            z, part(2, *groups[g]), pair_of(2, g) * tail, pair_of(3, g) * tail, end_of(2, g)
        )
        map_v[g, 0] = transit
        map_v[g, 1] = written
    @pl.when(tp == 0)
    def _():
        pl.semaphore_wait(go_sem, 1)

    own_map = [(tp == 1) & (sp == OWNERS[1][g]) for g in every]
    for g in every:
        copy = pltpu.make_async_remote_copy(
            src_ref=map_v.at[g],
            dst_ref=maps_in.at[sp],
            send_sem=map_send.at[g],
            recv_sem=map_recv.at[sp],
            device_id={"sp": owner_of(g), "tp": 1},
            device_id_type=MESH,
        )
        map_copies.append(copy)

        @pl.when(jnp.logical_not(own_map[g]) & (sp < N_SP - 1))
        def _():
            copy.start()

        @pl.when(own_map[g])
        def _():
            pltpu.make_async_copy(map_v.at[g], maps_in.at[sp], map_recv.at[sp]).start()

    def send_state(j):
        return pltpu.make_async_remote_copy(
            src_ref=state_v.at[j],
            dst_ref=states_in.at[group_of],
            send_sem=st_send.at[j],
            recv_sem=st_recv.at[group_of],
            device_id={"sp": j, "tp": side},
            device_id_type=MESH,
        )

    def wait_map(j):
        pltpu.make_async_copy(map_v.at[0], maps_in.at[j], map_recv.at[j]).wait()

    def centred(state):
        return (state - jnp.mean(state, axis=0, keepdims=True)).astype(bf16)

    def emit(j):
        @pl.when((j != sp) | (side == 0))
        def _():
            send_state(j).start()

    @pl.when(is_owner)
    def _():
        pltpu.make_async_copy(init_v, init_in, init_recv).wait()
        state_v[0] = centred(cat([init_in[0], init_in[1]], 1))
        emit(0)

    def late(index, copies, at):
        for half in (0, 1):
            for copy in loads[half][copies]:
                copy.wait()
        total = dot(norm_v[0], weight_v[0, :, at]) + dot(norm_v[1], weight_v[1, :, at])
        proj_v[:, at] = scaled(total)

    late(6, slice(6, 8), slice(OFFS[6], COLS))
    for b in range(SEQ):
        pool_v[b, 16:, :] = proj_v[b * ROWS : (b + 1) * ROWS, OFFS[6] : OFFS[7]]
    halo = pltpu.make_async_remote_copy(
        src_ref=pool_v.at[:, pl.ds(ROWS, 16), :],
        dst_ref=pool_v.at[:, pl.ds(0, 16), :],
        send_sem=halo_send,
        recv_sem=halo_recv,
        device_id={"sp": lax.rem(sp + 1, N_SP)},
        device_id_type=MESH,
    )

    @pl.when(sp < N_SP - 1)
    def _():
        halo.start()

    @pl.when(sp == 0)
    def _():
        pool_v[:, 0:16, :] = jnp.zeros((SEQ, 16, PCOLS), bf16)

    late(0, slice(4, 5), slice(OFFS[0], OFFS[5]))
    for g in every:
        rho = part(0, *groups[g]).astype(f32) * pair_of(1, g)
        pairs = pair_products(rho, turn_v[g])
        within_beta = jnp.where(inclusive, pairs[:, :128], 0.0).astype(bf16)
        within_kappa = jnp.where(inclusive, pairs[:, 128:], 0.0).astype(bf16)
        drop = pick(dot(within_beta, z_v[g]))
        reads_v[g] = rho * end_of(0, g) - drop[:, :128]
        local = pick(dot(within_kappa, part(2, *groups[g]))) - drop[:, 128:]
        local_v[g] = local - head_mean(local)
    def late_work():
        late(5, slice(5, 6), slice(OFFS[5], OFFS[6]))
        for copy in small[4:7] + small[8:]:
            copy.wait()
        for b in range(SEQ):
            gate = rows_of(5, b)
            gate_v[b] = local_row(2) * (gate * sig(gate))

        @pl.when(sp > 0)
        def _():
            halo.wait_recv()

        places = (sp * ROWS + 1 + lax.broadcasted_iota(jnp.int32, (ROWS, 128), 0)).astype(f32)
        for b in range(SEQ):
            outs = []
            for s in range(2):
                at = slice(128 * s, 128 * s + 128)
                own = pool_v[b, :, at].astype(f32)
                total = own + pltpu.roll(own, 1, 0)
                if s == 1:
                    total = total + pltpu.roll(total, 2, 0)
                wide = total + pltpu.roll(total, 2 if s == 0 else 4, 0)
                wide = wide + pltpu.roll(wide, 4 if s == 0 else 8, 0)
                trail = jnp.where(tp == 0, total, wide)[16:]
                window = jnp.where(tp == 0, float(2 << s), float(8 << s))
                diff = (trail / jnp.minimum(places, window) - own[16:]).astype(bf16)
                pooled = dot(diff, mix_v[s])
                gate = proj_v[b * ROWS : (b + 1) * ROWS, OFFS[7] + 128 * s : OFFS[7] + 128 * s + 128]
                gate = gate.astype(f32)
                outs.append((pooled * pscale_v[:, at] * (gate * sig(gate))).astype(bf16))
            recout_v[b * ROWS : (b + 1) * ROWS, RCOLS:] = cat(outs, 1)

        for at in (slice(0, 1024), slice(1024, D)):
            merged_v[:, at] = dot(recout_v[:, RCOLS:], wout_v[RCOLS:, at])

    @pl.when(sp < 6)
    def _():
        late_work()

    @pl.when(is_owner)
    def _():
        state = cat([init_in[0], init_in[1]], 1)
        for block in ((0,), (1,), (2,), (3,), (4, 5), (6, 7), (8,), (9,), (10,), (11,), (12,), (13,), (14,)):
            for j in block:
                wait_map(j)
            for j in block:
                state = after_given(state, maps_in[j, 0]) + maps_in[j, 1].astype(f32)
                state_v[j + 1] = centred(state)
            for j in block:
                emit(j + 1)

        @pl.when(side == 1)
        def _():
            pltpu.make_async_copy(
                state_v.at[sp], states_in.at[group_of], st_recv.at[group_of]
            ).start()

    @pl.when(sp >= 6)
    def _():
        late_work()

    for g in every:
        pltpu.make_async_copy(state_v.at[0], states_in.at[g], st_recv.at[g]).wait()
    centre = [state_reads(reads_v[g], states_in[g]) + local_v[g] for g in every]
    for b in range(SEQ):
        rec = cat(centre[PAIRS * b : PAIRS * b + PAIRS], 1)
        spread = head_mean(rec * rec)
        recout_v[b * ROWS : (b + 1) * ROWS, :RCOLS] = (
            rec * lax.rsqrt(spread + 1.0) * gate_v[b]
        ).astype(bf16)

    def product(at):
        total = merged_v[:, at] + dot(recout_v[:, :RCOLS], wout_v[:RCOLS, at])
        return total.astype(bf16).reshape(SEQ, ROWS, 512)

    def columns(ref, tile):
        return ref.at[:, :, pl.ds(512 * tile, 512)]

    def send_part(tile):
        return pltpu.make_async_remote_copy(
            src_ref=part_v.at[tile],
            dst_ref=columns(arrived_out, tile),
            send_sem=part_send.at[tile],
            recv_sem=part_recv.at[tile],
            device_id={"tp": other},
            device_id_type=MESH,
        )

    for tile in range(2):
        part_v[tile] = product(pl.ds(pl.multiple_of(theirs + tile * 512, 512), 512))
        send_part(tile).start()
    for tile in range(2):
        at = pl.ds(pl.multiple_of(mine + tile * 512, 512), 512)
        own_out[:, :, 512 * tile : 512 * tile + 512] = product(at)

    for copy in send_tok:
        copy.wait_send()

    @pl.when(sp < N_SP - 1)
    def _():
        halo.wait_send()

    for g, copy in enumerate(map_copies):
        @pl.when(jnp.logical_not(own_map[g]) & (sp < N_SP - 1))
        def _():
            copy.wait_send()

    @pl.when(gives_init)
    def _():
        give.wait_send()

    @pl.when(is_owner)
    def _():
        @pl.loop(0, N_SP)
        def _(j):
            @pl.when((j != sp) | (side == 0))
            def _():
                send_state(j).wait_send()

    for tile in range(2):
        send_part(tile).wait()


def shards(
    tokens, norm_gain, w_recept, w_key, w_value, w_decay, w_rate, w_gate_rec, w_pool, w_gate_pool,
    decay_base, rate_base, head_gain, pool_mix, pool_scale, w_out_rec, w_out_pool, init_state,
):
    vmem, sem = pltpu.VMEM, pltpu.SemaphoreType.DMA
    row = lambda x: x.reshape(1, -1)
    tile = lambda x: x.reshape(6, 128)
    scratch = [
        vmem((SEQ, ROWS, HALF), bf16),
        vmem((1, HALF), f32),
        vmem((2, HALF, COLS), bf16),
        vmem((TOK, EARLY), f32),
        vmem((TOK, COLS), bf16),
        vmem((2, TOK, HALF), bf16),
        vmem((2, TOK, 128), f32),
        vmem((3, 6, 128), f32),
        vmem((2, 128, 128), bf16),
        vmem((1, PCOLS), f32),
        vmem((RCOLS + PCOLS, D), bf16),
        vmem((2, HD, HD), f32),
        vmem((2, HD, HD), f32),
        vmem((TOK, 128), f32),
        vmem((SEQ, 16 + ROWS, PCOLS), bf16),
        vmem((SEQ, 4, ROWS, RCOLS), f32),
        vmem((GROUPS, 128, 256), bf16),
        vmem((GROUPS, 256, 128), bf16),
        vmem((GROUPS, 128, 256), f32),
        vmem((GROUPS, 128, 256), bf16),
        vmem((GROUPS, 128, 128), f32),
        vmem((GROUPS, 128, 128), f32),
        vmem((GROUPS, 2, HD, 128), bf16),
        vmem((N_SP, 2, HD, 128), bf16),
        vmem((SEQ, ROWS, RCOLS), f32),
        vmem((N_SP, HD, 128), bf16),
        vmem((GROUPS, HD, 128), bf16),
        vmem((TOK, D), f32),
        vmem((TOK, RCOLS + PCOLS), bf16),
        vmem((2, SEQ, ROWS, 512), bf16),
        sem((2, 8)),
        sem((10,)),
        sem((2,)),
        sem((2,)),
        sem,
        sem,
        sem((GROUPS,)),
        sem((N_SP,)),
        sem((N_SP,)),
        sem((GROUPS,)),
        sem((2,)),
        sem((2,)),
        sem,
        sem,
        pltpu.SemaphoreType.REGULAR,
        pltpu.SemaphoreType.REGULAR,
    ]
    pin = lambda x: pltpu.with_memory_space_constraint(x, pltpu.HBM)
    own, arrived = pl.pallas_call(
        kernel,
        out_shape=[jax.ShapeDtypeStruct((SEQ, ROWS, HALF), bf16)] * 2,
        in_specs=[pl.BlockSpec(memory_space=pl.ANY)] * 18,
        out_specs=[pl.BlockSpec(memory_space=pltpu.VMEM)] * 2,
        scratch_shapes=scratch,
        compiler_params=pltpu.CompilerParams(
            collective_id=0, has_side_effects=True, vmem_limit_bytes=48 << 20
        ),
        name="layer",
    )(*(pin(x) for x in (
        tokens, row(norm_gain), w_recept, w_key, w_value, w_decay, w_rate, w_gate_rec, w_pool,
        w_gate_pool, tile(decay_base), tile(rate_base), tile(head_gain), pool_mix, row(pool_scale),
        w_out_rec, w_out_pool, init_state,
    )))
    return (own.astype(f32) + arrived.astype(f32)).astype(bf16)


def solution(mesh):
    split = P(None, "tp")
    placed = (
        P("fs", "sp", "tp"), P(),
        split, split, split, split, split, split, split, split,
        P(), P(), P(), P(), P(),
        P("tp", None), P("tp", None), P("fs", "tp", None, None),
    )
    return jax.shard_map(
        shards, mesh=mesh, in_specs=placed, out_specs=P("fs", "sp", "tp"), check_vma=False
    )
```

```python
import math

import jax
import jax.numpy as jnp
from jax import lax
from jax.experimental import pallas as pl
from jax.experimental.pallas import tpu as pltpu
from jax.sharding import PartitionSpec as P

D = 2048
HALF = 1024
SEQ = 2
ROWS = 128
TOK = SEQ * ROWS
RCOLS = 384
PCOLS = 256
PAIRS = 3
GROUPS = SEQ * PAIRS
HD = 64
N_SP = 16
COLS = 6 * RCOLS + 2 * PCOLS
OFFS = (1536, 0, 1152, 384, 768, 1920, 2304, 2560)
NEED = (1, 3, 4, 2, 0, 5, 6, 7)
EARLY = 4 * RCOLS
OWNERS = ((0, 2, 4, 6, 8, 10), (1, 3, 5, 7, 9, 11))
WIDTHS = (384, 384, 384, 384, 384, 384, 256, 256)
MESH = pl.DeviceIdType.MESH
f32 = jnp.float32
bf16 = jnp.bfloat16


def dot(a, b):
    return lax.dot_general(a, b, (((1,), (0,)), ((), ())), preferred_element_type=f32)


def dot_nt(a, b):
    return lax.dot_general(a, b, (((1,), (1,)), ((), ())), preferred_element_type=f32)


def dot_tn(a, b):
    return lax.dot_general(a, b, (((0,), (0,)), ((), ())), preferred_element_type=f32)


def split2(x):
    hi = x.astype(bf16)
    return hi, (x - hi.astype(f32)).astype(bf16)


def cat(parts, axis):
    return jnp.concatenate(parts, axis=axis)


def sig(x):
    e = jnp.exp(-jnp.abs(x))
    return jnp.where(x >= 0, 1.0, e) / (1.0 + e)


def lane_first(shape):
    return lax.broadcasted_iota(jnp.int32, shape, len(shape) - 1) < HD


def keep(x, head):
    first = lane_first(x.shape)
    zero = jnp.zeros_like(x)
    return jnp.where(first, x, zero) if head == 0 else jnp.where(first, zero, x)


def two_heads(x):
    return cat([keep(x, 0), keep(x, 1)], 0)


def block_ones():
    i = lax.broadcasted_iota(jnp.int32, (128, 128), 0) < HD
    j = lax.broadcasted_iota(jnp.int32, (128, 128), 1) < HD
    return jnp.where(i == j, 1.0, 0.0).astype(bf16)


def head_sums(x, ones2):
    hi, lo = split2(x)
    return dot(cat([hi, lo], 1), ones2)


def prepare(k, d_in, a_in, d_base, a_base):
    ones = block_ones()
    ones2 = cat([ones, ones], 0)
    x = d_base + d_in
    log_decay = -math.exp(-0.5) * sig(x)
    rate = sig(a_base + a_in)
    squares = k * k
    sums = cat([head_sums(squares[:, o : o + 128], ones2) for o in range(0, RCOLS, 128)], 1)
    unit = k * lax.rsqrt(sums + 1.0)
    removal = unit * rate
    i = lax.broadcasted_iota(jnp.int32, (128, 128), 0)
    j = lax.broadcasted_iota(jnp.int32, (128, 128), 1)
    tri = jnp.where(i >= j, 1.0, 0.0).astype(bf16)
    hi, lo = split2(log_decay)
    rest = (log_decay - hi.astype(f32) - lo.astype(f32)).astype(bf16)
    cum = dot(cat([tri, tri, tri], 1), cat([hi, lo, rest], 0))
    mid = cum[63:64, :]
    last = cum[127:128, :]
    shrink = jnp.exp(cum - mid)
    grow = jnp.exp(mid - cum)
    alpha = jnp.exp(cum - log_decay - mid) * unit
    beta = removal * grow
    kappa = k * grow
    return alpha, shrink, beta, kappa, jnp.exp(mid), jnp.exp(last - mid), jnp.exp(last)


def pair_products(x, turned):
    parts = [split2(keep(x, head)) for head in (0, 1)]
    lhs = cat([cat([hi, lo], 1) for hi, lo in parts], 0)
    return dot(lhs, cat([turned, turned], 0))


def pick(x):
    first = (lax.broadcasted_iota(jnp.int32, (128, x.shape[1]), 1) & 127) < HD
    return jnp.where(first, x[:128], x[128:])


def inverses(lowers):
    i = lax.broadcasted_iota(jnp.int32, (128, 128), 0)
    j = lax.broadcasted_iota(jnp.int32, (128, 128), 1)
    apart = i ^ j
    same = apart < 32
    zero = jnp.zeros((128, 128), bf16)

    def packed(x):
        return (x[:32] + x[32:64]) + (x[64:96] + x[96:])

    def spread(x):
        return jnp.where(same, cat([x] * 4, 0), jnp.zeros((128, 128), x.dtype))

    eye = packed(jnp.where(i == j, 1.0, 0.0))
    inv = [eye - packed(jnp.where(apart == 1, low, zero).astype(f32)) for low in lowers]
    for size in (2, 8):
        inside = (apart >= size) & (apart < 4 * size)
        inv_b = [x.astype(bf16) for x in inv]
        hop = [
            dot(x, jnp.where(inside, low, zero)).astype(bf16) for x, low in zip(inv_b, lowers)
        ]
        both = [dot(h, cat([spread(h), spread(x)], 1)) for h, x in zip(hop, inv_b)]
        once = [x - y[:, 128:] for x, y in zip(inv, both)]
        inv = [
            x + dot(y[:, :128].astype(bf16), spread(x.astype(bf16))) for x, y in zip(once, both)
        ]
    inv = [spread(x) for x in inv]
    inv_b = [x.astype(bf16) for x in inv]
    outside = apart >= 32
    top = jnp.zeros((32, 128), bf16)
    hop = [
        dot(x[32:], jnp.where(outside, low, zero)).astype(bf16) for x, low in zip(inv_b, lowers)
    ]
    both = [dot(h, cat([cat([top, h], 0), x], 1)) for h, x in zip(hop, inv_b)]
    once = [cat([x[:32], x[32:] - y[:, 128:]], 0) for x, y in zip(inv, both)]
    last = [dot(y[32:, :128].astype(bf16), x.astype(bf16)) for x, y in zip(once, both)]
    return [cat([x[:64], x[64:] + y], 0).astype(bf16) for x, y in zip(once, last)]


def solve_all(invs, lows, sides):
    first = [pick(dot(inv, side.astype(bf16))).astype(bf16) for inv, side in zip(invs, sides)]
    back = [pick(dot(low, x)) for low, x in zip(lows, first)]
    miss = [
        (side - x.astype(f32) - y).astype(bf16) for side, x, y in zip(sides, first, back)
    ]
    return [x.astype(f32) + pick(dot(inv, m)) for x, inv, m in zip(first, invs, miss)]


def maps_of(z, value, beta_end, kappa_end, gain_end):
    zero = jnp.zeros((128, 128), bf16)
    lhs = cat([z.astype(bf16), cat([zero, -value], 1)], 0)
    both = dot_tn(lhs, cat([beta_end, kappa_end], 0).astype(bf16))
    first = lane_first((64, 128))
    packed = [
        jnp.where(first, both[o : o + 64], both[o + 64 : o + 128]) for o in (0, 128)
    ]
    i = lax.broadcasted_iota(jnp.int32, (64, 128), 0)
    j = lax.broadcasted_iota(jnp.int32, (64, 128), 1) & 63
    transit = jnp.where(i == j, gain_end, 0.0) - packed[0]
    return transit.astype(bf16), (-packed[1]).astype(bf16)


def after_given(state, transit):
    both = dot(cat(split2(state), 0), two_heads(transit))
    return both[:HD] + both[HD:]


def state_reads(reads, state):
    both = dot_nt(cat(split2(reads), 0), two_heads(state))
    return both[:128] + both[128:]


def head_mean(x):
    ones = block_ones()
    ones2 = cat([ones, ones], 0)
    parts = [head_sums(x[:, o : o + 128], ones2) for o in range(0, x.shape[1], 128)]
    return cat(parts, 1) * (1.0 / HD)


def kernel(
    tok, gain, wr, wk, wv, wd, wa, wg, wp, wgp, dbase, rbase, hgain, mix, pscale, wor, wop, init,
    own_out, arrived_out,
    tok_v, gain_v, weight_v, acc_v, proj_v, norm_v, square_v, base_v, mix_v, pscale_v, wout_v, init_v, init_in,
    scale_v, pool_v, keys_v, turn_v, low_v, side_v, z_v, reads_v, local_v, map_v, maps_in,
    gate_v, state_v, states_in, merged_v, recout_v, part_v,
    w_sem, small_sem, tok_send, tok_recv, halo_send, halo_recv, map_send, map_recv,
    st_send, st_recv, part_send, part_recv, init_send, init_recv, pair_sem, go_sem,
):
    sp = lax.axis_index("sp")
    tp = lax.axis_index("tp")
    other = 1 - tp
    weights = (wr, wk, wv, wd, wa, wg, wp, wgp)
    group_of, side, owning = 0, 0, 0
    for core in (0, 1):
        for g, owner in enumerate(OWNERS[core]):
            here = (sp == owner).astype(jnp.int32)
            group_of, side, owning = group_of + here * g, side + here * core, owning + here
    is_owner = (tp == 1) & (owning == 1)
    gives_init = (tp == 0) & (side == 0) & (owning == 1)
    keeps_init = (tp == 1) & (side == 1) & (owning == 1)

    def owner_of(g):
        return OWNERS[0][g] + tp * (OWNERS[1][g] - OWNERS[0][g])


    barrier = pltpu.get_barrier_semaphore()

    def tell(semaphore, **device):
        pl.semaphore_signal(semaphore, inc=1, device_id=device, device_id_type=MESH)

    @pl.when(tp == 1)
    def _():
        tell(barrier, tp=other)

    mine = pl.multiple_of(tp * HALF, HALF)
    theirs = pl.multiple_of(other * HALF, HALF)
    pool_at = pl.multiple_of(tp * PCOLS, 128)
    held = group_of
    small = [
        pltpu.make_async_copy(tok, tok_v, small_sem.at[0]),
        pltpu.make_async_copy(gain.at[:, pl.ds(mine, HALF)], gain_v, small_sem.at[1]),
        pltpu.make_async_copy(dbase, base_v.at[0], small_sem.at[2]),
        pltpu.make_async_copy(rbase, base_v.at[1], small_sem.at[3]),
        pltpu.make_async_copy(hgain, base_v.at[2], small_sem.at[4]),
        pltpu.make_async_copy(mix.at[pl.ds(tp * 2, 2)], mix_v, small_sem.at[5]),
        pltpu.make_async_copy(pscale.at[:, pl.ds(pool_at, PCOLS)], pscale_v, small_sem.at[6]),
        pltpu.make_async_copy(
            init.at[lax.div(held, PAIRS), pl.ds(2 * lax.rem(held, PAIRS), 2)],
            init_v,
            small_sem.at[7],
        ),
        pltpu.make_async_copy(wor, wout_v.at[pl.ds(0, RCOLS)], small_sem.at[8]),
        pltpu.make_async_copy(wop, wout_v.at[pl.ds(RCOLS, PCOLS)], small_sem.at[9]),
    ]
    loads = [
        [
            pltpu.make_async_copy(
                w.at[pl.ds(at, HALF)],
                weight_v.at[half, :, pl.ds(OFFS[i], WIDTHS[i])],
                w_sem.at[half, i],
            )
            for i, w in ((i, weights[i]) for i in NEED)
        ]
        for half, at in ((0, mine), (1, theirs))
    ]
    def start(copies):
        for copy in copies:
            copy.start()

    start(small[:2])
    start(loads[0][:2])

    small[0].wait()

    @pl.when(tp == 0)
    def _():
        pl.semaphore_wait(barrier, 1)
        tell(pair_sem, tp=other)

    start(loads[0][2:4])
    small[1].wait()
    wide = tok_v[...].reshape(TOK, HALF).astype(f32)
    norm_v[0] = (wide * gain_v[...]).astype(bf16)
    squares = wide * wide
    square_v[0] = sum(squares[:, o : o + 128] for o in range(0, HALF, 128))
    start(loads[1][:4] + small[2:4])

    @pl.when(tp == 1)
    def _():
        pl.semaphore_wait(pair_sem, 1)

        @pl.loop(1, N_SP)
        def _(step):
            tell(barrier, sp=lax.rem(sp + step, N_SP))

    send_tok = [
        pltpu.make_async_remote_copy(
            src_ref=ref.at[0],
            dst_ref=ref.at[1],
            send_sem=tok_send.at[i],
            recv_sem=tok_recv.at[i],
            device_id={"tp": other},
            device_id_type=MESH,
        )
        for i, ref in enumerate((norm_v, square_v))
    ]
    start(send_tok)
    early = (slice(0, EARLY // 2), slice(EARLY // 2, EARLY))
    for step, at in enumerate(early):
        for copy in loads[0][2 * step : 2 * step + 2]:
            copy.wait()
        acc_v[:, at] = dot(norm_v[0], weight_v[0, :, at])
        if step == 0:
            start(loads[0][4:] + loads[1][4:] + small[4:])

    send_tok[0].wait_recv()

    def scaled(total):
        return (total * cat([scale_v[...]] * (total.shape[1] // 128), 1)).astype(bf16)

    for step, at in enumerate(early):
        for copy in loads[1][2 * step : 2 * step + 2]:
            copy.wait()
        total = acc_v[:, at] + dot(norm_v[1], weight_v[1, :, at])
        if step == 0:
            send_tok[1].wait_recv()
            squares = jnp.sum(square_v[0] + square_v[1], axis=1, keepdims=True)
            scale = lax.rsqrt(squares * (1.0 / D) + 0.25)
            scale_v[...] = jnp.broadcast_to(scale, (TOK, 128))
        proj_v[:, at] = scaled(total)

    for copy in small[2:4]:
        copy.wait()
    groups = [(b, p) for b in range(SEQ) for p in range(PAIRS)]

    def part(index, b, p):
        at = OFFS[index] + 128 * p
        return proj_v[b * ROWS : (b + 1) * ROWS, at : at + 128]

    row = lax.broadcasted_iota(jnp.int32, (256, 128), 0) & 127
    col = lax.broadcasted_iota(jnp.int32, (256, 128), 1)
    strict = row > col
    inclusive = row >= col

    def rows_of(index, b):
        at = OFFS[index]
        return proj_v[b * ROWS : (b + 1) * ROWS, at : at + WIDTHS[index]].astype(f32)

    def local_row(index):
        return cat([base_v[index, pl.ds(3 * tp + p, 1), :] for p in range(PAIRS)], 1)

    small[7].wait()
    give = pltpu.make_async_remote_copy(
        src_ref=init_v,
        dst_ref=init_in,
        send_sem=init_send,
        recv_sem=init_recv,
        device_id={"tp": other},
        device_id_type=MESH,
    )

    @pl.when(gives_init)
    def _():
        give.start()

    @pl.when(keeps_init)
    def _():
        pltpu.make_async_copy(init_v, init_in, init_recv).start()

    ends = []
    for b in range(SEQ):
        alpha, shrink, beta, kappa, e_mid, e_tail, e_last = prepare(
            rows_of(1, b), rows_of(3, b), rows_of(4, b), local_row(0), local_row(1)
        )
        keys_v[b, 0] = alpha
        keys_v[b, 1] = shrink
        keys_v[b, 2] = beta
        keys_v[b, 3] = kappa
        ends.append((e_mid, e_tail, e_last))

    def pair_of(index, g):
        b, p = groups[g]
        return keys_v[b, index, :, 128 * p : 128 * p + 128]

    def end_of(index, g):
        b, p = groups[g]
        return ends[b][index][:, 128 * p : 128 * p + 128]

    every = range(GROUPS)
    turns = [
        cat([pair_of(2, g).astype(bf16).T, pair_of(3, g).astype(bf16).T], 1) for g in every
    ]
    products = [pair_products(pair_of(0, g), turns[g]) for g in every]
    crosses = [jnp.where(strict, x[:, 128:], 0.0).astype(bf16) for x in products]
    carried = [pick(dot(x, part(2, *groups[g]))) for g, x in zip(every, crosses)]
    for g in every:
        turn_v[g] = turns[g]
        low_v[g] = jnp.where(strict, products[g][:, :128], 0.0).astype(bf16)
        side_v[g, :, :128] = pair_of(0, g) * end_of(0, g)
        side_v[g, :, 128:] = carried[g]
    @pl.when(tp == 1)
    def _():
        pl.semaphore_wait(barrier, N_SP - 1)
        tell(go_sem, tp=other)

    by_head = inverses([low_v[g, 128 * h : 128 * h + 128, :] for g in every for h in (0, 1)])
    invs = [cat(by_head[2 * g : 2 * g + 2], 0) for g in every]
    map_copies = []
    solved = solve_all(invs, [low_v[g] for g in every], [side_v[g] for g in every])
    for g, z in zip(every, solved):
        z_v[g] = z.astype(bf16)
        tail = end_of(1, g)
        transit, written = maps_of(
            z, part(2, *groups[g]), pair_of(2, g) * tail, pair_of(3, g) * tail, end_of(2, g)
        )
        map_v[g, 0] = transit
        map_v[g, 1] = written
    @pl.when(tp == 0)
    def _():
        pl.semaphore_wait(go_sem, 1)

    own_map = [(tp == 1) & (sp == OWNERS[1][g]) for g in every]
    for g in every:
        copy = pltpu.make_async_remote_copy(
            src_ref=map_v.at[g],
            dst_ref=maps_in.at[sp],
            send_sem=map_send.at[g],
            recv_sem=map_recv.at[sp],
            device_id={"sp": owner_of(g), "tp": 1},
            device_id_type=MESH,
        )
        map_copies.append(copy)

        @pl.when(jnp.logical_not(own_map[g]) & (sp < N_SP - 1))
        def _():
            copy.start()

        @pl.when(own_map[g])
        def _():
            pltpu.make_async_copy(map_v.at[g], maps_in.at[sp], map_recv.at[sp]).start()

    def send_state(j):
        return pltpu.make_async_remote_copy(
            src_ref=state_v.at[j],
            dst_ref=states_in.at[group_of],
            send_sem=st_send.at[j],
            recv_sem=st_recv.at[group_of],
            device_id={"sp": j, "tp": side},
            device_id_type=MESH,
        )

    def wait_map(j):
        pltpu.make_async_copy(map_v.at[0], maps_in.at[j], map_recv.at[j]).wait()

    def centred(state):
        return (state - jnp.mean(state, axis=0, keepdims=True)).astype(bf16)

    def emit(j):
        @pl.when((j != sp) | (side == 0))
        def _():
            send_state(j).start()

    @pl.when(is_owner)
    def _():
        pltpu.make_async_copy(init_v, init_in, init_recv).wait()
        state_v[0] = centred(cat([init_in[0], init_in[1]], 1))
        emit(0)

    def late(index, copies, at):
        for half in (0, 1):
            for copy in loads[half][copies]:
                copy.wait()
        total = dot(norm_v[0], weight_v[0, :, at]) + dot(norm_v[1], weight_v[1, :, at])
        proj_v[:, at] = scaled(total)

    late(6, slice(6, 8), slice(OFFS[6], COLS))
    for b in range(SEQ):
        pool_v[b, 16:, :] = proj_v[b * ROWS : (b + 1) * ROWS, OFFS[6] : OFFS[7]]
    halo = pltpu.make_async_remote_copy(
        src_ref=pool_v.at[:, pl.ds(ROWS, 16), :],
        dst_ref=pool_v.at[:, pl.ds(0, 16), :],
        send_sem=halo_send,
        recv_sem=halo_recv,
        device_id={"sp": lax.rem(sp + 1, N_SP)},
        device_id_type=MESH,
    )

    @pl.when(sp < N_SP - 1)
    def _():
        halo.start()

    @pl.when(sp == 0)
    def _():
        pool_v[:, 0:16, :] = jnp.zeros((SEQ, 16, PCOLS), bf16)

    late(0, slice(4, 5), slice(OFFS[0], OFFS[5]))
    for g in every:
        rho = part(0, *groups[g]).astype(f32) * pair_of(1, g)
        pairs = pair_products(rho, turn_v[g])
        within_beta = jnp.where(inclusive, pairs[:, :128], 0.0).astype(bf16)
        within_kappa = jnp.where(inclusive, pairs[:, 128:], 0.0).astype(bf16)
        drop = pick(dot(within_beta, z_v[g]))
        reads_v[g] = rho * end_of(0, g) - drop[:, :128]
        local = pick(dot(within_kappa, part(2, *groups[g]))) - drop[:, 128:]
        local_v[g] = local - head_mean(local)
    def late_work():
        late(5, slice(5, 6), slice(OFFS[5], OFFS[6]))
        for copy in small[4:7] + small[8:]:
            copy.wait()
        for b in range(SEQ):
            gate = rows_of(5, b)
            gate_v[b] = local_row(2) * (gate * sig(gate))

        @pl.when(sp > 0)
        def _():
            halo.wait_recv()

        places = (sp * ROWS + 1 + lax.broadcasted_iota(jnp.int32, (ROWS, 128), 0)).astype(f32)
        for b in range(SEQ):
            outs = []
            for s in range(2):
                at = slice(128 * s, 128 * s + 128)
                own = pool_v[b, :, at].astype(f32)
                total = own + pltpu.roll(own, 1, 0)
                if s == 1:
                    total = total + pltpu.roll(total, 2, 0)
                wide = total + pltpu.roll(total, 2 if s == 0 else 4, 0)
                wide = wide + pltpu.roll(wide, 4 if s == 0 else 8, 0)
                trail = jnp.where(tp == 0, total, wide)[16:]
                window = jnp.where(tp == 0, float(2 << s), float(8 << s))
                diff = (trail / jnp.minimum(places, window) - own[16:]).astype(bf16)
                pooled = dot(diff, mix_v[s])
                gate = proj_v[b * ROWS : (b + 1) * ROWS, OFFS[7] + 128 * s : OFFS[7] + 128 * s + 128]
                gate = gate.astype(f32)
                outs.append((pooled * pscale_v[:, at] * (gate * sig(gate))).astype(bf16))
            recout_v[b * ROWS : (b + 1) * ROWS, RCOLS:] = cat(outs, 1)

        for at in (slice(0, 1024), slice(1024, D)):
            merged_v[:, at] = dot(recout_v[:, RCOLS:], wout_v[RCOLS:, at])

    @pl.when(sp < 6)
    def _():
        late_work()

    @pl.when(is_owner)
    def _():
        state = cat([init_in[0], init_in[1]], 1)
        for block in ((0,), (1,), (2,), (3,), (4, 5), (6, 7), (8,), (9,), (10,), (11,), (12,), (13,), (14,)):
            for j in block:
                wait_map(j)
            for j in block:
                state = after_given(state, maps_in[j, 0]) + maps_in[j, 1].astype(f32)
                state_v[j + 1] = centred(state)
            for j in block:
                emit(j + 1)

        @pl.when(side == 1)
        def _():
            pltpu.make_async_copy(
                state_v.at[sp], states_in.at[group_of], st_recv.at[group_of]
            ).start()

    @pl.when(sp >= 6)
    def _():
        late_work()

    for g in every:
        pltpu.make_async_copy(state_v.at[0], states_in.at[g], st_recv.at[g]).wait()
    centre = [state_reads(reads_v[g], states_in[g]) + local_v[g] for g in every]
    for b in range(SEQ):
        rec = cat(centre[PAIRS * b : PAIRS * b + PAIRS], 1)
        spread = head_mean(rec * rec)
        recout_v[b * ROWS : (b + 1) * ROWS, :RCOLS] = (
            rec * lax.rsqrt(spread + 1.0) * gate_v[b]
        ).astype(bf16)

    def product(at):
        total = merged_v[:, at] + dot(recout_v[:, :RCOLS], wout_v[:RCOLS, at])
        return total.astype(bf16).reshape(SEQ, ROWS, 512)

    def columns(ref, tile):
        return ref.at[:, :, pl.ds(512 * tile, 512)]

    def send_part(tile):
        return pltpu.make_async_remote_copy(
            src_ref=part_v.at[tile],
            dst_ref=columns(arrived_out, tile),
            send_sem=part_send.at[tile],
            recv_sem=part_recv.at[tile],
            device_id={"tp": other},
            device_id_type=MESH,
        )

    for tile in range(2):
        part_v[tile] = product(pl.ds(pl.multiple_of(theirs + tile * 512, 512), 512))
        send_part(tile).start()
    for tile in range(2):
        at = pl.ds(pl.multiple_of(mine + tile * 512, 512), 512)
        own_out[:, :, 512 * tile : 512 * tile + 512] = product(at)

    for copy in send_tok:
        copy.wait_send()

    @pl.when(sp < N_SP - 1)
    def _():
        halo.wait_send()

    for g, copy in enumerate(map_copies):
        @pl.when(jnp.logical_not(own_map[g]) & (sp < N_SP - 1))
        def _():
            copy.wait_send()

    @pl.when(gives_init)
    def _():
        give.wait_send()

    @pl.when(is_owner)
    def _():
        @pl.loop(0, N_SP)
        def _(j):
            @pl.when((j != sp) | (side == 0))
            def _():
                send_state(j).wait_send()

    for tile in range(2):
        send_part(tile).wait()


def shards(
    tokens, norm_gain, w_recept, w_key, w_value, w_decay, w_rate, w_gate_rec, w_pool, w_gate_pool,
    decay_base, rate_base, head_gain, pool_mix, pool_scale, w_out_rec, w_out_pool, init_state,
):
    vmem, sem = pltpu.VMEM, pltpu.SemaphoreType.DMA
    row = lambda x: x.reshape(1, -1)
    tile = lambda x: x.reshape(6, 128)
    scratch = [
        vmem((SEQ, ROWS, HALF), bf16),
        vmem((1, HALF), f32),
        vmem((2, HALF, COLS), bf16),
        vmem((TOK, EARLY), f32),
        vmem((TOK, COLS), bf16),
        vmem((2, TOK, HALF), bf16),
        vmem((2, TOK, 128), f32),
        vmem((3, 6, 128), f32),
        vmem((2, 128, 128), bf16),
        vmem((1, PCOLS), f32),
        vmem((RCOLS + PCOLS, D), bf16),
        vmem((2, HD, HD), f32),
        vmem((2, HD, HD), f32),
        vmem((TOK, 128), f32),
        vmem((SEQ, 16 + ROWS, PCOLS), bf16),
        vmem((SEQ, 4, ROWS, RCOLS), f32),
        vmem((GROUPS, 128, 256), bf16),
        vmem((GROUPS, 256, 128), bf16),
        vmem((GROUPS, 128, 256), f32),
        vmem((GROUPS, 128, 256), bf16),
        vmem((GROUPS, 128, 128), f32),
        vmem((GROUPS, 128, 128), f32),
        vmem((GROUPS, 2, HD, 128), bf16),
        vmem((N_SP, 2, HD, 128), bf16),
        vmem((SEQ, ROWS, RCOLS), f32),
        vmem((N_SP, HD, 128), bf16),
        vmem((GROUPS, HD, 128), bf16),
        vmem((TOK, D), f32),
        vmem((TOK, RCOLS + PCOLS), bf16),
        vmem((2, SEQ, ROWS, 512), bf16),
        sem((2, 8)),
        sem((10,)),
        sem((2,)),
        sem((2,)),
        sem,
        sem,
        sem((GROUPS,)),
        sem((N_SP,)),
        sem((N_SP,)),
        sem((GROUPS,)),
        sem((2,)),
        sem((2,)),
        sem,
        sem,
        pltpu.SemaphoreType.REGULAR,
        pltpu.SemaphoreType.REGULAR,
    ]
    pin = lambda x: pltpu.with_memory_space_constraint(x, pltpu.HBM)
    own, arrived = pl.pallas_call(
        kernel,
        out_shape=[jax.ShapeDtypeStruct((SEQ, ROWS, HALF), bf16)] * 2,
        in_specs=[pl.BlockSpec(memory_space=pl.ANY)] * 18,
        out_specs=[pl.BlockSpec(memory_space=pltpu.VMEM)] * 2,
        scratch_shapes=scratch,
        compiler_params=pltpu.CompilerParams(
            collective_id=0, has_side_effects=True, vmem_limit_bytes=48 << 20
        ),
        name="layer",
    )(*(pin(x) for x in (
        tokens, row(norm_gain), w_recept, w_key, w_value, w_decay, w_rate, w_gate_rec, w_pool,
        w_gate_pool, tile(decay_base), tile(rate_base), tile(head_gain), pool_mix, row(pool_scale),
        w_out_rec, w_out_pool, init_state,
    )))
    return (own.astype(f32) + arrived.astype(f32)).astype(bf16)


def solution(mesh):
    split = P(None, "tp")
    placed = (
        P("fs", "sp", "tp"), P(),
        split, split, split, split, split, split, split, split,
        P(), P(), P(), P(), P(),
        P("tp", None), P("tp", None), P("fs", "tp", None, None),
    )
    return jax.shard_map(
        shards, mesh=mesh, in_specs=placed, out_specs=P("fs", "sp", "tp"), check_vma=False
    )
```

```python
import math

import jax
import jax.numpy as jnp
from jax import lax
from jax.experimental import pallas as pl
from jax.experimental.pallas import tpu as pltpu
from jax.sharding import PartitionSpec as P

D = 2048
HALF = 1024
SEQ = 2
ROWS = 128
TOK = SEQ * ROWS
RCOLS = 384
PCOLS = 256
PAIRS = 3
GROUPS = SEQ * PAIRS
HD = 64
N_SP = 16
COLS = 6 * RCOLS + 2 * PCOLS
OFFS = (1536, 0, 1152, 384, 768, 1920, 2304, 2560)
NEED = (1, 3, 4, 2, 0, 5, 6, 7)
EARLY = 4 * RCOLS
OWNERS = ((0, 2, 4, 6, 8, 10), (1, 3, 5, 7, 9, 11))
WIDTHS = (384, 384, 384, 384, 384, 384, 256, 256)
MESH = pl.DeviceIdType.MESH
f32 = jnp.float32
bf16 = jnp.bfloat16


def dot(a, b):
    return lax.dot_general(a, b, (((1,), (0,)), ((), ())), preferred_element_type=f32)


def dot_nt(a, b):
    return lax.dot_general(a, b, (((1,), (1,)), ((), ())), preferred_element_type=f32)


def dot_tn(a, b):
    return lax.dot_general(a, b, (((0,), (0,)), ((), ())), preferred_element_type=f32)


def split2(x):
    hi = x.astype(bf16)
    return hi, (x - hi.astype(f32)).astype(bf16)


def cat(parts, axis):
    return jnp.concatenate(parts, axis=axis)


def sig(x):
    e = jnp.exp(-jnp.abs(x))
    return jnp.where(x >= 0, 1.0, e) / (1.0 + e)


def lane_first(shape):
    return lax.broadcasted_iota(jnp.int32, shape, len(shape) - 1) < HD


def keep(x, head):
    first = lane_first(x.shape)
    zero = jnp.zeros_like(x)
    return jnp.where(first, x, zero) if head == 0 else jnp.where(first, zero, x)


def two_heads(x):
    return cat([keep(x, 0), keep(x, 1)], 0)


def block_ones():
    i = lax.broadcasted_iota(jnp.int32, (128, 128), 0) < HD
    j = lax.broadcasted_iota(jnp.int32, (128, 128), 1) < HD
    return jnp.where(i == j, 1.0, 0.0).astype(bf16)


def head_sums(x, ones2):
    hi, lo = split2(x)
    return dot(cat([hi, lo], 1), ones2)


def prepare(k, d_in, a_in, d_base, a_base):
    ones = block_ones()
    ones2 = cat([ones, ones], 0)
    x = d_base + d_in
    log_decay = -math.exp(-0.5) * sig(x)
    rate = sig(a_base + a_in)
    squares = k * k
    sums = cat([head_sums(squares[:, o : o + 128], ones2) for o in range(0, RCOLS, 128)], 1)
    unit = k * lax.rsqrt(sums + 1.0)
    removal = unit * rate
    i = lax.broadcasted_iota(jnp.int32, (128, 128), 0)
    j = lax.broadcasted_iota(jnp.int32, (128, 128), 1)
    tri = jnp.where(i >= j, 1.0, 0.0).astype(bf16)
    hi, lo = split2(log_decay)
    rest = (log_decay - hi.astype(f32) - lo.astype(f32)).astype(bf16)
    cum = dot(cat([tri, tri, tri], 1), cat([hi, lo, rest], 0))
    mid = cum[63:64, :]
    last = cum[127:128, :]
    shrink = jnp.exp(cum - mid)
    grow = jnp.exp(mid - cum)
    alpha = jnp.exp(cum - log_decay - mid) * unit
    beta = removal * grow
    kappa = k * grow
    return alpha, shrink, beta, kappa, jnp.exp(mid), jnp.exp(last - mid), jnp.exp(last)


def pair_products(x, turned):
    parts = [split2(keep(x, head)) for head in (0, 1)]
    lhs = cat([cat([hi, lo], 1) for hi, lo in parts], 0)
    return dot(lhs, cat([turned, turned], 0))


def pick(x):
    first = (lax.broadcasted_iota(jnp.int32, (128, x.shape[1]), 1) & 127) < HD
    return jnp.where(first, x[:128], x[128:])


def inverses(lowers):
    i = lax.broadcasted_iota(jnp.int32, (128, 128), 0)
    j = lax.broadcasted_iota(jnp.int32, (128, 128), 1)
    apart = i ^ j
    same = apart < 32
    zero = jnp.zeros((128, 128), bf16)

    def packed(x):
        return (x[:32] + x[32:64]) + (x[64:96] + x[96:])

    def spread(x):
        return jnp.where(same, cat([x] * 4, 0), jnp.zeros((128, 128), x.dtype))

    eye = packed(jnp.where(i == j, 1.0, 0.0))
    inv = [eye - packed(jnp.where(apart == 1, low, zero).astype(f32)) for low in lowers]
    for size in (2, 8):
        inside = (apart >= size) & (apart < 4 * size)
        inv_b = [x.astype(bf16) for x in inv]
        hop = [
            dot(x, jnp.where(inside, low, zero)).astype(bf16) for x, low in zip(inv_b, lowers)
        ]
        both = [dot(h, cat([spread(h), spread(x)], 1)) for h, x in zip(hop, inv_b)]
        once = [x - y[:, 128:] for x, y in zip(inv, both)]
        inv = [
            x + dot(y[:, :128].astype(bf16), spread(x.astype(bf16))) for x, y in zip(once, both)
        ]
    inv = [spread(x) for x in inv]
    inv_b = [x.astype(bf16) for x in inv]
    outside = apart >= 32
    top = jnp.zeros((32, 128), bf16)
    hop = [
        dot(x[32:], jnp.where(outside, low, zero)).astype(bf16) for x, low in zip(inv_b, lowers)
    ]
    both = [dot(h, cat([cat([top, h], 0), x], 1)) for h, x in zip(hop, inv_b)]
    once = [cat([x[:32], x[32:] - y[:, 128:]], 0) for x, y in zip(inv, both)]
    last = [dot(y[32:, :128].astype(bf16), x.astype(bf16)) for x, y in zip(once, both)]
    return [cat([x[:64], x[64:] + y], 0).astype(bf16) for x, y in zip(once, last)]


def solve_all(invs, lows, sides):
    first = [pick(dot(inv, side.astype(bf16))).astype(bf16) for inv, side in zip(invs, sides)]
    back = [pick(dot(low, x)) for low, x in zip(lows, first)]
    miss = [
        (side - x.astype(f32) - y).astype(bf16) for side, x, y in zip(sides, first, back)
    ]
    return [x.astype(f32) + pick(dot(inv, m)) for x, inv, m in zip(first, invs, miss)]


def maps_of(z, value, beta_end, kappa_end, gain_end):
    zero = jnp.zeros((128, 128), bf16)
    lhs = cat([z.astype(bf16), cat([zero, -value], 1)], 0)
    both = dot_tn(lhs, cat([beta_end, kappa_end], 0).astype(bf16))
    first = lane_first((64, 128))
    packed = [
        jnp.where(first, both[o : o + 64], both[o + 64 : o + 128]) for o in (0, 128)
    ]
    i = lax.broadcasted_iota(jnp.int32, (64, 128), 0)
    j = lax.broadcasted_iota(jnp.int32, (64, 128), 1) & 63
    transit = jnp.where(i == j, gain_end, 0.0) - packed[0]
    return transit.astype(bf16), (-packed[1]).astype(bf16)


def after_given(state, transit):
    both = dot(cat(split2(state), 0), two_heads(transit))
    return both[:HD] + both[HD:]


def state_reads(reads, state):
    both = dot_nt(cat(split2(reads), 0), two_heads(state))
    return both[:128] + both[128:]


def head_mean(x):
    ones = block_ones()
    ones2 = cat([ones, ones], 0)
    parts = [head_sums(x[:, o : o + 128], ones2) for o in range(0, x.shape[1], 128)]
    return cat(parts, 1) * (1.0 / HD)


def kernel(
    tok, gain, wr, wk, wv, wd, wa, wg, wp, wgp, dbase, rbase, hgain, mix, pscale, wor, wop, init,
    own_out, arrived_out,
    tok_v, gain_v, weight_v, acc_v, proj_v, norm_v, square_v, base_v, mix_v, pscale_v, wout_v, init_v, init_in,
    scale_v, pool_v, keys_v, turn_v, low_v, side_v, z_v, reads_v, local_v, map_v, maps_in,
    gate_v, state_v, states_in, merged_v, recout_v, part_v,
    w_sem, small_sem, tok_send, tok_recv, halo_send, halo_recv, map_send, map_recv,
    st_send, st_recv, part_send, part_recv, init_send, init_recv, pair_sem, go_sem,
):
    sp = lax.axis_index("sp")
    tp = lax.axis_index("tp")
    other = 1 - tp
    weights = (wr, wk, wv, wd, wa, wg, wp, wgp)
    group_of, side, owning = 0, 0, 0
    for core in (0, 1):
        for g, owner in enumerate(OWNERS[core]):
            here = (sp == owner).astype(jnp.int32)
            group_of, side, owning = group_of + here * g, side + here * core, owning + here
    is_owner = (tp == 1) & (owning == 1)
    gives_init = (tp == 0) & (side == 0) & (owning == 1)
    keeps_init = (tp == 1) & (side == 1) & (owning == 1)

    def owner_of(g):
        return OWNERS[0][g] + tp * (OWNERS[1][g] - OWNERS[0][g])


    barrier = pltpu.get_barrier_semaphore()

    def tell(semaphore, **device):
        pl.semaphore_signal(semaphore, inc=1, device_id=device, device_id_type=MESH)

    @pl.when(tp == 1)
    def _():
        tell(barrier, tp=other)

    mine = pl.multiple_of(tp * HALF, HALF)
    theirs = pl.multiple_of(other * HALF, HALF)
    pool_at = pl.multiple_of(tp * PCOLS, 128)
    held = group_of
    small = [
        pltpu.make_async_copy(tok, tok_v, small_sem.at[0]),
        pltpu.make_async_copy(gain.at[:, pl.ds(mine, HALF)], gain_v, small_sem.at[1]),
        pltpu.make_async_copy(dbase, base_v.at[0], small_sem.at[2]),
        pltpu.make_async_copy(rbase, base_v.at[1], small_sem.at[3]),
        pltpu.make_async_copy(hgain, base_v.at[2], small_sem.at[4]),
        pltpu.make_async_copy(mix.at[pl.ds(tp * 2, 2)], mix_v, small_sem.at[5]),
        pltpu.make_async_copy(pscale.at[:, pl.ds(pool_at, PCOLS)], pscale_v, small_sem.at[6]),
        pltpu.make_async_copy(
            init.at[lax.div(held, PAIRS), pl.ds(2 * lax.rem(held, PAIRS), 2)],
            init_v,
            small_sem.at[7],
        ),
        pltpu.make_async_copy(wor, wout_v.at[pl.ds(0, RCOLS)], small_sem.at[8]),
        pltpu.make_async_copy(wop, wout_v.at[pl.ds(RCOLS, PCOLS)], small_sem.at[9]),
    ]
    loads = [
        [
            pltpu.make_async_copy(
                w.at[pl.ds(at, HALF)],
                weight_v.at[half, :, pl.ds(OFFS[i], WIDTHS[i])],
                w_sem.at[half, i],
            )
            for i, w in ((i, weights[i]) for i in NEED)
        ]
        for half, at in ((0, mine), (1, theirs))
    ]
    def start(copies):
        for copy in copies:
            copy.start()

    start(small[:2])
    start(loads[0][:2])

    small[0].wait()

    @pl.when(tp == 0)
    def _():
        pl.semaphore_wait(barrier, 1)
        tell(pair_sem, tp=other)

    start(loads[0][2:4])
    small[1].wait()
    wide = tok_v[...].reshape(TOK, HALF).astype(f32)
    norm_v[0] = (wide * gain_v[...]).astype(bf16)
    squares = wide * wide
    square_v[0] = sum(squares[:, o : o + 128] for o in range(0, HALF, 128))
    start(loads[1][:4] + small[2:4])

    @pl.when(tp == 1)
    def _():
        pl.semaphore_wait(pair_sem, 1)

        @pl.loop(1, N_SP)
        def _(step):
            tell(barrier, sp=lax.rem(sp + step, N_SP))

    send_tok = [
        pltpu.make_async_remote_copy(
            src_ref=ref.at[0],
            dst_ref=ref.at[1],
            send_sem=tok_send.at[i],
            recv_sem=tok_recv.at[i],
            device_id={"tp": other},
            device_id_type=MESH,
        )
        for i, ref in enumerate((norm_v, square_v))
    ]
    start(send_tok)
    early = (slice(0, EARLY // 2), slice(EARLY // 2, EARLY))
    for step, at in enumerate(early):
        for copy in loads[0][2 * step : 2 * step + 2]:
            copy.wait()
        acc_v[:, at] = dot(norm_v[0], weight_v[0, :, at])
        if step == 0:
            start(loads[0][4:] + loads[1][4:] + small[4:])

    send_tok[0].wait_recv()

    def scaled(total):
        return (total * cat([scale_v[...]] * (total.shape[1] // 128), 1)).astype(bf16)

    for step, at in enumerate(early):
        for copy in loads[1][2 * step : 2 * step + 2]:
            copy.wait()
        total = acc_v[:, at] + dot(norm_v[1], weight_v[1, :, at])
        if step == 0:
            send_tok[1].wait_recv()
            squares = jnp.sum(square_v[0] + square_v[1], axis=1, keepdims=True)
            scale = lax.rsqrt(squares * (1.0 / D) + 0.25)
            scale_v[...] = jnp.broadcast_to(scale, (TOK, 128))
        proj_v[:, at] = scaled(total)

    for copy in small[2:4]:
        copy.wait()
    groups = [(b, p) for b in range(SEQ) for p in range(PAIRS)]

    def part(index, b, p):
        at = OFFS[index] + 128 * p
        return proj_v[b * ROWS : (b + 1) * ROWS, at : at + 128]

    row = lax.broadcasted_iota(jnp.int32, (256, 128), 0) & 127
    col = lax.broadcasted_iota(jnp.int32, (256, 128), 1)
    strict = row > col
    inclusive = row >= col

    def rows_of(index, b):
        at = OFFS[index]
        return proj_v[b * ROWS : (b + 1) * ROWS, at : at + WIDTHS[index]].astype(f32)

    def local_row(index):
        return cat([base_v[index, pl.ds(3 * tp + p, 1), :] for p in range(PAIRS)], 1)

    small[7].wait()
    give = pltpu.make_async_remote_copy(
        src_ref=init_v,
        dst_ref=init_in,
        send_sem=init_send,
        recv_sem=init_recv,
        device_id={"tp": other},
        device_id_type=MESH,
    )

    @pl.when(gives_init)
    def _():
        give.start()

    @pl.when(keeps_init)
    def _():
        pltpu.make_async_copy(init_v, init_in, init_recv).start()

    ends = []
    for b in range(SEQ):
        alpha, shrink, beta, kappa, e_mid, e_tail, e_last = prepare(
            rows_of(1, b), rows_of(3, b), rows_of(4, b), local_row(0), local_row(1)
        )
        keys_v[b, 0] = alpha
        keys_v[b, 1] = shrink
        keys_v[b, 2] = beta
        keys_v[b, 3] = kappa
        ends.append((e_mid, e_tail, e_last))

    def pair_of(index, g):
        b, p = groups[g]
        return keys_v[b, index, :, 128 * p : 128 * p + 128]

    def end_of(index, g):
        b, p = groups[g]
        return ends[b][index][:, 128 * p : 128 * p + 128]

    every = range(GROUPS)
    turns = [
        cat([pair_of(2, g).astype(bf16).T, pair_of(3, g).astype(bf16).T], 1) for g in every
    ]
    products = [pair_products(pair_of(0, g), turns[g]) for g in every]
    crosses = [jnp.where(strict, x[:, 128:], 0.0).astype(bf16) for x in products]
    carried = [pick(dot(x, part(2, *groups[g]))) for g, x in zip(every, crosses)]
    for g in every:
        turn_v[g] = turns[g]
        low_v[g] = jnp.where(strict, products[g][:, :128], 0.0).astype(bf16)
        side_v[g, :, :128] = pair_of(0, g) * end_of(0, g)
        side_v[g, :, 128:] = carried[g]
    @pl.when(tp == 1)
    def _():
        pl.semaphore_wait(barrier, N_SP - 1)
        tell(go_sem, tp=other)

    by_head = inverses([low_v[g, 128 * h : 128 * h + 128, :] for g in every for h in (0, 1)])
    invs = [cat(by_head[2 * g : 2 * g + 2], 0) for g in every]
    map_copies = []
    solved = solve_all(invs, [low_v[g] for g in every], [side_v[g] for g in every])
    for g, z in zip(every, solved):
        z_v[g] = z.astype(bf16)
        tail = end_of(1, g)
        transit, written = maps_of(
            z, part(2, *groups[g]), pair_of(2, g) * tail, pair_of(3, g) * tail, end_of(2, g)
        )
        map_v[g, 0] = transit
        map_v[g, 1] = written
    @pl.when(tp == 0)
    def _():
        pl.semaphore_wait(go_sem, 1)

    own_map = [(tp == 1) & (sp == OWNERS[1][g]) for g in every]
    for g in every:
        copy = pltpu.make_async_remote_copy(
            src_ref=map_v.at[g],
            dst_ref=maps_in.at[sp],
            send_sem=map_send.at[g],
            recv_sem=map_recv.at[sp],
            device_id={"sp": owner_of(g), "tp": 1},
            device_id_type=MESH,
        )
        map_copies.append(copy)

        @pl.when(jnp.logical_not(own_map[g]) & (sp < N_SP - 1))
        def _():
            copy.start()

        @pl.when(own_map[g])
        def _():
            pltpu.make_async_copy(map_v.at[g], maps_in.at[sp], map_recv.at[sp]).start()

    def send_state(j):
        return pltpu.make_async_remote_copy(
            src_ref=state_v.at[j],
            dst_ref=states_in.at[group_of],
            send_sem=st_send.at[j],
            recv_sem=st_recv.at[group_of],
            device_id={"sp": j, "tp": side},
            device_id_type=MESH,
        )

    def wait_map(j):
        pltpu.make_async_copy(map_v.at[0], maps_in.at[j], map_recv.at[j]).wait()

    def centred(state):
        return (state - jnp.mean(state, axis=0, keepdims=True)).astype(bf16)

    def emit(j):
        @pl.when((j != sp) | (side == 0))
        def _():
            send_state(j).start()

    @pl.when(is_owner)
    def _():
        pltpu.make_async_copy(init_v, init_in, init_recv).wait()
        state_v[0] = centred(cat([init_in[0], init_in[1]], 1))
        emit(0)

    def late(index, copies, at):
        for half in (0, 1):
            for copy in loads[half][copies]:
                copy.wait()
        total = dot(norm_v[0], weight_v[0, :, at]) + dot(norm_v[1], weight_v[1, :, at])
        proj_v[:, at] = scaled(total)

    late(6, slice(6, 8), slice(OFFS[6], COLS))
    for b in range(SEQ):
        pool_v[b, 16:, :] = proj_v[b * ROWS : (b + 1) * ROWS, OFFS[6] : OFFS[7]]
    halo = pltpu.make_async_remote_copy(
        src_ref=pool_v.at[:, pl.ds(ROWS, 16), :],
        dst_ref=pool_v.at[:, pl.ds(0, 16), :],
        send_sem=halo_send,
        recv_sem=halo_recv,
        device_id={"sp": lax.rem(sp + 1, N_SP)},
        device_id_type=MESH,
    )

    @pl.when(sp < N_SP - 1)
    def _():
        halo.start()

    @pl.when(sp == 0)
    def _():
        pool_v[:, 0:16, :] = jnp.zeros((SEQ, 16, PCOLS), bf16)

    late(0, slice(4, 5), slice(OFFS[0], OFFS[5]))
    rhos = [part(0, *groups[g]).astype(f32) * pair_of(1, g) for g in every]
    products = [pair_products(rho, turn_v[g]) for g, rho in zip(every, rhos)]
    masked = [
        [jnp.where(inclusive, x[:, o : o + 128], 0.0).astype(bf16) for o in (0, 128)]
        for x in products
    ]
    drops = [pick(dot(masked[g][0], z_v[g])) for g in every]
    adds = [pick(dot(masked[g][1], part(2, *groups[g]))) for g in every]
    locals_ = [x - y[:, 128:] for x, y in zip(adds, drops)]
    means = [head_mean(x) for x in locals_]
    for g in every:
        reads_v[g] = rhos[g] * end_of(0, g) - drops[g][:, :128]
        local_v[g] = locals_[g] - means[g]
    def late_work():
        late(5, slice(5, 6), slice(OFFS[5], OFFS[6]))
        for copy in small[4:7] + small[8:]:
            copy.wait()
        for b in range(SEQ):
            gate = rows_of(5, b)
            gate_v[b] = local_row(2) * (gate * sig(gate))

        @pl.when(sp > 0)
        def _():
            halo.wait_recv()

        places = (sp * ROWS + 1 + lax.broadcasted_iota(jnp.int32, (ROWS, 128), 0)).astype(f32)
        for b in range(SEQ):
            outs = []
            for s in range(2):
                at = slice(128 * s, 128 * s + 128)
                own = pool_v[b, :, at].astype(f32)
                total = own + pltpu.roll(own, 1, 0)
                if s == 1:
                    total = total + pltpu.roll(total, 2, 0)
                wide = total + pltpu.roll(total, 2 if s == 0 else 4, 0)
                wide = wide + pltpu.roll(wide, 4 if s == 0 else 8, 0)
                trail = jnp.where(tp == 0, total, wide)[16:]
                window = jnp.where(tp == 0, float(2 << s), float(8 << s))
                diff = (trail / jnp.minimum(places, window) - own[16:]).astype(bf16)
                pooled = dot(diff, mix_v[s])
                gate = proj_v[b * ROWS : (b + 1) * ROWS, OFFS[7] + 128 * s : OFFS[7] + 128 * s + 128]
                gate = gate.astype(f32)
                outs.append((pooled * pscale_v[:, at] * (gate * sig(gate))).astype(bf16))
            recout_v[b * ROWS : (b + 1) * ROWS, RCOLS:] = cat(outs, 1)

        for at in (slice(0, 1024), slice(1024, D)):
            merged_v[:, at] = dot(recout_v[:, RCOLS:], wout_v[RCOLS:, at])

    @pl.when(sp < 6)
    def _():
        late_work()

    @pl.when(is_owner)
    def _():
        state = cat([init_in[0], init_in[1]], 1)
        for block in ((0,), (1,), (2,), (3,), (4, 5), (6, 7), (8,), (9,), (10,), (11,), (12,), (13,), (14,)):
            for j in block:
                wait_map(j)
            for j in block:
                state = after_given(state, maps_in[j, 0]) + maps_in[j, 1].astype(f32)
                state_v[j + 1] = centred(state)
            for j in block:
                emit(j + 1)

        @pl.when(side == 1)
        def _():
            pltpu.make_async_copy(
                state_v.at[sp], states_in.at[group_of], st_recv.at[group_of]
            ).start()

    @pl.when(sp >= 6)
    def _():
        late_work()

    for g in every:
        pltpu.make_async_copy(state_v.at[0], states_in.at[g], st_recv.at[g]).wait()
    centre = [state_reads(reads_v[g], states_in[g]) + local_v[g] for g in every]
    for b in range(SEQ):
        rec = cat(centre[PAIRS * b : PAIRS * b + PAIRS], 1)
        spread = head_mean(rec * rec)
        recout_v[b * ROWS : (b + 1) * ROWS, :RCOLS] = (
            rec * lax.rsqrt(spread + 1.0) * gate_v[b]
        ).astype(bf16)

    def product(at):
        total = merged_v[:, at] + dot(recout_v[:, :RCOLS], wout_v[:RCOLS, at])
        return total.astype(bf16).reshape(SEQ, ROWS, 512)

    def columns(ref, tile):
        return ref.at[:, :, pl.ds(512 * tile, 512)]

    def send_part(tile):
        return pltpu.make_async_remote_copy(
            src_ref=part_v.at[tile],
            dst_ref=columns(arrived_out, tile),
            send_sem=part_send.at[tile],
            recv_sem=part_recv.at[tile],
            device_id={"tp": other},
            device_id_type=MESH,
        )

    for tile in range(2):
        part_v[tile] = product(pl.ds(pl.multiple_of(theirs + tile * 512, 512), 512))
        send_part(tile).start()
    for tile in range(2):
        at = pl.ds(pl.multiple_of(mine + tile * 512, 512), 512)
        own_out[:, :, 512 * tile : 512 * tile + 512] = product(at)

    for copy in send_tok:
        copy.wait_send()

    @pl.when(sp < N_SP - 1)
    def _():
        halo.wait_send()

    for g, copy in enumerate(map_copies):
        @pl.when(jnp.logical_not(own_map[g]) & (sp < N_SP - 1))
        def _():
            copy.wait_send()

    @pl.when(gives_init)
    def _():
        give.wait_send()

    @pl.when(is_owner)
    def _():
        @pl.loop(0, N_SP)
        def _(j):
            @pl.when((j != sp) | (side == 0))
            def _():
                send_state(j).wait_send()

    for tile in range(2):
        send_part(tile).wait()


def shards(
    tokens, norm_gain, w_recept, w_key, w_value, w_decay, w_rate, w_gate_rec, w_pool, w_gate_pool,
    decay_base, rate_base, head_gain, pool_mix, pool_scale, w_out_rec, w_out_pool, init_state,
):
    vmem, sem = pltpu.VMEM, pltpu.SemaphoreType.DMA
    row = lambda x: x.reshape(1, -1)
    tile = lambda x: x.reshape(6, 128)
    scratch = [
        vmem((SEQ, ROWS, HALF), bf16),
        vmem((1, HALF), f32),
        vmem((2, HALF, COLS), bf16),
        vmem((TOK, EARLY), f32),
        vmem((TOK, COLS), bf16),
        vmem((2, TOK, HALF), bf16),
        vmem((2, TOK, 128), f32),
        vmem((3, 6, 128), f32),
        vmem((2, 128, 128), bf16),
        vmem((1, PCOLS), f32),
        vmem((RCOLS + PCOLS, D), bf16),
        vmem((2, HD, HD), f32),
        vmem((2, HD, HD), f32),
        vmem((TOK, 128), f32),
        vmem((SEQ, 16 + ROWS, PCOLS), bf16),
        vmem((SEQ, 4, ROWS, RCOLS), f32),
        vmem((GROUPS, 128, 256), bf16),
        vmem((GROUPS, 256, 128), bf16),
        vmem((GROUPS, 128, 256), f32),
        vmem((GROUPS, 128, 256), bf16),
        vmem((GROUPS, 128, 128), f32),
        vmem((GROUPS, 128, 128), f32),
        vmem((GROUPS, 2, HD, 128), bf16),
        vmem((N_SP, 2, HD, 128), bf16),
        vmem((SEQ, ROWS, RCOLS), f32),
        vmem((N_SP, HD, 128), bf16),
        vmem((GROUPS, HD, 128), bf16),
        vmem((TOK, D), f32),
        vmem((TOK, RCOLS + PCOLS), bf16),
        vmem((2, SEQ, ROWS, 512), bf16),
        sem((2, 8)),
        sem((10,)),
        sem((2,)),
        sem((2,)),
        sem,
        sem,
        sem((GROUPS,)),
        sem((N_SP,)),
        sem((N_SP,)),
        sem((GROUPS,)),
        sem((2,)),
        sem((2,)),
        sem,
        sem,
        pltpu.SemaphoreType.REGULAR,
        pltpu.SemaphoreType.REGULAR,
    ]
    pin = lambda x: pltpu.with_memory_space_constraint(x, pltpu.HBM)
    own, arrived = pl.pallas_call(
        kernel,
        out_shape=[jax.ShapeDtypeStruct((SEQ, ROWS, HALF), bf16)] * 2,
        in_specs=[pl.BlockSpec(memory_space=pl.ANY)] * 18,
        out_specs=[pl.BlockSpec(memory_space=pltpu.VMEM)] * 2,
        scratch_shapes=scratch,
        compiler_params=pltpu.CompilerParams(
            collective_id=0, has_side_effects=True, vmem_limit_bytes=48 << 20
        ),
        name="layer",
    )(*(pin(x) for x in (
        tokens, row(norm_gain), w_recept, w_key, w_value, w_decay, w_rate, w_gate_rec, w_pool,
        w_gate_pool, tile(decay_base), tile(rate_base), tile(head_gain), pool_mix, row(pool_scale),
        w_out_rec, w_out_pool, init_state,
    )))
    return (own.astype(f32) + arrived.astype(f32)).astype(bf16)


def solution(mesh):
    split = P(None, "tp")
    placed = (
        P("fs", "sp", "tp"), P(),
        split, split, split, split, split, split, split, split,
        P(), P(), P(), P(), P(),
        P("tp", None), P("tp", None), P("fs", "tp", None, None),
    )
    return jax.shard_map(
        shards, mesh=mesh, in_specs=placed, out_specs=P("fs", "sp", "tp"), check_vma=False
    )
```
